128 devices in a mesh: rep: 2 (over z_hi), fs: 32 (over z_lo, y, x), tp: 2 (over core).
Axes of the slice: x: 4, y: 4, z: 4 (z_hi: 2, z_lo: 2; z = z_hi * 2 + z_lo), core: 2. Of those that a mesh axis runs over, the one named last changes fastest.
Arguments:
- tokens: bfloat16 [40960, 2048], P(('rep', 'fs'), 'tp'), may hold values from -6 to 6
- norm_first: float32 [2048], replicated, may hold values from 0.1 to 1.9
- norm_mix: float32 [2048], replicated, may hold values from 0.1 to 1.9
- norm_second: float32 [2048], replicated, may hold values from 0.1 to 1.9
- gate_weight: float32 [2048, 2816], P('fs', 'tp'), may hold values from -0.125 to 0.125
- up_weight: float32 [2048, 2816], P('fs', 'tp'), may hold values from -0.125 to 0.125
- down_weight: float32 [2816, 2048], P('tp', 'fs'), may hold values from -0.109375 to 0.109375
- gate_scale: float32 [2816], P('tp'), may hold values from 0.3 to 3
- up_scale: float32 [2816], P('tp'), may hold values from 0.3 to 3
- down_scale: float32 [2048], P('fs'), may hold values from 0.3 to 3
- u_weight: float32 [2048, 1024], P('fs', 'tp'), may hold values from -0.125 to 0.125
- v_weight: float32 [2048, 1024], P('fs', 'tp'), may hold values from -0.125 to 0.125
- u_scale: float32 [1024], P('tp'), may hold values from 0.3 to 3
- v_scale: float32 [1024], P('tp'), may hold values from 0.15 to 6
- ln_gain: float32 [1024], P('tp'), may hold values from 0.1 to 1.9
- ln_bias: float32 [1024], P('tp'), may hold values from -3 to 3
- spatial_weight: bfloat16 [8, 128, 128], P('tp'), may hold values from -0.25 to 0.25
- spatial_bias: float32 [8, 128], P('tp'), may hold values from 0.1 to 1.9
- out_weight: float32 [1024, 2048], P('tp', 'fs'), may hold values from -0.1875 to 0.1875
- out_scale: float32 [2048], P('fs'), may hold values from 0.3 to 3
Outputs:
- layer_out: bfloat16 [40960, 2048], P(('rep', 'fs'), 'tp')
The draws below stay inside these ranges and needn't reach their ends.
All inputs are finite; a program needn't handle non-finite values.
Results may differ from the reference program's by a relative error of at most 0.019.
Values may be sent and summed in bfloat16 or wider, within the bound.
No kernel may reach another device: no remote copies, remote signals or barrier semaphores. Data moves between devices by JAX's collectives and lax.ppermute only.
A program may use at most 128 MiB of HBM per device.

```python
import math
import jax
import jax.numpy as jnp
from jax import lax

D = 2048
FF = 2816
BW = 1024
SPAN = 128
GROUPS = 8
TOKENS = 40960
N_TP = 2


def draw_v_scale(key, part):
    position = jnp.arange(BW, dtype=jnp.float32) / (BW - 1)
    rough = jax.random.uniform(key, (BW,), jnp.float32, 0.6, 1.4)
    return (10.0 ** (position - 0.5) * rough).astype(jnp.float32)


def steps_of(key, shape, pieces, least, largest):
    level = 1.0
    for dim, blocks in pieces:
        draws = jax.random.uniform(jax.random.fold_in(jax.random.fold_in(key, 6), dim), (blocks,), jnp.float32, least / len(pieces), largest / len(pieces))
        level = level * jnp.repeat(jnp.exp(draws), shape[dim] // blocks).reshape((-1,) + (1,) * (len(shape) - 1 - dim))
    return level


def centred(rng, dims, deviation, limit, split=(), kind=jnp.bfloat16):
    values = deviation * jax.random.normal(rng, dims, jnp.float32)
    if split:
        values = values * steps_of(rng, dims, split, -0.22, 0.18)
    return jnp.clip(values, -limit, limit).astype(kind)


def setup_inputs(seed: int = 0) -> dict:
    splits = jax.random.split(jax.random.key(seed), 21)
    return {
        "tokens": centred(splits[0], (TOKENS, D), 1.0, 6.0, ((0, 64), (1, 2))),
        "norm_first": jnp.clip(1.0 + 0.18 * jax.random.normal(splits[1], (D,), jnp.float32), 0.1, 1.9),
        "norm_mix": jnp.clip(1.0 + 0.18 * jax.random.normal(splits[2], (D,), jnp.float32), 0.1, 1.9),
        "norm_second": jnp.clip(1.0 + 0.18 * jax.random.normal(splits[3], (D,), jnp.float32), 0.1, 1.9),
        "gate_weight": centred(splits[4], (D, FF), D ** -0.5, 0.125, ((0, 32), (1, 2)), jnp.float32),
        "up_weight": centred(splits[5], (D, FF), D ** -0.5, 0.125, ((0, 32), (1, 2)), jnp.float32),
        "down_weight": centred(splits[6], (FF, D), FF ** -0.5, 0.109375, ((0, 2), (1, 32)), jnp.float32),
        "gate_scale": jnp.clip(jnp.exp(math.log(3.0) - 2.3025851 * jax.random.uniform(splits[7], (FF,), jnp.float32) ** steps_of(splits[7], (FF,), ((0, 2),), -0.2, 0.2)), 0.3, 3.0),
        "up_scale": jnp.clip(jnp.exp(math.log(3.0) - 2.3025851 * jax.random.uniform(splits[8], (FF,), jnp.float32) ** steps_of(splits[8], (FF,), ((0, 2),), -0.2, 0.2)), 0.3, 3.0),
        "down_scale": jnp.clip(jnp.exp(math.log(3.0) - 2.3025851 * jax.random.uniform(splits[9], (D,), jnp.float32) ** steps_of(splits[9], (D,), ((0, 32),), -0.2, 0.2)), 0.3, 3.0),
        "u_weight": centred(splits[10], (D, BW), D ** -0.5, 0.125, ((0, 32), (1, 2)), jnp.float32),
        "v_weight": centred(splits[11], (D, BW), D ** -0.5, 0.125, ((0, 32), (1, 2)), jnp.float32),
        "u_scale": jnp.clip(jnp.exp(math.log(3.0) - 2.3025851 * jax.random.uniform(splits[12], (BW,), jnp.float32) ** steps_of(splits[12], (BW,), ((0, 2),), -0.2, 0.2)), 0.3, 3.0),
        "v_scale": draw_v_scale(jax.random.fold_in(splits[20], 71), 0),
        "ln_gain": jnp.clip(1.0 + 0.18 * jax.random.normal(splits[14], (BW,), jnp.float32), 0.1, 1.9),
        "ln_bias": centred(splits[15], (BW,), 0.5, 3.0, ((0, 2),), jnp.float32),
        "spatial_weight": centred(splits[16], (GROUPS, SPAN, SPAN), (4 * SPAN) ** -0.5, 0.25, ((0, 2),)),
        "spatial_bias": jnp.clip(1.0 + 0.18 * jax.random.normal(splits[17], (GROUPS, SPAN), jnp.float32), 0.1, 1.9),
        "out_weight": centred(splits[18], (BW, D), BW ** -0.5, 0.1875, ((0, 2), (1, 32)), jnp.float32),
        "out_scale": jnp.clip(jnp.exp(math.log(3.0) - 2.3025851 * jax.random.uniform(splits[19], (D,), jnp.float32) ** steps_of(splits[19], (D,), ((0, 32),), -0.2, 0.2)), 0.3, 3.0),
    }


EPS = 1e-06

def rms_norm(rows, gain):
    values = rows.astype(jnp.float32)
    scale = lax.rsqrt(lax.optimization_barrier(jnp.mean(values * values, axis=1, keepdims=True)) + EPS)
    return (values * scale * gain).astype(jnp.bfloat16)

def project(left, weight, scale):
    return jnp.dot(left, weight.astype(jnp.bfloat16), preferred_element_type=jnp.float32) * scale

def block_sum(left, weight, scale):
    width = left.shape[1] // N_TP
    total = jnp.zeros((left.shape[0], weight.shape[1]), jnp.float32)
    for index in range(N_TP):
        partial_term = project(left[:, index * width:(index + 1) * width], weight[index * width:(index + 1) * width], scale)
        partial_term = lax.optimization_barrier(partial_term.astype(jnp.bfloat16))
        total = total + partial_term.astype(jnp.float32)
    return total

def feed_forward(normed, gate_weight, up_weight, down_weight, gate_scale, up_scale, down_scale):
    gate = project(normed, gate_weight, gate_scale)
    up_part = project(normed, up_weight, up_scale)
    hidden = (jax.nn.silu(gate) * up_part).astype(jnp.bfloat16)
    return block_sum(hidden, down_weight, down_scale)

def reference(tokens, norm_first, norm_mix, norm_second, gate_weight, up_weight, down_weight, gate_scale, up_scale, down_scale, u_weight, v_weight, u_scale, v_scale, ln_gain, ln_bias, spatial_weight, spatial_bias, out_weight, out_scale):
    first = feed_forward(rms_norm(tokens, norm_first), gate_weight, up_weight, down_weight, gate_scale, up_scale, down_scale)
    middle = (tokens.astype(jnp.float32) + 0.5 * first).astype(jnp.bfloat16)
    mix_normed = rms_norm(middle, norm_mix)
    u_pre = project(mix_normed, u_weight, u_scale)
    v_pre = project(mix_normed, v_weight, v_scale)
    v_act = jax.nn.gelu(v_pre, approximate=True)
    v_mean = lax.optimization_barrier(jnp.mean(v_act, axis=1, keepdims=True))
    v_var = lax.optimization_barrier(jnp.mean(v_act * v_act, axis=1, keepdims=True)) - v_mean * v_mean
    v_normed = ((v_act - v_mean) * lax.rsqrt(v_var + EPS) * ln_gain + ln_bias).astype(jnp.bfloat16)
    count = tokens.shape[0]
    groups = spatial_weight.shape[0]
    blocks = v_normed.reshape(count // SPAN, SPAN, groups, BW // groups).astype(jnp.float32)
    lower = jnp.tril(jnp.ones((SPAN, SPAN), jnp.float32))
    masked = (spatial_weight.astype(jnp.float32) * lower[None]).astype(jnp.float32)
    spatial = jnp.einsum('gts,nsgc->ntgc', masked, blocks) + spatial_bias.T[None, :, :, None]
    mixed = (jax.nn.gelu(u_pre, approximate=True) * spatial.reshape(count, BW)).astype(jnp.bfloat16)
    second = (middle.astype(jnp.float32) + block_sum(mixed, out_weight, out_scale)).astype(jnp.bfloat16)
    last = feed_forward(rms_norm(second, norm_second), gate_weight, up_weight, down_weight, gate_scale, up_scale, down_scale)
    return (second.astype(jnp.float32) + 0.5 * last).astype(jnp.bfloat16)
```

```python
import jax
import jax.numpy as jnp
from jax import lax
from jax.sharding import Mesh
from jax.sharding import PartitionSpec as P

BW = 1024
SPAN = 128
FS = ("fs_0", "fs_1", "fs_2")
REP_FS = ("rep", "fs_0", "fs_1", "fs_2")


EPS = 1e-06


def other_core(x):
    return lax.ppermute(x, "tp", [(0, 1), (1, 0)])


def on_device(
    tokens,
    norm_first,
    norm_mix,
    norm_second,
    gate_weight,
    up_weight,
    down_weight,
    gate_scale,
    up_scale,
    down_scale,
    u_weight,
    v_weight,
    u_scale,
    v_scale,
    ln_gain,
    ln_bias,
    spatial_weight,
    spatial_bias,
    out_weight,
    out_scale,
):
    count, half = tokens.shape
    units = gate_weight.shape[1]
    chans = u_weight.shape[1]
    first_core = lax.axis_index("tp") == 0

    low = jnp.bfloat16
    gate_low = (gate_weight * gate_scale).astype(low)
    up_low = (up_weight * up_scale).astype(low)
    down_low = (down_weight * down_scale).T.astype(low)
    u_low = (u_weight * u_scale).astype(low)
    v_low = (v_weight * v_scale).astype(low)
    out_low = (out_weight * out_scale).T.astype(low)
    pad = jnp.zeros((gate_low.shape[0], 3 * chans - units), low)
    mine = jnp.where(
        lax.axis_index("rep") == 0,
        jnp.concatenate([gate_low, down_low, pad], axis=1),
        jnp.concatenate([up_low, u_low, v_low, out_low], axis=1),
    )
    both = lax.all_gather(mine, REP_FS, axis=0, tiled=True)
    both = both.reshape(2, -1, both.shape[1])
    gate_all = both[0, :, :units]
    down_all = both[0, :, units : 2 * units]
    up_all = both[1, :, :units]
    u_all = both[1, :, units : units + chans]
    v_all = both[1, :, units + chans : units + 2 * chans]
    out_all = both[1, :, units + 2 * chans :]

    def full_norm(rows, gain):
        other = other_core(rows)
        whole = jnp.concatenate(
            [jnp.where(first_core, rows, other), jnp.where(first_core, other, rows)], axis=1
        )
        values = whole.astype(jnp.float32)
        factor = lax.rsqrt(jnp.mean(values * values, axis=1, keepdims=True) + EPS)
        return (values * factor * gain).astype(low)

    def spread_sum(term):
        term = term.astype(low)
        left, right = term[:, :half], term[:, half:]
        arrived = other_core(jnp.where(first_core, right, left))
        kept = jnp.where(first_core, left, right)
        return kept.astype(jnp.float32) + arrived.astype(jnp.float32)

    def times_rows(left, rows):
        return lax.dot_general(
            left, rows, (((1,), (1,)), ((), ())), preferred_element_type=jnp.float32
        )

    def feed_forward(normed):
        gate = jnp.dot(normed, gate_all, preferred_element_type=jnp.float32)
        up_part = jnp.dot(normed, up_all, preferred_element_type=jnp.float32)
        hidden = (jax.nn.silu(gate) * up_part).astype(low)
        return spread_sum(times_rows(hidden, down_all))

    first = feed_forward(full_norm(tokens, norm_first))
    middle = (tokens.astype(jnp.float32) + 0.5 * first).astype(low)
    mix_normed = full_norm(middle, norm_mix)
    u_pre = jnp.dot(mix_normed, u_all, preferred_element_type=jnp.float32)
    v_act = jax.nn.gelu(
        jnp.dot(mix_normed, v_all, preferred_element_type=jnp.float32), approximate=True
    )
    sums = jnp.stack([jnp.sum(v_act, axis=1), jnp.sum(v_act * v_act, axis=1)])
    totals = sums + other_core(sums)
    v_mean = (totals[0] / BW)[:, None]
    v_var = (totals[1] / BW)[:, None] - v_mean * v_mean
    v_normed = ((v_act - v_mean) * lax.rsqrt(v_var + EPS) * ln_gain + ln_bias).astype(low)
    local_groups = spatial_weight.shape[0]
    channels = chans // local_groups
    blocks = v_normed.reshape(count // SPAN, SPAN, local_groups, channels)
    lower = jnp.tril(jnp.ones((SPAN, SPAN), jnp.bool_))
    masked = jnp.where(lower[None], spatial_weight, jnp.zeros_like(spatial_weight))
    spatial = jnp.einsum("gts,nsgc->ntgc", masked, blocks, preferred_element_type=jnp.float32)
    spatial = spatial + spatial_bias.T[None, :, :, None]
    mixed = (jax.nn.gelu(u_pre, approximate=True) * spatial.reshape(count, chans)).astype(low)
    second = (middle.astype(jnp.float32) + spread_sum(times_rows(mixed, out_all))).astype(low)
    last = feed_forward(full_norm(second, norm_second))
    return (second.astype(jnp.float32) + 0.5 * last).astype(low)


def solution(mesh):
    torus = Mesh(
        mesh.devices.reshape(mesh.shape["rep"], 2, 4, 4, mesh.shape["tp"]),
        ("rep", "fs_0", "fs_1", "fs_2", "tp"),
    )
    in_specs = (
        P(REP_FS, "tp"),
        P(),
        P(),
        P(),
        P(FS, "tp"),
        P(FS, "tp"),
        P("tp", FS),
        P("tp"),
        P("tp"),
        P(FS),
        P(FS, "tp"),
        P(FS, "tp"),
        P("tp"),
        P("tp"),
        P("tp"),
        P("tp"),
        P("tp", None, None),
        P("tp", None),
        P("tp", FS),
        P(FS),
    )
    out_specs = P(REP_FS, "tp")
    return jax.shard_map(
        on_device, mesh=torus, in_specs=in_specs, out_specs=out_specs, check_vma=False
    )
```

```python
import functools

import jax
import jax.numpy as jnp
from jax import lax
from jax.experimental import pallas as pl
from jax.experimental.pallas import tpu as pltpu
from jax.sharding import Mesh
from jax.sharding import PartitionSpec as P

BW = 1024
SPAN = 128
FS = ("fs_0", "fs_1", "fs_2")
REP_FS = ("rep", "fs_0", "fs_1", "fs_2")
LANES = 128
WIDE = 256

EPS = 1e-06


def other_core(x):
    return lax.ppermute(x, "tp", [(0, 1), (1, 0)])


def normed_rows(values, gain):
    factor = lax.rsqrt(jnp.mean(values * values, axis=1, keepdims=True) + EPS)
    return (values * factor * gain).astype(jnp.bfloat16)


def dot(left, right):
    return jnp.dot(left, right, preferred_element_type=jnp.float32)


def dot_rows(left, rows):
    return lax.dot_general(
        left, rows, (((1,), (1,)), ((), ())), preferred_element_type=jnp.float32
    )


def gelu(a):
    return 0.5 * a * (1.0 + jnp.tanh(0.7978845608028654 * (a + 0.044715 * a * a * a)))


def hidden_tile(normed, gate, up):
    both = dot(normed, jnp.concatenate([gate, up], axis=1))
    gate_part, up_part = both[:, :LANES], both[:, LANES:]
    return (gate_part / (1.0 + jnp.exp(-gate_part)) * up_part).astype(jnp.bfloat16)


def spec(block, index):
    return pl.BlockSpec(block, index)


def whole(shape):
    return pl.BlockSpec(shape, lambda *_: (0,) * len(shape))


def params(steps):
    return pltpu.CompilerParams(
        dimension_semantics=("arbitrary",) * steps, vmem_limit_bytes=60 * 1024 * 1024
    )


def cost(flops, moved, special):
    return pl.CostEstimate(flops=flops, bytes_accessed=moved, transcendentals=special)


def first_kernel(tiles, core, own, other, gain, gate, up, down, term, normed, hidden):
    step = pl.program_id(0)

    @pl.when(step == 0)
    def _():
        left = jnp.where(core[0] == 0, own[...], other[...])
        right = jnp.where(core[0] == 0, other[...], own[...])
        values = jnp.concatenate([left, right], axis=1).astype(jnp.float32)
        normed[...] = normed_rows(values, gain[...])

    @pl.when(step < tiles)
    def _():
        hidden[step] = hidden_tile(normed[...], gate[0], up[0])

    @pl.when(step >= tiles)
    def _():
        units = jnp.concatenate([hidden[k] for k in range(tiles)], axis=1)
        term[...] = dot_rows(units, down[0]).astype(jnp.bfloat16)


def first_pass(core, own, other, gain, both):
    count, half = own.shape
    width = 2 * half
    units = both.shape[2] // 2 // LANES * LANES
    tiles, outs = units // LANES, width // WIDE
    shift = both.shape[2] // LANES - tiles
    return pl.pallas_call(
        functools.partial(first_kernel, tiles),
        out_shape=jax.ShapeDtypeStruct((count, width), jnp.bfloat16),
        grid_spec=pltpu.PrefetchScalarGridSpec(
            num_scalar_prefetch=1,
            grid=(tiles + outs,),
            in_specs=[
                whole((count, half)),
                whole((count, half)),
                whole((1, width)),
                spec((1, width, LANES), lambda j, c: (0, 0, jnp.minimum(j, tiles - 1))),
                spec((1, width, LANES), lambda j, c: (1, 0, shift + jnp.minimum(j, tiles - 1))),
                spec((1, WIDE, units), lambda j, c: (0, jnp.maximum(j - tiles, 0), 1)),
            ],
            out_specs=spec((count, WIDE), lambda j, c: (0, jnp.maximum(j - tiles, 0))),
            scratch_shapes=[
                pltpu.VMEM((count, width), jnp.bfloat16),
                pltpu.VMEM((tiles, count, LANES), jnp.bfloat16),
            ],
        ),
        compiler_params=params(1),
        cost_estimate=cost(6 * count * width * units, 6 * width * units, count * units),
        name="first_pass",
    )(core, own, other, gain, both, both, both)


def second_kernel(
    tiles, sent, core, middle, term, far, gain, gate, up, down, send, keep, base, normed, hidden
):
    step = pl.program_id(0)

    @pl.when(step == 0)
    def _():
        values = middle[...].astype(jnp.float32) + (
            term[...].astype(jnp.float32) + far[...].astype(jnp.float32)
        )
        second = values.astype(jnp.bfloat16)
        half = second.shape[1] // 2
        base[...] = jnp.where(core[0] == 0, second[:, :half], second[:, half:])
        normed[...] = normed_rows(second.astype(jnp.float32), gain[...])

    @pl.when(step < tiles)
    def _():
        hidden[step] = hidden_tile(normed[...], gate[0], up[0])

    @pl.when(step >= tiles)
    def _():
        units = jnp.concatenate([hidden[k] for k in range(tiles)], axis=1)
        part = dot_rows(units, down[0]).astype(jnp.bfloat16)

        @pl.when(step < tiles + sent)
        def _():
            send[...] = part

        @pl.when(step >= tiles + sent)
        def _():
            keep[...] = part


def second_pass(core, middle, term, far, gain, both):
    count, width = middle.shape
    half = width // 2
    units = both.shape[2] // 2 // LANES * LANES
    tiles, outs = units // LANES, width // WIDE
    sent = outs // 2
    shift = both.shape[2] // LANES - tiles

    def rows_of(j, c):
        n = jnp.maximum(j - tiles, 0)
        return jnp.where(n < sent, n + (1 - c[0]) * sent, n - sent + c[0] * sent)

    return pl.pallas_call(
        functools.partial(second_kernel, tiles, sent),
        out_shape=[jax.ShapeDtypeStruct((count, half), jnp.bfloat16)] * 3,
        grid_spec=pltpu.PrefetchScalarGridSpec(
            num_scalar_prefetch=1,
            grid=(tiles + outs,),
            in_specs=[
                whole((count, width)),
                whole((count, width)),
                whole((count, width)),
                whole((1, width)),
                spec((1, width, LANES), lambda j, c: (0, 0, jnp.minimum(j, tiles - 1))),
                spec((1, width, LANES), lambda j, c: (1, 0, shift + jnp.minimum(j, tiles - 1))),
                spec((1, WIDE, units), lambda j, c: (0, rows_of(j, c), 1)),
            ],
            out_specs=[
                spec((count, WIDE), lambda j, c: (0, jnp.clip(j - tiles, 0, sent - 1))),
                spec((count, WIDE), lambda j, c: (0, jnp.maximum(j - tiles - sent, 0))),
                whole((count, half)),
            ],
            scratch_shapes=[
                pltpu.VMEM((count, width), jnp.bfloat16),
                pltpu.VMEM((tiles, count, LANES), jnp.bfloat16),
            ],
        ),
        compiler_params=params(1),
        cost_estimate=cost(6 * count * width * units, 6 * width * units, count * units),
        name="second_pass",
    )(core, middle, term, far, gain, both, both, both)


def gates_kernel(core, own, other, term, far, gain, u_rows, v_rows, middle, u_out, v_out, sums):
    left = jnp.where(core[0] == 0, own[...], other[...])
    right = jnp.where(core[0] == 0, other[...], own[...])
    values = jnp.concatenate([left, right], axis=1).astype(jnp.float32)
    values = values + 0.5 * (term[...].astype(jnp.float32) + far[...].astype(jnp.float32))
    mid = values.astype(jnp.bfloat16)
    middle[...] = mid
    normed = normed_rows(mid.astype(jnp.float32), gain[...])
    v_act = gelu(dot(normed, v_rows[0]))
    v_out[...] = v_act
    lane = lax.broadcasted_iota(jnp.int32, sums.shape, 1)
    total = jnp.sum(v_act, axis=1, keepdims=True)
    squares = jnp.sum(v_act * v_act, axis=1, keepdims=True)
    sums[...] = jnp.where(lane == 0, total, squares)
    u_out[...] = gelu(dot(normed, u_rows[0]))


def gates(core, own, other, term, far, gain, both, chans):
    count, half = own.shape
    width = 2 * half
    rows = SPAN

    def block(columns):
        return spec((rows, columns), lambda i, c: (i, 0))

    return pl.pallas_call(
        gates_kernel,
        out_shape=[
            jax.ShapeDtypeStruct((count, width), jnp.bfloat16),
            jax.ShapeDtypeStruct((count, chans), jnp.float32),
            jax.ShapeDtypeStruct((count, chans), jnp.float32),
            jax.ShapeDtypeStruct((count, LANES), jnp.float32),
        ],
        grid_spec=pltpu.PrefetchScalarGridSpec(
            num_scalar_prefetch=1,
            grid=(count // rows,),
            in_specs=[
                block(half),
                block(half),
                block(width),
                block(width),
                whole((1, width)),
                spec((1, width, chans), lambda i, c: (1, 0, 0)),
                spec((1, width, chans), lambda i, c: (1, 0, 1)),
            ],
            out_specs=[block(width), block(chans), block(chans), block(LANES)],
        ),
        compiler_params=params(1),
        cost_estimate=cost(4 * count * width * chans, 4 * width * chans, 2 * count * chans),
        name="gates",
    )(core, own, other, term, far, gain, both, both)


def mix_kernel(u_act, v_act, sums, far, gain, bias, weight, shift, rows, term, masked):
    groups = weight.shape[0]

    @pl.when(pl.program_id(0) == 0)
    def _():
        at = lax.broadcasted_iota(jnp.int32, (SPAN, SPAN), 0)
        source = lax.broadcasted_iota(jnp.int32, (SPAN, SPAN), 1)
        for g in range(groups):
            masked[g] = jnp.where(source <= at, weight[g], jnp.zeros_like(weight[g]))

    totals = (sums[...] + far[...]) / BW
    v_mean = totals[:, 0:1]
    v_var = totals[:, 1:2] - v_mean * v_mean
    v_normed = (v_act[...] - v_mean) * lax.rsqrt(v_var + EPS) * gain[...] + bias[...]
    v_normed = v_normed.astype(jnp.bfloat16)
    wide = v_normed.shape[1] // groups
    spatial = [
        dot(masked[g], v_normed[:, g * wide : (g + 1) * wide]) + shift[:, g : g + 1]
        for g in range(groups)
    ]
    mixed = (u_act[...] * jnp.concatenate(spatial, axis=1)).astype(jnp.bfloat16)
    term[...] = dot_rows(mixed, rows[0]).astype(jnp.bfloat16)


def mix(u_act, v_act, sums, far, gain, bias, weight, shift, both):
    count, chans = u_act.shape
    width = both.shape[1]
    groups = weight.shape[0]

    def block(columns):
        return spec((SPAN, columns), lambda i: (i, 0))

    return pl.pallas_call(
        mix_kernel,
        out_shape=jax.ShapeDtypeStruct((count, width), jnp.bfloat16),
        grid=(count // SPAN,),
        in_specs=[
            block(chans),
            block(chans),
            block(LANES),
            block(LANES),
            whole((1, chans)),
            whole((1, chans)),
            whole((groups, SPAN, SPAN)),
            whole((SPAN, groups)),
            spec((1, width, chans), lambda i: (1, 0, 2)),
        ],
        out_specs=block(width),
        scratch_shapes=[pltpu.VMEM((groups, SPAN, SPAN), jnp.bfloat16)],
        compiler_params=params(1),
        cost_estimate=cost(2 * count * width * chans, 2 * width * chans, count),
        name="mix",
    )(u_act, v_act, sums, far, gain, bias, weight, shift, both)


def on_device(
    tokens,
    norm_first,
    norm_mix,
    norm_second,
    gate_weight,
    up_weight,
    down_weight,
    gate_scale,
    up_scale,
    down_scale,
    u_weight,
    v_weight,
    u_scale,
    v_scale,
    ln_gain,
    ln_bias,
    spatial_weight,
    spatial_bias,
    out_weight,
    out_scale,
):
    units = gate_weight.shape[1]
    chans = u_weight.shape[1]
    core = lax.axis_index("tp").reshape(1).astype(jnp.int32)

    low = jnp.bfloat16
    gate_low = (gate_weight * gate_scale).astype(low)
    up_low = (up_weight * up_scale).astype(low)
    down_low = (down_weight * down_scale).T.astype(low)
    u_low = (u_weight * u_scale).astype(low)
    v_low = (v_weight * v_scale).astype(low)
    out_low = (out_weight * out_scale).T.astype(low)
    pad = jnp.zeros((gate_low.shape[0], 3 * chans - units), low)
    mine = jnp.where(
        lax.axis_index("rep") == 0,
        jnp.concatenate([gate_low, down_low, pad], axis=1),
        jnp.concatenate([u_low, v_low, out_low, up_low], axis=1),
    )
    both = lax.all_gather(mine, REP_FS, axis=0, tiled=True)
    both = both.reshape(2, -1, both.shape[1])

    own, other = tokens, other_core(tokens)
    term = first_pass(core, own, other, norm_first[None], both)
    middle, u_act, v_act, sums = gates(
        core, own, other, term, other_core(term), norm_mix[None], both, chans
    )
    term = mix(
        u_act,
        v_act,
        sums,
        other_core(sums),
        ln_gain[None],
        ln_bias[None],
        spatial_weight,
        spatial_bias.T,
        both,
    )
    send, keep, base = second_pass(core, middle, term, other_core(term), norm_second[None], both)
    last = keep.astype(jnp.float32) + other_core(send).astype(jnp.float32)
    return (base.astype(jnp.float32) + 0.5 * last).astype(low)


def solution(mesh):
    torus = Mesh(
        mesh.devices.reshape(mesh.shape["rep"], 2, 4, 4, mesh.shape["tp"]),
        ("rep", "fs_0", "fs_1", "fs_2", "tp"),
    )
    in_specs = (
        P(REP_FS, "tp"),
        P(),
        P(),
        P(),
        P(FS, "tp"),
        P(FS, "tp"),
        P("tp", FS),
        P("tp"),
        P("tp"),
        P(FS),
        P(FS, "tp"),
        P(FS, "tp"),
        P("tp"),
        P("tp"),
        P("tp"),
        P("tp"),
        P("tp", None, None),
        P("tp", None),
        P("tp", FS),
        P(FS),
    )
    out_specs = P(REP_FS, "tp")
    return jax.shard_map(
        on_device, mesh=torus, in_specs=in_specs, out_specs=out_specs, check_vma=False
    )
```

```python
import functools

import jax
import jax.numpy as jnp
from jax import lax
from jax.experimental import pallas as pl
from jax.experimental.pallas import tpu as pltpu
from jax.sharding import Mesh
from jax.sharding import PartitionSpec as P

BW = 1024
SPAN = 128
FS = ("fs_0", "fs_1", "fs_2")
REP_FS = ("rep", "fs_0", "fs_1", "fs_2")
LANES = 128
WIDE = 512
HALF_ROWS = 32
FIRST = (4, 4, 4, 4, 3, 3)
OTHERS = (4, 4, 4, 3, 4, 4)
RINGS = (("fs_2", 1), ("fs_1", 1), ("z", 1), ("fs_2", 3), ("fs_1", 3), ("z", 3))
PLACES = (2, 8, 32, 6, 24, 33)

EPS = 1e-06


def other_core(x):
    return lax.ppermute(x, "tp", [(0, 1), (1, 0)])


def normed_rows(values, gain):
    factor = lax.rsqrt(jnp.mean(values * values, axis=1, keepdims=True) + EPS)
    return (values * factor * gain).astype(jnp.bfloat16)


def dot(left, right):
    return jnp.dot(left, right, preferred_element_type=jnp.float32)


def dot_rows(left, rows):
    return lax.dot_general(
        left, rows, (((1,), (1,)), ((), ())), preferred_element_type=jnp.float32
    )


def gelu(a):
    return 0.5 * a * (1.0 + jnp.tanh(0.7978845608028654 * (a + 0.044715 * a * a * a)))


def spec(block, index):
    return pl.BlockSpec(block, index)


def whole(shape):
    return pl.BlockSpec(shape, lambda *_: (0,) * len(shape))


ANY = pl.BlockSpec(memory_space=pl.ANY)


def params(steps):
    return pltpu.CompilerParams(
        dimension_semantics=("arbitrary",) * steps, vmem_limit_bytes=60 * 1024 * 1024
    )


def cost(flops, moved, special):
    return pl.CostEstimate(flops=flops, bytes_accessed=moved, transcendentals=special)


def exchange(x, color, turn):
    name, flip = RINGS[(color + turn) % 6]
    axis = ("rep", "fs_0") if name == "z" else name
    return lax.ppermute(x, axis, [(i, i ^ flip) for i in range(4)])


def place(color, slot):
    at = 0
    for turn in range(6):
        if slot >> turn & 1:
            at ^= PLACES[(color + turn) % 6]
    return at


def starts(widths):
    ends = [0]
    for n in widths:
        ends.append(ends[-1] + n * LANES)
    return ends


PAIRS = [(p, t + k) for t in (0, 2, 4, 6) for p in (0, 1) for k in (0, 1)]
PAIRS += [(0, 8), (0, 9), (1, 8), (1, 9), (0, 10), (1, 10)]


def prepare_kernel(
    rep, gate, up, down, u, v, out, gate_s, up_s, down_s, u_s, v_s, out_s, *colors
):
    rows = pl.ds(pl.multiple_of(rep[0] * HALF_ROWS, HALF_ROWS), HALF_ROWS)
    low = jnp.bfloat16
    pair = ((gate[rows, :] * gate_s[...]).astype(low), (up[rows, :] * up_s[...]).astype(low))
    firsts = [pair[p][:, t * LANES : (t + 1) * LANES] for p, t in PAIRS]
    rest = jnp.concatenate(
        [
            (out[rows, :] * out_s[rows, :]).astype(low),
            (u[rows, :] * u_s[...]).astype(low),
            (v[rows, :] * v_s[...]).astype(low),
            (down[rows, :] * down_s[rows, :]).astype(low),
        ],
        axis=1,
    )
    at, begin = 0, starts(OTHERS)
    for c, ref in enumerate(colors):
        mine = firsts[at : at + FIRST[c]] + [rest[:, begin[c] : begin[c + 1]]]
        ref[...] = jnp.concatenate(mine, axis=1)
        at += FIRST[c]


def prepare(rep, *arrays):
    return pl.pallas_call(
        prepare_kernel,
        out_shape=[
            jax.ShapeDtypeStruct((HALF_ROWS, (a + b) * LANES), jnp.bfloat16)
            for a, b in zip(FIRST, OTHERS)
        ],
        grid_spec=pltpu.PrefetchScalarGridSpec(
            num_scalar_prefetch=1,
            grid=(1,),
            in_specs=[whole(a.shape) for a in arrays],
            out_specs=[whole((HALF_ROWS, (a + b) * LANES)) for a, b in zip(FIRST, OTHERS)],
        ),
        compiler_params=params(1),
        name="prepare",
    )(rep, *arrays)


def gather(colors):
    held = list(colors)
    for turn in range(4):
        arrived = [exchange(x, c, turn) for c, x in enumerate(held)]
        held = [jnp.concatenate([x, y], axis=0) for x, y in zip(held, arrived)]
    one = [x[:, : FIRST[c] * LANES] for c, x in enumerate(held)]
    two = [x[:, FIRST[c] * LANES :] for c, x in enumerate(held)]
    groups = []
    for group in (one, two):
        if groups:
            group, _ = lax.optimization_barrier((group, groups[0][1]))
        fourth = [exchange(x, c, 4) for c, x in enumerate(group)]
        fifth = [exchange(x, c, 5) for c, x in enumerate(group)]
        last = [exchange(x, c, 5) for c, x in enumerate(fourth)]
        groups.append((group, fourth, fifth, last))
    return [[piece[c] for c in range(6) for piece in g] for g in groups]


def place_blocks(at, pieces, weight, sems, widths, colors):
    begin = starts(widths)
    for c in colors:
        columns = pl.ds(begin[c], widths[c] * LANES)
        for k in range(4):
            for slot in range(16):
                to = (at ^ place(c, slot + 16 * k)) * HALF_ROWS
                pltpu.make_async_copy(
                    pieces[4 * c + k].at[pl.ds(slot * HALF_ROWS, HALF_ROWS), :],
                    weight.at[pl.ds(pl.multiple_of(to, HALF_ROWS), HALF_ROWS), columns],
                    sems.at[c],
                ).start()


def wait_color(weight, sems, widths, c):
    columns = pl.ds(starts(widths)[c], widths[c] * LANES)
    part = weight.at[:, columns]
    pltpu.make_async_copy(part, part, sems.at[c]).wait()


def silu_product(gate, up):
    return (gate / (1.0 + jnp.exp(-gate)) * up).astype(jnp.bfloat16)


def narrow_step(normed, weight):
    both = dot(normed, weight)
    tile = [both[:, k * LANES : (k + 1) * LANES] for k in range(6)]
    gate = jnp.concatenate([tile[0], tile[1], tile[4]], axis=1)
    up = jnp.concatenate([tile[2], tile[3], tile[5]], axis=1)
    return silu_product(gate, up)


def hidden_step(step, normed, weight, hidden):
    @pl.when(step < 4)
    def _():
        columns = pl.ds(pl.multiple_of(step * WIDE, WIDE), WIDE)
        both = dot(normed[...], weight[:, columns])
        to = pl.ds(pl.multiple_of(step * (WIDE // 2), WIDE // 2), WIDE // 2)
        hidden[:, to] = silu_product(both[:, : WIDE // 2], both[:, WIDE // 2 :])

    @pl.when(step == 4)
    def _():
        hidden[:, 2 * WIDE :] = narrow_step(normed[...], weight[:, 4 * WIDE :])


def first_kernel(core, at, own, other, gain, *rest):
    pieces, (hidden, kept, weight, normed, sems, out_sem) = rest[:24], rest[24:]
    step = pl.program_id(0)

    @pl.when(step == 0)
    def _():
        place_blocks(at[0], pieces, weight, sems, FIRST, range(6))
        left = jnp.where(core[0] == 0, own[...], other[...])
        right = jnp.where(core[0] == 0, other[...], own[...])
        values = jnp.concatenate([left, right], axis=1).astype(jnp.float32)
        normed[...] = normed_rows(values, gain[...])

    for c in range(6):

        @pl.when(step == min(c, 4))
        def _():
            wait_color(weight, sems, FIRST, c)

    hidden_step(step, normed, weight, hidden)

    @pl.when(step == 4)
    def _():
        copy = pltpu.make_async_copy(weight, kept, out_sem)
        copy.start()
        copy.wait()


def first_hidden(core, at, own, other, gain, pieces):
    count, half = own.shape
    width = 2 * half
    columns = sum(FIRST) * LANES
    units = columns // 2
    return pl.pallas_call(
        first_kernel,
        out_shape=[
            jax.ShapeDtypeStruct((count, units), jnp.bfloat16),
            jax.ShapeDtypeStruct((width, columns), jnp.bfloat16),
        ],
        grid_spec=pltpu.PrefetchScalarGridSpec(
            num_scalar_prefetch=2,
            grid=(5,),
            in_specs=[whole((count, half)), whole((count, half)), whole((1, width))] + [ANY] * 24,
            out_specs=[whole((count, units)), ANY],
            scratch_shapes=[
                pltpu.VMEM((width, columns), jnp.bfloat16),
                pltpu.VMEM((count, width), jnp.bfloat16),
                pltpu.SemaphoreType.DMA((6,)),
                pltpu.SemaphoreType.DMA,
            ],
        ),
        compiler_params=params(1),
        cost_estimate=cost(2 * count * width * columns, 4 * width * columns, count * units),
        name="first_hidden",
    )(core, at, own, other, gain, *pieces)


def down_kernel(at, hidden, *rest):
    pieces, (term, kept, weight, sems, out_sem) = rest[:24], rest[24:]
    step = pl.program_id(0)
    begin = starts(OTHERS)
    copy = pltpu.make_async_copy(weight, kept, out_sem)

    @pl.when(step == 0)
    def _():
        place_blocks(at[0], pieces, weight, sems, OTHERS, (3, 4, 5, 0, 1, 2))
        for c in (3, 4, 5):
            wait_color(weight, sems, OTHERS, c)

    rows = pl.ds(pl.multiple_of(step * WIDE, WIDE), WIDE)
    term[...] = dot_rows(hidden[...], weight[rows, begin[3] :]).astype(jnp.bfloat16)

    @pl.when(step == 0)
    def _():
        for c in (0, 1, 2):
            wait_color(weight, sems, OTHERS, c)
        copy.start()

    @pl.when(step == pl.num_programs(0) - 1)
    def _():
        copy.wait()


def first_down(at, hidden, width, pieces):
    count, units = hidden.shape
    columns = sum(OTHERS) * LANES
    return pl.pallas_call(
        down_kernel,
        out_shape=[
            jax.ShapeDtypeStruct((count, width), jnp.bfloat16),
            jax.ShapeDtypeStruct((width, columns), jnp.bfloat16),
        ],
        grid_spec=pltpu.PrefetchScalarGridSpec(
            num_scalar_prefetch=1,
            grid=(width // WIDE,),
            in_specs=[whole((count, units))] + [ANY] * 24,
            out_specs=[spec((count, WIDE), lambda j, a: (0, j)), ANY],
            scratch_shapes=[
                pltpu.VMEM((width, columns), jnp.bfloat16),
                pltpu.SemaphoreType.DMA((6,)),
                pltpu.SemaphoreType.DMA,
            ],
        ),
        compiler_params=params(1),
        cost_estimate=cost(2 * count * width * units, 4 * width * columns, 0),
        name="first_down",
    )(at, hidden, *pieces)


def gates_kernel(core, own, other, term, far, gain, rows, middle, act, sums, normed):
    @pl.when(pl.program_id(0) == 0)
    def _():
        left = jnp.where(core[0] == 0, own[...], other[...])
        right = jnp.where(core[0] == 0, other[...], own[...])
        values = jnp.concatenate([left, right], axis=1).astype(jnp.float32)
        values = values + 0.5 * (term[...].astype(jnp.float32) + far[...].astype(jnp.float32))
        mid = values.astype(jnp.bfloat16)
        middle[...] = mid
        normed[...] = normed_rows(mid.astype(jnp.float32), gain[...])

    acted = gelu(dot(normed[...], rows[...]))
    act[0] = acted

    @pl.when(pl.program_id(0) == 0)
    def _():
        lane = lax.broadcasted_iota(jnp.int32, sums.shape, 1)
        total = jnp.sum(acted, axis=1, keepdims=True)
        squares = jnp.sum(acted * acted, axis=1, keepdims=True)
        sums[...] = jnp.where(lane == 0, total, squares)


def gates(core, own, other, term, far, gain, weight, chans):
    count, half = own.shape
    width = 2 * half
    return pl.pallas_call(
        gates_kernel,
        out_shape=[
            jax.ShapeDtypeStruct((count, width), jnp.bfloat16),
            jax.ShapeDtypeStruct((2, count, chans), jnp.float32),
            jax.ShapeDtypeStruct((count, LANES), jnp.float32),
        ],
        grid_spec=pltpu.PrefetchScalarGridSpec(
            num_scalar_prefetch=1,
            grid=(2,),
            in_specs=[
                whole((count, half)),
                whole((count, half)),
                whole((count, width)),
                whole((count, width)),
                whole((1, width)),
                spec((width, chans), lambda i, c: (0, 2 - i)),
            ],
            out_specs=[
                whole((count, width)),
                spec((1, count, chans), lambda i, c: (i, 0, 0)),
                whole((count, LANES)),
            ],
            scratch_shapes=[pltpu.VMEM((count, width), jnp.bfloat16)],
        ),
        compiler_params=params(1),
        cost_estimate=cost(4 * count * width * chans, 4 * width * chans, 2 * count * chans),
        name="gates",
    )(core, own, other, term, far, gain, weight)


def mix_kernel(act, sums, far, gain, bias, weight, shift, rows, term, mixed):
    groups = weight.shape[0]

    @pl.when(pl.program_id(0) == 0)
    def _():
        at = lax.broadcasted_iota(jnp.int32, (SPAN, SPAN), 0)
        source = lax.broadcasted_iota(jnp.int32, (SPAN, SPAN), 1)
        masked = [
            jnp.where(source <= at, weight[g], jnp.zeros_like(weight[g])) for g in range(groups)
        ]
        count, chans = mixed.shape
        wide = chans // groups
        for n in range(count // SPAN):
            block = pl.ds(n * SPAN, SPAN)
            totals = (sums[block, :] + far[block, :]) / BW
            v_mean = totals[:, 0:1]
            v_var = totals[:, 1:2] - v_mean * v_mean
            v_normed = (act[0, block, :] - v_mean) * lax.rsqrt(v_var + EPS) * gain[...] + bias[...]
            v_normed = v_normed.astype(jnp.bfloat16)
            spatial = [
                dot(masked[g], v_normed[:, g * wide : (g + 1) * wide]) + shift[:, g : g + 1]
                for g in range(groups)
            ]
            product = act[1, block, :] * jnp.concatenate(spatial, axis=1)
            mixed[block, :] = product.astype(jnp.bfloat16)

    term[...] = dot_rows(mixed[...], rows[...]).astype(jnp.bfloat16)


def mix(act, sums, far, gain, bias, weight, shift, rows):
    _, count, chans = act.shape
    width = rows.shape[0]
    groups = weight.shape[0]
    return pl.pallas_call(
        mix_kernel,
        out_shape=jax.ShapeDtypeStruct((count, width), jnp.bfloat16),
        grid=(width // WIDE,),
        in_specs=[
            whole(act.shape),
            whole((count, LANES)),
            whole((count, LANES)),
            whole((1, chans)),
            whole((1, chans)),
            whole((groups, SPAN, SPAN)),
            whole((SPAN, groups)),
            spec((WIDE, chans), lambda j: (j, 0)),
        ],
        out_specs=spec((count, WIDE), lambda j: (0, j)),
        scratch_shapes=[pltpu.VMEM((count, chans), jnp.bfloat16)],
        compiler_params=params(1),
        cost_estimate=cost(2 * count * width * chans, 2 * width * chans, count),
        name="mix",
    )(act, sums, far, gain, bias, weight, shift, rows)


def second_kernel(
    core, middle, term, far, gain, first, others, send, keep, base, normed, hidden, wide, down, sems
):
    step = pl.program_id(0)
    steps = 5
    outs = down.shape[0] // WIDE
    begin = starts(OTHERS)[3]
    cuts = [pl.ds(k * WIDE, WIDE) for k in range(4)] + [pl.ds(4 * WIDE, 6 * LANES)]
    copies = [
        pltpu.make_async_copy(first.at[:, cut], wide.at[:, cut], sems.at[k])
        for k, cut in enumerate(cuts)
    ]
    copies.append(
        pltpu.make_async_copy(others.at[:, pl.ds(begin, down.shape[1])], down, sems.at[steps])
    )

    @pl.when(step == 0)
    def _():
        for copy in copies:
            copy.start()
        values = middle[...].astype(jnp.float32) + (
            term[...].astype(jnp.float32) + far[...].astype(jnp.float32)
        )
        second = values.astype(jnp.bfloat16)
        half = second.shape[1] // 2
        base[...] = jnp.where(core[0] == 0, second[:, :half], second[:, half:])
        normed[...] = normed_rows(second.astype(jnp.float32), gain[...])

    for k, copy in enumerate(copies):

        @pl.when(step == k)
        def _():
            copy.wait()

    hidden_step(step, normed, wide, hidden)

    @pl.when(step >= steps)
    def _():
        n = step - steps
        mine = jnp.where(n < outs // 2, 1 - core[0], core[0])
        row = mine * (outs // 2) + lax.rem(n, outs // 2)
        rows = pl.ds(pl.multiple_of(row * WIDE, WIDE), WIDE)
        part = dot_rows(hidden[...], down[rows, :]).astype(jnp.bfloat16)

        @pl.when(n < outs // 2)
        def _():
            send[...] = part

        @pl.when(n >= outs // 2)
        def _():
            keep[...] = part


def second_pass(core, middle, term, far, gain, first, others):
    count, width = middle.shape
    half = width // 2
    columns = first.shape[1]
    units = columns // 2
    outs = width // WIDE
    sent = outs // 2
    return pl.pallas_call(
        second_kernel,
        out_shape=[jax.ShapeDtypeStruct((count, half), jnp.bfloat16)] * 3,
        grid_spec=pltpu.PrefetchScalarGridSpec(
            num_scalar_prefetch=1,
            grid=(5 + outs,),
            in_specs=[
                whole((count, width)),
                whole((count, width)),
                whole((count, width)),
                whole((1, width)),
                ANY,
                ANY,
            ],
            out_specs=[
                spec((count, WIDE), lambda j, c: (0, jnp.clip(j - 5, 0, sent - 1))),
                spec((count, WIDE), lambda j, c: (0, jnp.maximum(j - 5 - sent, 0))),
                whole((count, half)),
            ],
            scratch_shapes=[
                pltpu.VMEM((count, width), jnp.bfloat16),
                pltpu.VMEM((count, units), jnp.bfloat16),
                pltpu.VMEM((width, columns), jnp.bfloat16),
                pltpu.VMEM((width, units), jnp.bfloat16),
                pltpu.SemaphoreType.DMA((6,)),
            ],
        ),
        compiler_params=params(1),
        cost_estimate=cost(6 * count * width * units, 6 * width * units, count * units),
        name="second_pass",
    )(core, middle, term, far, gain, first, others)


def on_device(
    tokens,
    norm_first,
    norm_mix,
    norm_second,
    gate_weight,
    up_weight,
    down_weight,
    gate_scale,
    up_scale,
    down_scale,
    u_weight,
    v_weight,
    u_scale,
    v_scale,
    ln_gain,
    ln_bias,
    spatial_weight,
    spatial_bias,
    out_weight,
    out_scale,
):
    chans = u_weight.shape[1]
    width = 2 * tokens.shape[1]

    def number(x):
        return x.reshape(1).astype(jnp.int32)

    core = number(lax.axis_index("tp"))
    rep = lax.axis_index("rep")
    at = number(2 * lax.axis_index(FS) + rep)

    colors = prepare(
        number(rep),
        gate_weight,
        up_weight,
        down_weight.T,
        u_weight,
        v_weight,
        out_weight.T,
        gate_scale[None],
        up_scale[None],
        down_scale[:, None],
        u_scale[None],
        v_scale[None],
        out_scale[:, None],
    )
    one, two = gather(colors)

    own, other = tokens, other_core(tokens)
    hidden, first = first_hidden(core, at, own, other, norm_first[None], one)
    term, others = first_down(at, hidden, width, two)
    middle, act, sums = gates(
        core, own, other, term, other_core(term), norm_mix[None], others, chans
    )
    term = mix(
        act,
        sums,
        other_core(sums),
        ln_gain[None],
        ln_bias[None],
        spatial_weight,
        spatial_bias.T,
        others,
    )
    send, keep, base = second_pass(
        core, middle, term, other_core(term), norm_second[None], first, others
    )
    last = keep.astype(jnp.float32) + other_core(send).astype(jnp.float32)
    return (base.astype(jnp.float32) + 0.5 * last).astype(jnp.bfloat16)


def solution(mesh):
    torus = Mesh(
        mesh.devices.reshape(mesh.shape["rep"], 2, 4, 4, mesh.shape["tp"]),
        ("rep", "fs_0", "fs_1", "fs_2", "tp"),
    )
    in_specs = (
        P(REP_FS, "tp"),
        P(),
        P(),
        P(),
        P(FS, "tp"),
        P(FS, "tp"),
        P("tp", FS),
        P("tp"),
        P("tp"),
        P(FS),
        P(FS, "tp"),
        P(FS, "tp"),
        P("tp"),
        P("tp"),
        P("tp"),
        P("tp"),
        P("tp", None, None),
        P("tp", None),
        P("tp", FS),
        P(FS),
    )
    out_specs = P(REP_FS, "tp")
    return jax.shard_map(
        on_device, mesh=torus, in_specs=in_specs, out_specs=out_specs, check_vma=False
    )
```

```python
import functools

import jax
import jax.numpy as jnp
from jax import lax
from jax.experimental import pallas as pl
from jax.experimental.pallas import tpu as pltpu
from jax.sharding import Mesh
from jax.sharding import PartitionSpec as P


BW = 1024
SPAN = 128
FS = ("fs_0", "fs_1", "fs_2")
REP_FS = ("rep", "fs_0", "fs_1", "fs_2")
LANES = 128
WIDE = 512
HALF_ROWS = 32
FIRST = (4, 4, 4, 4, 3, 3)
OTHERS = (4, 4, 4, 3, 4, 4)
RINGS = (("fs_2", 1), ("fs_1", 1), ("z", 1), ("fs_2", 3), ("fs_1", 3), ("z", 3))
PLACES = (2, 8, 32, 6, 24, 33)

EPS = 1e-06


def other_core(x):
    return lax.ppermute(x, "tp", [(0, 1), (1, 0)])


def normed_rows(values, gain):
    factor = lax.rsqrt(jnp.mean(values * values, axis=1, keepdims=True) + EPS)
    return (values * factor * gain).astype(jnp.bfloat16)


def dot(left, right):
    return jnp.dot(left, right, preferred_element_type=jnp.float32)


def dot_rows(left, rows):
    return lax.dot_general(
        left, rows, (((1,), (1,)), ((), ())), preferred_element_type=jnp.float32
    )


def gelu(a):
    return 0.5 * a * (1.0 + jnp.tanh(0.7978845608028654 * (a + 0.044715 * a * a * a)))


def spec(block, index):
    return pl.BlockSpec(block, index)


def whole(shape):
    return pl.BlockSpec(shape, lambda *_: (0,) * len(shape))


ANY = pl.BlockSpec(memory_space=pl.ANY)


def params(steps):
    return pltpu.CompilerParams(
        dimension_semantics=("arbitrary",) * steps, vmem_limit_bytes=60 * 1024 * 1024
    )


def cost(flops, moved, special):
    return pl.CostEstimate(flops=flops, bytes_accessed=moved, transcendentals=special)


def exchange(x, color, turn):
    name, flip = RINGS[(color + turn) % 6]
    axis = ("rep", "fs_0") if name == "z" else name
    return lax.ppermute(x, axis, [(i, i ^ flip) for i in range(4)])


def place(color, slot):
    at = 0
    for turn in range(6):
        if slot >> turn & 1:
            at ^= PLACES[(color + turn) % 6]
    return at


def starts(widths):
    ends = [0]
    for n in widths:
        ends.append(ends[-1] + n * LANES)
    return ends


PAIRS = [(p, t + k) for t in (0, 2, 4, 6) for p in (0, 1) for k in (0, 1)]
PAIRS += [(0, 8), (0, 9), (1, 8), (1, 9), (0, 10), (1, 10)]


def prepare_kernel(
    rep, gate, up, down, u, v, out, gate_s, up_s, down_s, u_s, v_s, out_s, *colors
):
    rows = pl.ds(pl.multiple_of(rep[0] * HALF_ROWS, HALF_ROWS), HALF_ROWS)
    low = jnp.bfloat16

    def across(scale):
        return scale[...][None, :]

    def down_rows(scale):
        size = scale.shape[0]
        row = lax.broadcasted_iota(jnp.int32, (HALF_ROWS, size), 0) + rep[0] * HALF_ROWS
        column = lax.broadcasted_iota(jnp.int32, (HALF_ROWS, size), 1)
        return jnp.sum(jnp.where(row == column, across(scale), 0.0), axis=1, keepdims=True)

    pair = ((gate[rows, :] * across(gate_s)).astype(low), (up[rows, :] * across(up_s)).astype(low))
    firsts = [pair[p][:, t * LANES : (t + 1) * LANES] for p, t in PAIRS]
    rest = jnp.concatenate(
        [
            (out[rows, :] * down_rows(out_s)).astype(low),
            (u[rows, :] * across(u_s)).astype(low),
            (v[rows, :] * across(v_s)).astype(low),
            (down[rows, :] * down_rows(down_s)).astype(low),
        ],
        axis=1,
    )
    at, begin = 0, starts(OTHERS)
    for c, ref in enumerate(colors):
        mine = firsts[at : at + FIRST[c]] + [rest[:, begin[c] : begin[c + 1]]]
        ref[...] = jnp.concatenate(mine, axis=1)
        at += FIRST[c]


def prepare(rep, *arrays):
    return pl.pallas_call(
        prepare_kernel,
        out_shape=[
            jax.ShapeDtypeStruct((HALF_ROWS, (a + b) * LANES), jnp.bfloat16)
            for a, b in zip(FIRST, OTHERS)
        ],
        grid_spec=pltpu.PrefetchScalarGridSpec(
            num_scalar_prefetch=1,
            grid=(1,),
            in_specs=[whole(a.shape) for a in arrays],
            out_specs=[whole((HALF_ROWS, (a + b) * LANES)) for a, b in zip(FIRST, OTHERS)],
        ),
        compiler_params=params(1),
        name="prepare",
    )(rep, *arrays)


VMEM = pl.BlockSpec(memory_space=pltpu.VMEM)


def join_kernel(cuts, *refs):
    held, arrived, joined = refs[:6], refs[6:12], refs[12:]
    for c in range(6):
        begin, end = cuts[c]
        rows = held[c].shape[0]
        joined[c][pl.ds(0, rows), :] = held[c][:, begin:end]
        joined[c][pl.ds(rows, rows), :] = arrived[c][:, begin:end]


def join(held, arrived, cuts=None):
    rows, low = held[0].shape[0], jnp.bfloat16
    if cuts is None:
        cuts = [(0, x.shape[1]) for x in held]
    return pl.pallas_call(
        functools.partial(join_kernel, cuts),
        out_shape=[jax.ShapeDtypeStruct((2 * rows, b - a), low) for a, b in cuts],
        in_specs=[VMEM] * 12,
        out_specs=[VMEM] * 6,
        compiler_params=pltpu.CompilerParams(vmem_limit_bytes=32 * 1024 * 1024),
        name="join",
    )(*held, *arrived)


def gather(colors):
    held = list(colors)
    for turn in range(5):
        arrived = [exchange(x, c, turn) for c, x in enumerate(held)]
        if turn < 4:
            held = join(held, arrived)
    groups = []
    for g in range(2):
        edge = [n * LANES for n in FIRST]
        cuts = [(e, x.shape[1]) if g else (0, e) for e, x in zip(edge, held)]
        group = join(held, arrived, cuts)
        last = []
        for c, x in enumerate(group):
            last.append(exchange(x, c, 5))
        groups.append([piece[c] for c in range(6) for piece in (group, last)])
    return groups


def place_blocks(at, pieces, weight, sems, widths, colors):
    begin = starts(widths)
    for c in colors:
        columns = pl.ds(begin[c], widths[c] * LANES)
        for k in range(2):

            def copy_four(high, carry, c=c, k=k, columns=columns):
                moved = at ^ place(c, 32 * k)
                for bit in range(3):
                    moved = moved ^ ((high >> bit & 1) * place(c, 4 << bit))
                for low in range(4):
                    to = (moved ^ place(c, low)) * HALF_ROWS
                    origin = (high * 4 + low) * HALF_ROWS
                    pltpu.make_async_copy(
                        pieces[2 * c + k].at[
                            pl.ds(pl.multiple_of(origin, HALF_ROWS), HALF_ROWS), :
                        ],
                        weight.at[pl.ds(pl.multiple_of(to, HALF_ROWS), HALF_ROWS), columns],
                        sems.at[c],
                    ).start()
                return carry

            lax.fori_loop(0, 8, copy_four, 0)


def wait_color(weight, sems, widths, c):
    columns = pl.ds(starts(widths)[c], widths[c] * LANES)
    part = weight.at[:, columns]
    pltpu.make_async_copy(part, part, sems.at[c]).wait()


def silu_product(gate, up):
    return (gate / (1.0 + jnp.exp(-gate)) * up).astype(jnp.bfloat16)


def narrow_step(normed, weight):
    both = dot(normed, weight)
    tile = [both[:, k * LANES : (k + 1) * LANES] for k in range(6)]
    gate = jnp.concatenate([tile[0], tile[1], tile[4]], axis=1)
    up = jnp.concatenate([tile[2], tile[3], tile[5]], axis=1)
    return silu_product(gate, up)


def hidden_step(step, normed, weight, hidden):
    @pl.when(step < 4)
    def _():
        columns = pl.ds(pl.multiple_of(step * WIDE, WIDE), WIDE)
        both = dot(normed[...], weight[:, columns])
        to = pl.ds(pl.multiple_of(step * (WIDE // 2), WIDE // 2), WIDE // 2)
        hidden[:, to] = silu_product(both[:, : WIDE // 2], both[:, WIDE // 2 :])

    @pl.when(step == 4)
    def _():
        hidden[:, 2 * WIDE :] = narrow_step(normed[...], weight[:, 4 * WIDE :])


def first_kernel(core, at, own, other, gain, *rest):
    pieces, (hidden, kept, weight, normed, sems, out_sem) = rest[:12], rest[12:]
    step = pl.program_id(0)

    @pl.when(step == 0)
    def _():
        place_blocks(at[0], pieces, weight, sems, FIRST, range(6))
        left = jnp.where(core[0] == 0, own[...], other[...])
        right = jnp.where(core[0] == 0, other[...], own[...])
        values = jnp.concatenate([left, right], axis=1).astype(jnp.float32)
        normed[...] = normed_rows(values, gain[...])

    for c in range(6):

        @pl.when(step == min(c, 4))
        def _():
            wait_color(weight, sems, FIRST, c)

    hidden_step(step, normed, weight, hidden)

    @pl.when(step == 4)
    def _():
        copy = pltpu.make_async_copy(weight, kept, out_sem)
        copy.start()
        copy.wait()


def first_hidden(core, at, own, other, gain, pieces):
    count, half = own.shape
    width = 2 * half
    columns = sum(FIRST) * LANES
    units = columns // 2
    return pl.pallas_call(
        first_kernel,
        out_shape=[
            jax.ShapeDtypeStruct((count, units), jnp.bfloat16),
            jax.ShapeDtypeStruct((width, columns), jnp.bfloat16),
        ],
        grid_spec=pltpu.PrefetchScalarGridSpec(
            num_scalar_prefetch=2,
            grid=(5,),
            in_specs=[whole((count, half)), whole((count, half)), whole((1, width))] + [ANY] * 12,
            out_specs=[whole((count, units)), ANY],
            scratch_shapes=[
                pltpu.VMEM((width, columns), jnp.bfloat16),
                pltpu.VMEM((count, width), jnp.bfloat16),
                pltpu.SemaphoreType.DMA((6,)),
                pltpu.SemaphoreType.DMA,
            ],
        ),
        compiler_params=params(1),
        cost_estimate=cost(2 * count * width * columns, 4 * width * columns, count * units),
        name="first_hidden",
    )(core, at, own, other, gain, *pieces)


def down_kernel(at, hidden, *rest):
    pieces, (term, kept, weight, sems, out_sem) = rest[:12], rest[12:]
    step = pl.program_id(0)
    begin = starts(OTHERS)
    copy = pltpu.make_async_copy(weight, kept, out_sem)

    @pl.when(step == 0)
    def _():
        place_blocks(at[0], pieces, weight, sems, OTHERS, (3, 4, 5, 0, 1, 2))
        for c in (3, 4, 5):
            wait_color(weight, sems, OTHERS, c)

    rows = pl.ds(pl.multiple_of(step * WIDE, WIDE), WIDE)
    term[...] = dot_rows(hidden[...], weight[rows, begin[3] :]).astype(jnp.bfloat16)

    @pl.when(step == 0)
    def _():
        for c in (0, 1, 2):
            wait_color(weight, sems, OTHERS, c)
        copy.start()

    @pl.when(step == pl.num_programs(0) - 1)
    def _():
        copy.wait()


def first_down(at, hidden, width, pieces):
    count, units = hidden.shape
    columns = sum(OTHERS) * LANES
    return pl.pallas_call(
        down_kernel,
        out_shape=[
            jax.ShapeDtypeStruct((count, width), jnp.bfloat16),
            jax.ShapeDtypeStruct((width, columns), jnp.bfloat16),
        ],
        grid_spec=pltpu.PrefetchScalarGridSpec(
            num_scalar_prefetch=1,
            grid=(width // WIDE,),
            in_specs=[whole((count, units))] + [ANY] * 12,
            out_specs=[spec((count, WIDE), lambda j, a: (0, j)), ANY],
            scratch_shapes=[
                pltpu.VMEM((width, columns), jnp.bfloat16),
                pltpu.SemaphoreType.DMA((6,)),
                pltpu.SemaphoreType.DMA,
            ],
        ),
        compiler_params=params(1),
        cost_estimate=cost(2 * count * width * units, 4 * width * columns, 0),
        name="first_down",
    )(at, hidden, *pieces)


def gates_kernel(core, own, other, term, far, gain, rows, middle, act, sums, normed):
    @pl.when(pl.program_id(0) == 0)
    def _():
        left = jnp.where(core[0] == 0, own[...], other[...])
        right = jnp.where(core[0] == 0, other[...], own[...])
        values = jnp.concatenate([left, right], axis=1).astype(jnp.float32)
        values = values + 0.5 * (term[...].astype(jnp.float32) + far[...].astype(jnp.float32))
        mid = values.astype(jnp.bfloat16)
        middle[...] = mid
        normed[...] = normed_rows(mid.astype(jnp.float32), gain[...])

    acted = gelu(dot(normed[...], rows[...]))
    act[0] = acted

    @pl.when(pl.program_id(0) == 0)
    def _():
        lane = lax.broadcasted_iota(jnp.int32, sums.shape, 1)
        total = jnp.sum(acted, axis=1, keepdims=True)
        squares = jnp.sum(acted * acted, axis=1, keepdims=True)
        sums[...] = jnp.where(lane == 0, total, squares)


def gates(core, own, other, term, far, gain, weight, chans):
    count, half = own.shape
    width = 2 * half
    return pl.pallas_call(
        gates_kernel,
        out_shape=[
            jax.ShapeDtypeStruct((count, width), jnp.bfloat16),
            jax.ShapeDtypeStruct((2, count, chans), jnp.float32),
            jax.ShapeDtypeStruct((count, LANES), jnp.float32),
        ],
        grid_spec=pltpu.PrefetchScalarGridSpec(
            num_scalar_prefetch=1,
            grid=(2,),
            in_specs=[
                whole((count, half)),
                whole((count, half)),
                whole((count, width)),
                whole((count, width)),
                whole((1, width)),
                spec((width, chans), lambda i, c: (0, 2 - i)),
            ],
            out_specs=[
                whole((count, width)),
                spec((1, count, chans), lambda i, c: (i, 0, 0)),
                whole((count, LANES)),
            ],
            scratch_shapes=[pltpu.VMEM((count, width), jnp.bfloat16)],
        ),
        compiler_params=params(1),
        cost_estimate=cost(4 * count * width * chans, 4 * width * chans, 2 * count * chans),
        name="gates",
    )(core, own, other, term, far, gain, weight)


def mix_kernel(act, sums, far, gain, bias, weight, shift, rows, term, mixed):
    groups = weight.shape[0]

    @pl.when(pl.program_id(0) == 0)
    def _():
        at = lax.broadcasted_iota(jnp.int32, (SPAN, SPAN), 0)
        source = lax.broadcasted_iota(jnp.int32, (SPAN, SPAN), 1)
        masked = [
            jnp.where(source <= at, weight[g], jnp.zeros_like(weight[g])) for g in range(groups)
        ]
        count, chans = mixed.shape
        wide = chans // groups
        for n in range(count // SPAN):
            block = pl.ds(n * SPAN, SPAN)
            totals = (sums[block, :] + far[block, :]) / BW
            v_mean = totals[:, 0:1]
            v_var = totals[:, 1:2] - v_mean * v_mean
            v_normed = (act[0, block, :] - v_mean) * lax.rsqrt(v_var + EPS) * gain[...] + bias[...]
            v_normed = v_normed.astype(jnp.bfloat16)
            spatial = [
                dot(masked[g], v_normed[:, g * wide : (g + 1) * wide]) + shift[:, g : g + 1]
                for g in range(groups)
            ]
            product = act[1, block, :] * jnp.concatenate(spatial, axis=1)
            mixed[block, :] = product.astype(jnp.bfloat16)

    term[...] = dot_rows(mixed[...], rows[...]).astype(jnp.bfloat16)


def mix(act, sums, far, gain, bias, weight, shift, rows):
    _, count, chans = act.shape
    width = rows.shape[0]
    groups = weight.shape[0]
    return pl.pallas_call(
        mix_kernel,
        out_shape=jax.ShapeDtypeStruct((count, width), jnp.bfloat16),
        grid=(width // WIDE,),
        in_specs=[
            whole(act.shape),
            whole((count, LANES)),
            whole((count, LANES)),
            whole((1, chans)),
            whole((1, chans)),
            whole((groups, SPAN, SPAN)),
            whole((SPAN, groups)),
            spec((WIDE, chans), lambda j: (j, 0)),
        ],
        out_specs=spec((count, WIDE), lambda j: (0, j)),
        scratch_shapes=[pltpu.VMEM((count, chans), jnp.bfloat16)],
        compiler_params=params(1),
        cost_estimate=cost(2 * count * width * chans, 2 * width * chans, count),
        name="mix",
    )(act, sums, far, gain, bias, weight, shift, rows)


def second_kernel(
    core, middle, term, far, gain, first, others, send, keep, base, normed, hidden, wide, down, sems
):
    step = pl.program_id(0)
    steps = 5
    outs = down.shape[0] // WIDE
    begin = starts(OTHERS)[3]
    cuts = [pl.ds(k * WIDE, WIDE) for k in range(4)] + [pl.ds(4 * WIDE, 6 * LANES)]
    copies = [
        pltpu.make_async_copy(first.at[:, cut], wide.at[:, cut], sems.at[k])
        for k, cut in enumerate(cuts)
    ]
    copies.append(
        pltpu.make_async_copy(others.at[:, pl.ds(begin, down.shape[1])], down, sems.at[steps])
    )

    @pl.when(step == 0)
    def _():
        for copy in copies:
            copy.start()
        values = middle[...].astype(jnp.float32) + (
            term[...].astype(jnp.float32) + far[...].astype(jnp.float32)
        )
        second = values.astype(jnp.bfloat16)
        half = second.shape[1] // 2
        base[...] = jnp.where(core[0] == 0, second[:, :half], second[:, half:])
        normed[...] = normed_rows(second.astype(jnp.float32), gain[...])

    for k, copy in enumerate(copies):

        @pl.when(step == k)
        def _():
            copy.wait()

    hidden_step(step, normed, wide, hidden)

    @pl.when(step >= steps)
    def _():
        n = step - steps
        mine = jnp.where(n < outs // 2, 1 - core[0], core[0])
        row = mine * (outs // 2) + lax.rem(n, outs // 2)
        rows = pl.ds(pl.multiple_of(row * WIDE, WIDE), WIDE)
        part = dot_rows(hidden[...], down[rows, :]).astype(jnp.bfloat16)

        @pl.when(n < outs // 2)
        def _():
            send[...] = part

        @pl.when(n >= outs // 2)
        def _():
            keep[...] = part


def second_pass(core, middle, term, far, gain, first, others):
    count, width = middle.shape
    half = width // 2
    columns = first.shape[1]
    units = columns // 2
    outs = width // WIDE
    sent = outs // 2
    return pl.pallas_call(
        second_kernel,
        out_shape=[jax.ShapeDtypeStruct((count, half), jnp.bfloat16)] * 3,
        grid_spec=pltpu.PrefetchScalarGridSpec(
            num_scalar_prefetch=1,
            grid=(5 + outs,),
            in_specs=[
                whole((count, width)),
                whole((count, width)),
                whole((count, width)),
                whole((1, width)),
                ANY,
                ANY,
            ],
            out_specs=[
                spec((count, WIDE), lambda j, c: (0, jnp.clip(j - 5, 0, sent - 1))),
                spec((count, WIDE), lambda j, c: (0, jnp.maximum(j - 5 - sent, 0))),
                whole((count, half)),
            ],
            scratch_shapes=[
                pltpu.VMEM((count, width), jnp.bfloat16),
                pltpu.VMEM((count, units), jnp.bfloat16),
                pltpu.VMEM((width, columns), jnp.bfloat16),
                pltpu.VMEM((width, units), jnp.bfloat16),
                pltpu.SemaphoreType.DMA((6,)),
            ],
        ),
        compiler_params=params(1),
        cost_estimate=cost(6 * count * width * units, 6 * width * units, count * units),
        name="second_pass",
    )(core, middle, term, far, gain, first, others)


def layer(
    tokens,
    norm_first,
    norm_mix,
    norm_second,
    gate_weight,
    up_weight,
    down_weight,
    gate_scale,
    up_scale,
    down_scale,
    u_weight,
    v_weight,
    u_scale,
    v_scale,
    ln_gain,
    ln_bias,
    spatial_weight,
    spatial_bias,
    out_weight,
    out_scale,
):
    chans = u_weight.shape[1]
    width = 2 * tokens.shape[1]

    def number(x):
        return x.reshape(1).astype(jnp.int32)

    core = number(lax.axis_index("tp"))
    rep = lax.axis_index("rep")
    at = number(2 * lax.axis_index(FS) + rep)

    colors = prepare(
        number(rep),
        gate_weight,
        up_weight,
        down_weight.T,
        u_weight,
        v_weight,
        out_weight.T,
        gate_scale,
        up_scale,
        down_scale,
        u_scale,
        v_scale,
        out_scale,
    )
    one, two = gather(colors)

    own, other = tokens, other_core(tokens)
    hidden, first = first_hidden(core, at, own, other, norm_first[None], one)
    term, others = first_down(at, hidden, width, two)
    middle, act, sums = gates(
        core, own, other, term, other_core(term), norm_mix[None], others, chans
    )
    term = mix(
        act,
        sums,
        other_core(sums),
        ln_gain[None],
        ln_bias[None],
        spatial_weight,
        spatial_bias.T,
        others,
    )
    send, keep, base = second_pass(
        core, middle, term, other_core(term), norm_second[None], first, others
    )
    last = keep.astype(jnp.float32) + other_core(send).astype(jnp.float32)
    return (base.astype(jnp.float32) + 0.5 * last).astype(jnp.bfloat16)


def solution(mesh):
    torus = Mesh(
        mesh.devices.reshape(mesh.shape["rep"], 2, 4, 4, mesh.shape["tp"]),
        ("rep", "fs_0", "fs_1", "fs_2", "tp"),
    )
    in_specs = (
        P(REP_FS, "tp"),
        P(),
        P(),
        P(),
        P(FS, "tp"),
        P(FS, "tp"),
        P("tp", FS),
        P("tp"),
        P("tp"),
        P(FS),
        P(FS, "tp"),
        P(FS, "tp"),
        P("tp"),
        P("tp"),
        P("tp"),
        P("tp"),
        P("tp", None, None),
        P("tp", None),
        P("tp", FS),
        P(FS),
    )
    out_specs = P(REP_FS, "tp")
    return jax.shard_map(layer, mesh=torus, in_specs=in_specs, out_specs=out_specs, check_vma=False)
```

```python
import functools

import jax
import jax.numpy as jnp
from jax import lax
from jax.experimental import pallas as pl
from jax.experimental.pallas import tpu as pltpu
from jax.sharding import Mesh
from jax.sharding import PartitionSpec as P


BW = 1024
SPAN = 128
FS = ("fs_0", "fs_1", "fs_2")
REP_FS = ("rep", "fs_0", "fs_1", "fs_2")
LANES = 128
WIDE = 512
HALF_ROWS = 32
FIRST = (4, 4, 4, 4, 3, 3)
OTHERS = (4, 4, 4, 3, 4, 4)
RINGS = (("fs_2", 1), ("fs_1", 1), ("z", 1), ("fs_2", 3), ("fs_1", 3), ("z", 3))
PLACES = (2, 8, 32, 6, 24, 33)
ROUNDS = (
    (0, 4, 5, 3, 2, 1),
    (0, 4, 3, 5, 1, 2),
    (1, 5, 4, 2, 3, 0),
    (1, 5, 2, 4, 0, 3),
    (2, 3, 1, 0, 5, 4),
    (2, 3, 0, 1, 4, 5),
)

EPS = 1e-06


def other_core(x):
    return lax.ppermute(x, "tp", [(0, 1), (1, 0)])


def normed_rows(values, gain):
    factor = lax.rsqrt(jnp.mean(values * values, axis=1, keepdims=True) + EPS)
    return (values * factor * gain).astype(jnp.bfloat16)


def dot(left, right):
    return jnp.dot(left, right, preferred_element_type=jnp.float32)


def dot_rows(left, rows):
    return lax.dot_general(
        left, rows, (((1,), (1,)), ((), ())), preferred_element_type=jnp.float32
    )


def gelu(a):
    return 0.5 * a * (1.0 + jnp.tanh(0.7978845608028654 * (a + 0.044715 * a * a * a)))


def spec(block, index):
    return pl.BlockSpec(block, index)


def whole(shape):
    return pl.BlockSpec(shape, lambda *_: (0,) * len(shape))


ANY = pl.BlockSpec(memory_space=pl.ANY)


def params(steps):
    return pltpu.CompilerParams(
        dimension_semantics=("arbitrary",) * steps, vmem_limit_bytes=60 * 1024 * 1024
    )


def cost(flops, moved, special):
    return pl.CostEstimate(flops=flops, bytes_accessed=moved, transcendentals=special)


def exchange(x, color, turn):
    name, flip = RINGS[ROUNDS[color][turn]]
    axis = ("rep", "fs_0") if name == "z" else name
    return lax.ppermute(x, axis, [(i, i ^ flip) for i in range(4)])


def place(color, slot):
    at = 0
    for turn in range(6):
        if slot >> turn & 1:
            at ^= PLACES[ROUNDS[color][turn]]
    return at


def starts(widths):
    ends = [0]
    for n in widths:
        ends.append(ends[-1] + n * LANES)
    return ends


PAIRS = [(p, t + k) for t in (0, 2, 4, 6) for p in (0, 1) for k in (0, 1)]
PAIRS += [(0, 8), (0, 9), (1, 8), (1, 9), (0, 10), (1, 10)]


def prepare_kernel(rep, *refs):
    inputs, colors, held, sems = refs[:12], refs[12:15], refs[15:27], refs[27]
    copies = [
        pltpu.make_async_copy(x, y, sems.at[k]) for k, (x, y) in enumerate(zip(inputs, held))
    ]
    for copy in copies:
        copy.start()
    for copy in copies:
        copy.wait()
    gate, up, down, u, v, out, gate_s, up_s, down_s, u_s, v_s, out_s = held
    rows = pl.ds(pl.multiple_of(rep[0] * HALF_ROWS, HALF_ROWS), HALF_ROWS)
    low = jnp.bfloat16

    def across(scale):
        return scale[...][None, :]

    def down_rows(scale):
        size = scale.shape[0]
        row = lax.broadcasted_iota(jnp.int32, (HALF_ROWS, size), 0) + rep[0] * HALF_ROWS
        column = lax.broadcasted_iota(jnp.int32, (HALF_ROWS, size), 1)
        return jnp.sum(jnp.where(row == column, across(scale), 0.0), axis=1, keepdims=True)

    pair = ((gate[rows, :] * across(gate_s)).astype(low), (up[rows, :] * across(up_s)).astype(low))
    firsts = [pair[p][:, t * LANES : (t + 1) * LANES] for p, t in PAIRS]
    rest = jnp.concatenate(
        [
            (out[rows, :] * down_rows(out_s)).astype(low),
            (u[rows, :] * across(u_s)).astype(low),
            (v[rows, :] * across(v_s)).astype(low),
            (down[rows, :] * down_rows(down_s)).astype(low),
        ],
        axis=1,
    )
    at, begin = 0, starts(OTHERS)
    mine = []
    for c in range(6):
        mine.append(firsts[at : at + FIRST[c]] + [rest[:, begin[c] : begin[c + 1]]])
        at += FIRST[c]
    for pair, ref in enumerate(colors):
        ref[...] = jnp.concatenate(mine[2 * pair] + mine[2 * pair + 1], axis=1)


WIDTHS = [(a + b) * LANES for a, b in zip(FIRST, OTHERS)]
VMEM = pl.BlockSpec(memory_space=pltpu.VMEM)
SMEM = pl.BlockSpec(memory_space=pltpu.SMEM)
HBM = pl.BlockSpec(memory_space=pltpu.HBM)


def prepare(rep, *arrays):
    pairs = [WIDTHS[k] + WIDTHS[k + 1] for k in (0, 2, 4)]
    return pl.pallas_call(
        prepare_kernel,
        out_shape=[jax.ShapeDtypeStruct((HALF_ROWS, n), jnp.bfloat16) for n in pairs],
        in_specs=[SMEM] + [HBM] * len(arrays),
        out_specs=[VMEM] * 3,
        scratch_shapes=[pltpu.VMEM(x.shape, x.dtype) for x in arrays]
        + [pltpu.SemaphoreType.DMA((len(arrays),))],
        compiler_params=pltpu.CompilerParams(vmem_limit_bytes=16 * 1024 * 1024),
        name="prepare",
    )(rep, *arrays)


def join_kernel(cuts, *refs):
    sources = (len(refs) - len(cuts)) // 2
    for joined, (source, begin, end) in zip(refs[2 * sources :], cuts):
        held, arrived = refs[source], refs[sources + source]
        rows = held.shape[0]
        joined[pl.ds(0, rows), :] = held[:, begin:end]
        joined[pl.ds(rows, rows), :] = arrived[:, begin:end]


def join(held, arrived, cuts=None):
    rows, low = held[0].shape[0], jnp.bfloat16
    if cuts is None:
        cuts = [(k, 0, x.shape[1]) for k, x in enumerate(held)]
    return pl.pallas_call(
        functools.partial(join_kernel, cuts),
        out_shape=[jax.ShapeDtypeStruct((2 * rows, b - a), low) for _, a, b in cuts],
        in_specs=[VMEM] * (2 * len(held)),
        out_specs=[VMEM] * len(cuts),
        compiler_params=pltpu.CompilerParams(vmem_limit_bytes=16 * 1024 * 1024),
        name="join",
    )(*held, *arrived)


def gather(pairs):
    ready = []
    for p, x in enumerate(pairs):
        (held,) = join([x], [exchange(x, 2 * p, 0)])
        edge = WIDTHS[2 * p]
        cuts = [(0, 0, edge), (0, edge, held.shape[1])]
        held = join([held], [exchange(held, 2 * p, 1)], cuts)
        for turn in (2, 3):
            held = join(held, [exchange(y, 2 * p + k, turn) for k, y in enumerate(held)])
        ready.append((held, [exchange(y, 2 * p + k, 4) for k, y in enumerate(held)]))
    groups = []
    for g in range(2):
        pieces = []
        for p, (held, arrived) in enumerate(ready):
            cuts = []
            for k, y in enumerate(held):
                edge = FIRST[2 * p + k] * LANES
                cuts.append((k, edge, y.shape[1]) if g else (k, 0, edge))
            halves = join(held, arrived, cuts)
            for k, y in enumerate(halves):
                pieces += [y, exchange(y, 2 * p + k, 5)]
        groups.append(pieces)
    return groups


def place_blocks(at, pieces, weight, sems, widths, colors):
    begin = starts(widths)
    for c in colors:
        columns = pl.ds(begin[c], widths[c] * LANES)
        for k in range(2):

            def copy_four(high, carry, c=c, k=k, columns=columns):
                moved = at ^ place(c, 32 * k)
                for bit in range(3):
                    moved = moved ^ ((high >> bit & 1) * place(c, 4 << bit))
                for low in range(4):
                    to = (moved ^ place(c, low)) * HALF_ROWS
                    origin = (high * 4 + low) * HALF_ROWS
                    pltpu.make_async_copy(
                        pieces[2 * c + k].at[
                            pl.ds(pl.multiple_of(origin, HALF_ROWS), HALF_ROWS), :
                        ],
                        weight.at[pl.ds(pl.multiple_of(to, HALF_ROWS), HALF_ROWS), columns],
                        sems.at[c],
                    ).start()
                return carry

            lax.fori_loop(0, 8, copy_four, 0)


def wait_color(weight, sems, widths, c):
    columns = pl.ds(starts(widths)[c], widths[c] * LANES)
    part = weight.at[:, columns]
    pltpu.make_async_copy(part, part, sems.at[c]).wait()


def silu_product(gate, up):
    return (gate / (1.0 + jnp.exp(-gate)) * up).astype(jnp.bfloat16)


def narrow_step(normed, weight):
    both = dot(normed, weight)
    tile = [both[:, k * LANES : (k + 1) * LANES] for k in range(6)]
    gate = jnp.concatenate([tile[0], tile[1], tile[4]], axis=1)
    up = jnp.concatenate([tile[2], tile[3], tile[5]], axis=1)
    return silu_product(gate, up)


def hidden_step(step, normed, weight, hidden):
    @pl.when(step < 4)
    def _():
        columns = pl.ds(pl.multiple_of(step * WIDE, WIDE), WIDE)
        both = dot(normed[...], weight[:, columns])
        to = pl.ds(pl.multiple_of(step * (WIDE // 2), WIDE // 2), WIDE // 2)
        hidden[:, to] = silu_product(both[:, : WIDE // 2], both[:, WIDE // 2 :])

    @pl.when(step == 4)
    def _():
        hidden[:, 2 * WIDE :] = narrow_step(normed[...], weight[:, 4 * WIDE :])


def first_kernel(core, at, own, other, gain, *rest):
    pieces, (hidden, kept, weight, normed, sems, out_sem) = rest[:12], rest[12:]
    step = pl.program_id(0)

    @pl.when(step == 0)
    def _():
        place_blocks(at[0], pieces, weight, sems, FIRST, range(6))
        left = jnp.where(core[0] == 0, own[...], other[...])
        right = jnp.where(core[0] == 0, other[...], own[...])
        values = jnp.concatenate([left, right], axis=1).astype(jnp.float32)
        normed[...] = normed_rows(values, gain[...])

    for c in range(6):

        @pl.when(step == min(c, 4))
        def _():
            wait_color(weight, sems, FIRST, c)

    hidden_step(step, normed, weight, hidden)

    @pl.when(step == 4)
    def _():
        copy = pltpu.make_async_copy(weight, kept, out_sem)
        copy.start()
        copy.wait()


def first_hidden(core, at, own, other, gain, pieces):
    count, half = own.shape
    width = 2 * half
    columns = sum(FIRST) * LANES
    units = columns // 2
    return pl.pallas_call(
        first_kernel,
        out_shape=[
            jax.ShapeDtypeStruct((count, units), jnp.bfloat16),
            jax.ShapeDtypeStruct((width, columns), jnp.bfloat16),
        ],
        grid_spec=pltpu.PrefetchScalarGridSpec(
            num_scalar_prefetch=2,
            grid=(5,),
            in_specs=[whole((count, half)), whole((count, half)), whole((1, width))] + [ANY] * 12,
            out_specs=[whole((count, units)), ANY],
            scratch_shapes=[
                pltpu.VMEM((width, columns), jnp.bfloat16),
                pltpu.VMEM((count, width), jnp.bfloat16),
                pltpu.SemaphoreType.DMA((6,)),
                pltpu.SemaphoreType.DMA,
            ],
        ),
        compiler_params=params(1),
        cost_estimate=cost(2 * count * width * columns, 4 * width * columns, count * units),
        name="first_hidden",
    )(core, at, own, other, gain, *pieces)


def down_kernel(at, hidden, *rest):
    pieces, (term, kept, weight, sems, out_sem) = rest[:12], rest[12:]
    step = pl.program_id(0)
    begin = starts(OTHERS)
    copy = pltpu.make_async_copy(weight, kept, out_sem)

    @pl.when(step == 0)
    def _():
        place_blocks(at[0], pieces, weight, sems, OTHERS, (3, 4, 5, 0, 1, 2))
        for c in (3, 4, 5):
            wait_color(weight, sems, OTHERS, c)

    rows = pl.ds(pl.multiple_of(step * WIDE, WIDE), WIDE)
    term[...] = dot_rows(hidden[...], weight[rows, begin[3] :]).astype(jnp.bfloat16)

    @pl.when(step == 0)
    def _():
        for c in (0, 1, 2):
            wait_color(weight, sems, OTHERS, c)
        copy.start()

    @pl.when(step == pl.num_programs(0) - 1)
    def _():
        copy.wait()


def first_down(at, hidden, width, pieces):
    count, units = hidden.shape
    columns = sum(OTHERS) * LANES
    return pl.pallas_call(
        down_kernel,
        out_shape=[
            jax.ShapeDtypeStruct((count, width), jnp.bfloat16),
            jax.ShapeDtypeStruct((width, columns), jnp.bfloat16),
        ],
        grid_spec=pltpu.PrefetchScalarGridSpec(
            num_scalar_prefetch=1,
            grid=(width // WIDE,),
            in_specs=[whole((count, units))] + [ANY] * 12,
            out_specs=[spec((count, WIDE), lambda j, a: (0, j)), ANY],
            scratch_shapes=[
                pltpu.VMEM((width, columns), jnp.bfloat16),
                pltpu.SemaphoreType.DMA((6,)),
                pltpu.SemaphoreType.DMA,
            ],
        ),
        compiler_params=params(1),
        cost_estimate=cost(2 * count * width * units, 4 * width * columns, 0),
        name="first_down",
    )(at, hidden, *pieces)


def gates_kernel(core, own, other, term, far, gain, rows, middle, act, sums, normed):
    @pl.when(pl.program_id(0) == 0)
    def _():
        left = jnp.where(core[0] == 0, own[...], other[...])
        right = jnp.where(core[0] == 0, other[...], own[...])
        values = jnp.concatenate([left, right], axis=1).astype(jnp.float32)
        values = values + 0.5 * (term[...].astype(jnp.float32) + far[...].astype(jnp.float32))
        mid = values.astype(jnp.bfloat16)
        middle[...] = mid
        normed[...] = normed_rows(mid.astype(jnp.float32), gain[...])

    acted = gelu(dot(normed[...], rows[...]))
    act[0] = acted

    @pl.when(pl.program_id(0) == 0)
    def _():
        lane = lax.broadcasted_iota(jnp.int32, sums.shape, 1)
        total = jnp.sum(acted, axis=1, keepdims=True)
        squares = jnp.sum(acted * acted, axis=1, keepdims=True)
        sums[...] = jnp.where(lane == 0, total, squares)


def gates(core, own, other, term, far, gain, weight, chans):
    count, half = own.shape
    width = 2 * half
    return pl.pallas_call(
        gates_kernel,
        out_shape=[
            jax.ShapeDtypeStruct((count, width), jnp.bfloat16),
            jax.ShapeDtypeStruct((2, count, chans), jnp.float32),
            jax.ShapeDtypeStruct((count, LANES), jnp.float32),
        ],
        grid_spec=pltpu.PrefetchScalarGridSpec(
            num_scalar_prefetch=1,
            grid=(2,),
            in_specs=[
                whole((count, half)),
                whole((count, half)),
                whole((count, width)),
                whole((count, width)),
                whole((1, width)),
                spec((width, chans), lambda i, c: (0, 2 - i)),
            ],
            out_specs=[
                whole((count, width)),
                spec((1, count, chans), lambda i, c: (i, 0, 0)),
                whole((count, LANES)),
            ],
            scratch_shapes=[pltpu.VMEM((count, width), jnp.bfloat16)],
        ),
        compiler_params=params(1),
        cost_estimate=cost(4 * count * width * chans, 4 * width * chans, 2 * count * chans),
        name="gates",
    )(core, own, other, term, far, gain, weight)


def mix_kernel(act, sums, far, gain, bias, weight, shift, rows, term, mixed):
    groups = weight.shape[0]

    @pl.when(pl.program_id(0) == 0)
    def _():
        at = lax.broadcasted_iota(jnp.int32, (SPAN, SPAN), 0)
        source = lax.broadcasted_iota(jnp.int32, (SPAN, SPAN), 1)
        masked = [
            jnp.where(source <= at, weight[g], jnp.zeros_like(weight[g])) for g in range(groups)
        ]
        count, chans = mixed.shape
        wide = chans // groups
        for n in range(count // SPAN):
            block = pl.ds(n * SPAN, SPAN)
            totals = (sums[block, :] + far[block, :]) / BW
            v_mean = totals[:, 0:1]
            v_var = totals[:, 1:2] - v_mean * v_mean
            v_normed = (act[0, block, :] - v_mean) * lax.rsqrt(v_var + EPS) * gain[...] + bias[...]
            v_normed = v_normed.astype(jnp.bfloat16)
            spatial = [
                dot(masked[g], v_normed[:, g * wide : (g + 1) * wide]) + shift[:, g : g + 1]
                for g in range(groups)
            ]
            product = act[1, block, :] * jnp.concatenate(spatial, axis=1)
            mixed[block, :] = product.astype(jnp.bfloat16)

    term[...] = dot_rows(mixed[...], rows[...]).astype(jnp.bfloat16)


def mix(act, sums, far, gain, bias, weight, shift, rows):
    _, count, chans = act.shape
    width = rows.shape[0]
    groups = weight.shape[0]
    return pl.pallas_call(
        mix_kernel,
        out_shape=jax.ShapeDtypeStruct((count, width), jnp.bfloat16),
        grid=(width // WIDE,),
        in_specs=[
            whole(act.shape),
            whole((count, LANES)),
            whole((count, LANES)),
            whole((1, chans)),
            whole((1, chans)),
            whole((groups, SPAN, SPAN)),
            whole((SPAN, groups)),
            spec((WIDE, chans), lambda j: (j, 0)),
        ],
        out_specs=spec((count, WIDE), lambda j: (0, j)),
        scratch_shapes=[pltpu.VMEM((count, chans), jnp.bfloat16)],
        compiler_params=params(1),
        cost_estimate=cost(2 * count * width * chans, 2 * width * chans, count),
        name="mix",
    )(act, sums, far, gain, bias, weight, shift, rows)


def second_kernel(
    core, middle, term, far, gain, first, others, send, keep, base, normed, hidden, wide, down, sems
):
    step = pl.program_id(0)
    steps = 5
    outs = down.shape[0] // WIDE
    begin = starts(OTHERS)[3]
    cuts = [pl.ds(k * WIDE, WIDE) for k in range(4)] + [pl.ds(4 * WIDE, 6 * LANES)]
    copies = [
        pltpu.make_async_copy(first.at[:, cut], wide.at[:, cut], sems.at[k])
        for k, cut in enumerate(cuts)
    ]
    copies.append(
        pltpu.make_async_copy(others.at[:, pl.ds(begin, down.shape[1])], down, sems.at[steps])
    )

    @pl.when(step == 0)
    def _():
        for copy in copies:
            copy.start()
        values = middle[...].astype(jnp.float32) + (
            term[...].astype(jnp.float32) + far[...].astype(jnp.float32)
        )
        second = values.astype(jnp.bfloat16)
        half = second.shape[1] // 2
        base[...] = jnp.where(core[0] == 0, second[:, :half], second[:, half:])
        normed[...] = normed_rows(second.astype(jnp.float32), gain[...])

    for k, copy in enumerate(copies):

        @pl.when(step == k)
        def _():
            copy.wait()

    hidden_step(step, normed, wide, hidden)

    @pl.when(step >= steps)
    def _():
        n = step - steps
        mine = jnp.where(n < outs // 2, 1 - core[0], core[0])
        row = mine * (outs // 2) + lax.rem(n, outs // 2)
        rows = pl.ds(pl.multiple_of(row * WIDE, WIDE), WIDE)
        part = dot_rows(hidden[...], down[rows, :]).astype(jnp.bfloat16)

        @pl.when(n < outs // 2)
        def _():
            send[...] = part

        @pl.when(n >= outs // 2)
        def _():
            keep[...] = part


def second_pass(core, middle, term, far, gain, first, others):
    count, width = middle.shape
    half = width // 2
    columns = first.shape[1]
    units = columns // 2
    outs = width // WIDE
    sent = outs // 2
    return pl.pallas_call(
        second_kernel,
        out_shape=[jax.ShapeDtypeStruct((count, half), jnp.bfloat16)] * 3,
        grid_spec=pltpu.PrefetchScalarGridSpec(
            num_scalar_prefetch=1,
            grid=(5 + outs,),
            in_specs=[
                whole((count, width)),
                whole((count, width)),
                whole((count, width)),
                whole((1, width)),
                ANY,
                ANY,
            ],
            out_specs=[
                spec((count, WIDE), lambda j, c: (0, jnp.clip(j - 5, 0, sent - 1))),
                spec((count, WIDE), lambda j, c: (0, jnp.maximum(j - 5 - sent, 0))),
                whole((count, half)),
            ],
            scratch_shapes=[
                pltpu.VMEM((count, width), jnp.bfloat16),
                pltpu.VMEM((count, units), jnp.bfloat16),
                pltpu.VMEM((width, columns), jnp.bfloat16),
                pltpu.VMEM((width, units), jnp.bfloat16),
                pltpu.SemaphoreType.DMA((6,)),
            ],
        ),
        compiler_params=params(1),
        cost_estimate=cost(6 * count * width * units, 6 * width * units, count * units),
        name="second_pass",
    )(core, middle, term, far, gain, first, others)


def layer(
    tokens,
    norm_first,
    norm_mix,
    norm_second,
    gate_weight,
    up_weight,
    down_weight,
    gate_scale,
    up_scale,
    down_scale,
    u_weight,
    v_weight,
    u_scale,
    v_scale,
    ln_gain,
    ln_bias,
    spatial_weight,
    spatial_bias,
    out_weight,
    out_scale,
):
    chans = u_weight.shape[1]
    width = 2 * tokens.shape[1]

    def number(x):
        return x.reshape(1).astype(jnp.int32)

    core = number(lax.axis_index("tp"))
    rep = lax.axis_index("rep")
    at = number(2 * lax.axis_index(FS) + rep)

    colors = prepare(
        number(rep),
        gate_weight,
        up_weight,
        down_weight.T,
        u_weight,
        v_weight,
        out_weight.T,
        gate_scale,
        up_scale,
        down_scale,
        u_scale,
        v_scale,
        out_scale,
    )
    one, two = gather(colors)

    own, other = tokens, other_core(tokens)
    hidden, first = first_hidden(core, at, own, other, norm_first[None], one)
    term, others = first_down(at, hidden, width, two)
    middle, act, sums = gates(
        core, own, other, term, other_core(term), norm_mix[None], others, chans
    )
    term = mix(
        act,
        sums,
        other_core(sums),
        ln_gain[None],
        ln_bias[None],
        spatial_weight,
        spatial_bias.T,
        others,
    )
    send, keep, base = second_pass(
        core, middle, term, other_core(term), norm_second[None], first, others
    )
    last = keep.astype(jnp.float32) + other_core(send).astype(jnp.float32)
    return (base.astype(jnp.float32) + 0.5 * last).astype(jnp.bfloat16)


def solution(mesh):
    torus = Mesh(
        mesh.devices.reshape(mesh.shape["rep"], 2, 4, 4, mesh.shape["tp"]),
        ("rep", "fs_0", "fs_1", "fs_2", "tp"),
    )
    in_specs = (
        P(REP_FS, "tp"),
        P(),
        P(),
        P(),
        P(FS, "tp"),
        P(FS, "tp"),
        P("tp", FS),
        P("tp"),
        P("tp"),
        P(FS),
        P(FS, "tp"),
        P(FS, "tp"),
        P("tp"),
        P("tp"),
        P("tp"),
        P("tp"),
        P("tp", None, None),
        P("tp", None),
        P("tp", FS),
        P(FS),
    )
    out_specs = P(REP_FS, "tp")
    return jax.shard_map(layer, mesh=torus, in_specs=in_specs, out_specs=out_specs, check_vma=False)
```

```python
import functools

import jax
import jax.numpy as jnp
from jax import lax
from jax.experimental import pallas as pl
from jax.experimental.pallas import tpu as pltpu
from jax.sharding import Mesh
from jax.sharding import PartitionSpec as P


BW = 1024
SPAN = 128
FS = ("fs_0", "fs_1", "fs_2")
REP_FS = ("rep", "fs_0", "fs_1", "fs_2")
LANES = 128
WIDE = 512
HALF_ROWS = 32
CHUNK = 256
FIRST = (4, 4, 4, 4, 3, 3)
OTHERS = (4, 4, 4, 3, 4, 4)
RINGS = (("fs_2", 1), ("fs_1", 1), ("z", 1), ("fs_2", 3), ("fs_1", 3), ("z", 3))
PLACES = (2, 8, 32, 6, 24, 33)
ROUNDS = (
    (0, 4, 5, 3, 2, 1),
    (0, 4, 3, 5, 1, 2),
    (1, 5, 4, 2, 3, 0),
    (1, 5, 2, 4, 0, 3),
    (2, 3, 1, 0, 5, 4),
    (2, 3, 0, 1, 4, 5),
)

EPS = 1e-06


def other_core(x):
    return lax.ppermute(x, "tp", [(0, 1), (1, 0)])


def normed_rows(values, gain):
    factor = lax.rsqrt(jnp.mean(values * values, axis=1, keepdims=True) + EPS)
    return (values * factor * gain).astype(jnp.bfloat16)


def dot(left, right):
    return jnp.dot(left, right, preferred_element_type=jnp.float32)


def dot_rows(left, rows):
    return lax.dot_general(
        left, rows, (((1,), (1,)), ((), ())), preferred_element_type=jnp.float32
    )


def gelu(a):
    return 0.5 * a * (1.0 + jnp.tanh(0.7978845608028654 * (a + 0.044715 * a * a * a)))


def spec(block, index):
    return pl.BlockSpec(block, index)


def whole(shape):
    return pl.BlockSpec(shape, lambda *_: (0,) * len(shape))


ANY = pl.BlockSpec(memory_space=pl.ANY)


def params(steps, mib=60):
    return pltpu.CompilerParams(
        dimension_semantics=("arbitrary",) * steps, vmem_limit_bytes=mib * 1024 * 1024
    )


def cost(flops, moved, special):
    return pl.CostEstimate(flops=flops, bytes_accessed=moved, transcendentals=special)


def exchange(x, color, turn):
    name, flip = RINGS[ROUNDS[color][turn]]
    axis = ("rep", "fs_0") if name == "z" else name
    return lax.ppermute(x, axis, [(i, i ^ flip) for i in range(4)])


def place(color, slot):
    at = 0
    for turn in range(6):
        if slot >> turn & 1:
            at ^= PLACES[ROUNDS[color][turn]]
    return at


def starts(widths):
    ends = [0]
    for n in widths:
        ends.append(ends[-1] + n * LANES)
    return ends


PAIRS = [(p, t + k) for t in (0, 2, 4, 6) for p in (0, 1) for k in (0, 1)]
PAIRS += [(0, 8), (0, 9), (1, 8), (1, 9), (0, 10), (1, 10)]


def prepare_kernel(rep, *refs):
    inputs, colors, held, sems = refs[:12], refs[12:15], refs[15:27], refs[27]
    copies = [
        pltpu.make_async_copy(x, y, sems.at[k]) for k, (x, y) in enumerate(zip(inputs, held))
    ]
    for copy in copies:
        copy.start()
    for copy in copies:
        copy.wait()
    gate, up, down, u, v, out, gate_s, up_s, down_s, u_s, v_s, out_s = held
    rows = pl.ds(pl.multiple_of(rep[0] * HALF_ROWS, HALF_ROWS), HALF_ROWS)
    low = jnp.bfloat16

    def across(scale):
        return scale[...][None, :]

    def down_rows(scale):
        size = scale.shape[0]
        row = lax.broadcasted_iota(jnp.int32, (HALF_ROWS, size), 0) + rep[0] * HALF_ROWS
        column = lax.broadcasted_iota(jnp.int32, (HALF_ROWS, size), 1)
        return jnp.sum(jnp.where(row == column, across(scale), 0.0), axis=1, keepdims=True)

    pair = ((gate[rows, :] * across(gate_s)).astype(low), (up[rows, :] * across(up_s)).astype(low))
    firsts = [pair[p][:, t * LANES : (t + 1) * LANES] for p, t in PAIRS]
    rest = jnp.concatenate(
        [
            (out[rows, :] * down_rows(out_s)).astype(low),
            (u[rows, :] * across(u_s)).astype(low),
            (v[rows, :] * across(v_s)).astype(low),
            (down[rows, :] * down_rows(down_s)).astype(low),
        ],
        axis=1,
    )
    at, begin = 0, starts(OTHERS)
    mine = []
    for c in range(6):
        mine.append(firsts[at : at + FIRST[c]] + [rest[:, begin[c] : begin[c + 1]]])
        at += FIRST[c]
    for pair, ref in enumerate(colors):
        ref[...] = jnp.concatenate(mine[2 * pair] + mine[2 * pair + 1], axis=1)


WIDTHS = [(a + b) * LANES for a, b in zip(FIRST, OTHERS)]
VMEM = pl.BlockSpec(memory_space=pltpu.VMEM)
SMEM = pl.BlockSpec(memory_space=pltpu.SMEM)
HBM = pl.BlockSpec(memory_space=pltpu.HBM)


def prepare(rep, *arrays):
    pairs = [WIDTHS[k] + WIDTHS[k + 1] for k in (0, 2, 4)]
    return pl.pallas_call(
        prepare_kernel,
        out_shape=[jax.ShapeDtypeStruct((HALF_ROWS, n), jnp.bfloat16) for n in pairs],
        in_specs=[SMEM] + [HBM] * len(arrays),
        out_specs=[VMEM] * 3,
        scratch_shapes=[pltpu.VMEM(x.shape, x.dtype) for x in arrays]
        + [pltpu.SemaphoreType.DMA((len(arrays),))],
        compiler_params=pltpu.CompilerParams(vmem_limit_bytes=60 * 1024 * 1024),
        name="prepare",
    )(rep, *arrays)


def join_kernel(cuts, *refs):
    sources = (len(refs) - len(cuts)) // 2
    for joined, (source, begin, end) in zip(refs[2 * sources :], cuts):
        held, arrived = refs[source], refs[sources + source]
        rows = held.shape[0]
        joined[pl.ds(0, rows), :] = held[:, begin:end]
        joined[pl.ds(rows, rows), :] = arrived[:, begin:end]


def join(held, arrived, cuts=None):
    rows, low = held[0].shape[0], jnp.bfloat16
    if cuts is None:
        cuts = [(k, 0, x.shape[1]) for k, x in enumerate(held)]
    return pl.pallas_call(
        functools.partial(join_kernel, cuts),
        out_shape=[jax.ShapeDtypeStruct((2 * rows, b - a), low) for _, a, b in cuts],
        in_specs=[VMEM] * (2 * len(held)),
        out_specs=[VMEM] * len(cuts),
        compiler_params=pltpu.CompilerParams(vmem_limit_bytes=16 * 1024 * 1024),
        name="join",
    )(*held, *arrived)


def gather(pairs):
    ready = []
    for p, x in enumerate(pairs):
        (held,) = join([x], [exchange(x, 2 * p, 0)])
        edge = WIDTHS[2 * p]
        cuts = [(0, 0, edge), (0, edge, held.shape[1])]
        held = join([held], [exchange(held, 2 * p, 1)], cuts)
        for turn in (2, 3):
            held = join(held, [exchange(y, 2 * p + k, turn) for k, y in enumerate(held)])
        ready.append((held, [exchange(y, 2 * p + k, 4) for k, y in enumerate(held)]))
    groups = []
    for g in range(2):
        pieces = []
        for p, (held, arrived) in enumerate(ready):
            cuts = []
            for k, y in enumerate(held):
                edge = FIRST[2 * p + k] * LANES
                cuts.append((k, edge, y.shape[1]) if g else (k, 0, edge))
            halves = join(held, arrived, cuts)
            for k, y in enumerate(halves):
                pieces += [y, exchange(y, 2 * p + k, 5)]
        groups.append(pieces)
    return groups


def place_blocks(at, pieces, weight, sems, widths, colors):
    begin = starts(widths)
    for c in colors:
        columns = pl.ds(begin[c], widths[c] * LANES)
        for k in range(2):

            def copy_four(high, carry, c=c, k=k, columns=columns):
                moved = at ^ place(c, 32 * k)
                for bit in range(3):
                    moved = moved ^ ((high >> bit & 1) * place(c, 4 << bit))
                for low in range(4):
                    to = (moved ^ place(c, low)) * HALF_ROWS
                    origin = (high * 4 + low) * HALF_ROWS
                    pltpu.make_async_copy(
                        pieces[2 * c + k].at[
                            pl.ds(pl.multiple_of(origin, HALF_ROWS), HALF_ROWS), :
                        ],
                        weight.at[pl.ds(pl.multiple_of(to, HALF_ROWS), HALF_ROWS), columns],
                        sems.at[c],
                    ).start()
                return carry

            lax.fori_loop(0, 8, copy_four, 0)


def wait_color(weight, sems, widths, c):
    columns = pl.ds(starts(widths)[c], widths[c] * LANES)
    part = weight.at[:, columns]
    pltpu.make_async_copy(part, part, sems.at[c]).wait()


def silu_product(gate, up):
    return (gate / (1.0 + jnp.exp(-gate)) * up).astype(jnp.bfloat16)


def narrow_step(normed, weight):
    both = dot(normed, weight)
    tile = [both[:, k * LANES : (k + 1) * LANES] for k in range(6)]
    gate = jnp.concatenate([tile[0], tile[1], tile[4]], axis=1)
    up = jnp.concatenate([tile[2], tile[3], tile[5]], axis=1)
    return silu_product(gate, up)


def hidden_step(step, normed, weight, hidden):
    @pl.when(step < 4)
    def _():
        columns = pl.ds(pl.multiple_of(step * WIDE, WIDE), WIDE)
        both = dot(normed[...], weight[:, columns])
        to = pl.ds(pl.multiple_of(step * (WIDE // 2), WIDE // 2), WIDE // 2)
        hidden[:, to] = silu_product(both[:, : WIDE // 2], both[:, WIDE // 2 :])

    @pl.when(step == 4)
    def _():
        hidden[:, 2 * WIDE :] = narrow_step(normed[...], weight[:, 4 * WIDE :])


def first_kernel(core, at, own, other, gain, *rest):
    pieces, (hidden, kept, weight, normed, sems, out_sem) = rest[:12], rest[12:]
    step = pl.program_id(0)

    @pl.when(step == 0)
    def _():
        place_blocks(at[0], pieces, weight, sems, FIRST, range(6))
        left = jnp.where(core[0] == 0, own[...], other[...])
        right = jnp.where(core[0] == 0, other[...], own[...])
        values = jnp.concatenate([left, right], axis=1).astype(jnp.float32)
        normed[...] = normed_rows(values, gain[...])

    for c in range(6):

        @pl.when(step == min(c, 4))
        def _():
            wait_color(weight, sems, FIRST, c)

    hidden_step(step, normed, weight, hidden)

    @pl.when(step == 4)
    def _():
        copy = pltpu.make_async_copy(weight, kept, out_sem)
        copy.start()
        copy.wait()


def first_hidden(core, at, own, other, gain, pieces):
    count, half = own.shape
    width = 2 * half
    columns = sum(FIRST) * LANES
    units = columns // 2
    return pl.pallas_call(
        first_kernel,
        out_shape=[
            jax.ShapeDtypeStruct((count, units), jnp.bfloat16),
            jax.ShapeDtypeStruct((width, columns), jnp.bfloat16),
        ],
        grid_spec=pltpu.PrefetchScalarGridSpec(
            num_scalar_prefetch=2,
            grid=(5,),
            in_specs=[whole((count, half)), whole((count, half)), whole((1, width))] + [ANY] * 12,
            out_specs=[whole((count, units)), ANY],
            scratch_shapes=[
                pltpu.VMEM((width, columns), jnp.bfloat16),
                pltpu.VMEM((count, width), jnp.bfloat16),
                pltpu.SemaphoreType.DMA((6,)),
                pltpu.SemaphoreType.DMA,
            ],
        ),
        compiler_params=params(1),
        cost_estimate=cost(2 * count * width * columns, 4 * width * columns, count * units),
        name="first_hidden",
    )(core, at, own, other, gain, *pieces)


def down_kernel(at, hidden, *rest):
    pieces, (early, late, kept, weight, sems, out_sem) = rest[:12], rest[12:]
    step = pl.program_id(0)
    begin = starts(OTHERS)
    copy = pltpu.make_async_copy(weight, kept, out_sem)

    @pl.when(step == 0)
    def _():
        place_blocks(at[0], pieces, weight, sems, OTHERS, (3, 4, 5, 0, 1, 2))
        for c in (3, 4, 5):
            wait_color(weight, sems, OTHERS, c)

    rows = pl.ds(pl.multiple_of(step * WIDE, WIDE), WIDE)
    term = dot_rows(hidden[...], weight[rows, begin[3] :]).astype(jnp.bfloat16)
    early[...] = term[:CHUNK]
    late[...] = term[CHUNK:]

    @pl.when(step == 0)
    def _():
        for c in (0, 1, 2):
            wait_color(weight, sems, OTHERS, c)
        copy.start()

    @pl.when(step == pl.num_programs(0) - 1)
    def _():
        copy.wait()


def first_down(at, hidden, width, pieces):
    count, units = hidden.shape
    columns = sum(OTHERS) * LANES
    return pl.pallas_call(
        down_kernel,
        out_shape=[
            jax.ShapeDtypeStruct((CHUNK, width), jnp.bfloat16),
            jax.ShapeDtypeStruct((count - CHUNK, width), jnp.bfloat16),
            jax.ShapeDtypeStruct((width, columns), jnp.bfloat16),
        ],
        grid_spec=pltpu.PrefetchScalarGridSpec(
            num_scalar_prefetch=1,
            grid=(width // WIDE,),
            in_specs=[whole((count, units))] + [ANY] * 12,
            out_specs=[
                spec((CHUNK, WIDE), lambda j, a: (0, j)),
                spec((count - CHUNK, WIDE), lambda j, a: (0, j)),
                ANY,
            ],
            scratch_shapes=[
                pltpu.VMEM((width, columns), jnp.bfloat16),
                pltpu.SemaphoreType.DMA((6,)),
                pltpu.SemaphoreType.DMA,
            ],
        ),
        compiler_params=params(1),
        cost_estimate=cost(2 * count * width * units, 4 * width * columns, 0),
        name="first_down",
    )(at, hidden, *pieces)


def gates_kernel(core, own, other, term, far, gain, rows, middle, act, sums, normed):
    @pl.when(pl.program_id(0) == 0)
    def _():
        left = jnp.where(core[0] == 0, own[...], other[...])
        right = jnp.where(core[0] == 0, other[...], own[...])
        values = jnp.concatenate([left, right], axis=1).astype(jnp.float32)
        values = values + 0.5 * (term[...].astype(jnp.float32) + far[...].astype(jnp.float32))
        mid = values.astype(jnp.bfloat16)
        middle[...] = mid
        normed[...] = normed_rows(mid.astype(jnp.float32), gain[...])

    acted = gelu(dot(normed[...], rows[...]))
    act[0] = acted

    @pl.when(pl.program_id(0) == 0)
    def _():
        lane = lax.broadcasted_iota(jnp.int32, sums.shape, 1)
        total = jnp.sum(acted, axis=1, keepdims=True)
        squares = jnp.sum(acted * acted, axis=1, keepdims=True)
        sums[...] = jnp.where(lane == 0, total, squares)


def gates(core, own, other, term, far, gain, weight, chans):
    count, half = own.shape
    width = 2 * half
    return pl.pallas_call(
        gates_kernel,
        out_shape=[
            jax.ShapeDtypeStruct((count, width), jnp.bfloat16),
            jax.ShapeDtypeStruct((2, count, chans), jnp.float32),
            jax.ShapeDtypeStruct((count, LANES), jnp.float32),
        ],
        grid_spec=pltpu.PrefetchScalarGridSpec(
            num_scalar_prefetch=1,
            grid=(2,),
            in_specs=[
                whole((count, half)),
                whole((count, half)),
                whole((count, width)),
                whole((count, width)),
                whole((1, width)),
                spec((width, chans), lambda i, c: (0, 2 - i)),
            ],
            out_specs=[
                whole((count, width)),
                spec((1, count, chans), lambda i, c: (i, 0, 0)),
                whole((count, LANES)),
            ],
            scratch_shapes=[pltpu.VMEM((count, width), jnp.bfloat16)],
        ),
        compiler_params=params(1),
        cost_estimate=cost(4 * count * width * chans, 4 * width * chans, 2 * count * chans),
        name="gates",
    )(core, own, other, term, far, gain, weight)


def mix_kernel(act, sums, far, gain, bias, weight, shift, rows, term, mixed):
    groups = weight.shape[0]

    @pl.when(pl.program_id(0) == 0)
    def _():
        at = lax.broadcasted_iota(jnp.int32, (SPAN, SPAN), 0)
        source = lax.broadcasted_iota(jnp.int32, (SPAN, SPAN), 1)
        masked = [
            jnp.where(source <= at, weight[g], jnp.zeros_like(weight[g])) for g in range(groups)
        ]
        count, chans = mixed.shape
        wide = chans // groups
        for n in range(count // SPAN):
            block = pl.ds(n * SPAN, SPAN)
            totals = (sums[block, :] + far[block, :]) / BW
            v_mean = totals[:, 0:1]
            v_var = totals[:, 1:2] - v_mean * v_mean
            v_normed = (act[0, block, :] - v_mean) * lax.rsqrt(v_var + EPS) * gain[...] + bias[...]
            v_normed = v_normed.astype(jnp.bfloat16)
            spatial = [
                dot(masked[g], v_normed[:, g * wide : (g + 1) * wide]) + shift[:, g : g + 1]
                for g in range(groups)
            ]
            product = act[1, block, :] * jnp.concatenate(spatial, axis=1)
            mixed[block, :] = product.astype(jnp.bfloat16)

    term[...] = dot_rows(mixed[...], rows[...]).astype(jnp.bfloat16)


def mix(act, sums, far, gain, bias, weight, shift, rows):
    _, count, chans = act.shape
    width = rows.shape[0]
    groups = weight.shape[0]
    return pl.pallas_call(
        mix_kernel,
        out_shape=jax.ShapeDtypeStruct((count, width), jnp.bfloat16),
        grid=(width // WIDE,),
        in_specs=[
            whole(act.shape),
            whole((count, LANES)),
            whole((count, LANES)),
            whole((1, chans)),
            whole((1, chans)),
            whole((groups, SPAN, SPAN)),
            whole((SPAN, groups)),
            spec((WIDE, chans), lambda j: (j, 0)),
        ],
        out_specs=spec((count, WIDE), lambda j: (0, j)),
        scratch_shapes=[pltpu.VMEM((count, chans), jnp.bfloat16)],
        compiler_params=params(1),
        cost_estimate=cost(2 * count * width * chans, 2 * width * chans, count),
        name="mix",
    )(act, sums, far, gain, bias, weight, shift, rows)


def second_kernel(
    core, middle, term, far, gain, first, others, send, keep, base, normed, hidden, wide, down, sems
):
    step = pl.program_id(0)
    steps = 5
    outs = down.shape[0] // WIDE
    begin = starts(OTHERS)[3]
    cuts = [pl.ds(k * WIDE, WIDE) for k in range(4)] + [pl.ds(4 * WIDE, 6 * LANES)]
    copies = [
        pltpu.make_async_copy(first.at[:, cut], wide.at[:, cut], sems.at[k])
        for k, cut in enumerate(cuts)
    ]
    copies.append(
        pltpu.make_async_copy(others.at[:, pl.ds(begin, down.shape[1])], down, sems.at[steps])
    )

    @pl.when(step == 0)
    def _():
        for copy in copies:
            copy.start()
        values = middle[...].astype(jnp.float32) + (
            term[...].astype(jnp.float32) + far[...].astype(jnp.float32)
        )
        second = values.astype(jnp.bfloat16)
        half = second.shape[1] // 2
        base[...] = jnp.where(core[0] == 0, second[:, :half], second[:, half:])
        normed[...] = normed_rows(second.astype(jnp.float32), gain[...])

    for k, copy in enumerate(copies):

        @pl.when(step == k)
        def _():
            copy.wait()

    hidden_step(step, normed, wide, hidden)

    @pl.when(step >= steps)
    def _():
        n = step - steps
        mine = jnp.where(n < outs // 2, 1 - core[0], core[0])
        row = mine * (outs // 2) + lax.rem(n, outs // 2)
        rows = pl.ds(pl.multiple_of(row * WIDE, WIDE), WIDE)
        part = dot_rows(hidden[...], down[rows, :]).astype(jnp.bfloat16)

        @pl.when(n < outs // 2)
        def _():
            send[...] = part

        @pl.when(n >= outs // 2)
        def _():
            keep[...] = part


def second_pass(core, middle, term, far, gain, first, others):
    count, width = middle.shape
    half = width // 2
    columns = first.shape[1]
    units = columns // 2
    outs = width // WIDE
    sent = outs // 2
    return pl.pallas_call(
        second_kernel,
        out_shape=[jax.ShapeDtypeStruct((count, half), jnp.bfloat16)] * 3,
        grid_spec=pltpu.PrefetchScalarGridSpec(
            num_scalar_prefetch=1,
            grid=(5 + outs,),
            in_specs=[
                whole((count, width)),
                whole((count, width)),
                whole((count, width)),
                whole((1, width)),
                ANY,
                ANY,
            ],
            out_specs=[
                spec((count, WIDE), lambda j, c: (0, jnp.clip(j - 5, 0, sent - 1))),
                spec((count, WIDE), lambda j, c: (0, jnp.maximum(j - 5 - sent, 0))),
                whole((count, half)),
            ],
            scratch_shapes=[
                pltpu.VMEM((count, width), jnp.bfloat16),
                pltpu.VMEM((count, units), jnp.bfloat16),
                pltpu.VMEM((width, columns), jnp.bfloat16),
                pltpu.VMEM((width, units), jnp.bfloat16),
                pltpu.SemaphoreType.DMA((6,)),
            ],
        ),
        compiler_params=params(1),
        cost_estimate=cost(6 * count * width * units, 6 * width * units, count * units),
        name="second_pass",
    )(core, middle, term, far, gain, first, others)


def finish_kernel(base, keep, far, *rest):
    last = keep[...].astype(jnp.float32) + far[...].astype(jnp.float32)
    rest[-1][...] = (base[...].astype(jnp.float32) + 0.5 * last).astype(jnp.bfloat16)


def finish(base, keep, far, count, row, partial):
    rows, half = base.shape
    block = spec((SPAN, half), lambda i: (i, 0))
    held = [] if partial is None else [partial]
    return pl.pallas_call(
        finish_kernel,
        out_shape=jax.ShapeDtypeStruct((count, half), jnp.bfloat16),
        grid=(rows // SPAN,),
        in_specs=[block] * 3 + [ANY] * len(held),
        out_specs=spec((SPAN, half), lambda i: (i + row // SPAN, 0)),
        input_output_aliases={3: 0} if held else {},
        compiler_params=params(1, 8),
        cost_estimate=cost(4 * rows * half, 8 * rows * half, 0),
        name="finish",
    )(base, keep, far, *held)


def layer(
    tokens,
    norm_first,
    norm_mix,
    norm_second,
    gate_weight,
    up_weight,
    down_weight,
    gate_scale,
    up_scale,
    down_scale,
    u_weight,
    v_weight,
    u_scale,
    v_scale,
    ln_gain,
    ln_bias,
    spatial_weight,
    spatial_bias,
    out_weight,
    out_scale,
):
    chans = u_weight.shape[1]
    width = 2 * tokens.shape[1]

    def number(x):
        return x.reshape(1).astype(jnp.int32)

    core = number(lax.axis_index("tp"))
    rep = lax.axis_index("rep")
    at = number(2 * lax.axis_index(FS) + rep)

    colors = prepare(
        number(rep),
        gate_weight,
        up_weight,
        down_weight.T,
        u_weight,
        v_weight,
        out_weight.T,
        gate_scale,
        up_scale,
        down_scale,
        u_scale,
        v_scale,
        out_scale,
    )
    one, two = gather(colors)

    count = tokens.shape[0]
    chunks = (slice(0, CHUNK), slice(CHUNK, count))
    own, other = tokens, other_core(tokens)
    hidden, first = first_hidden(core, at, own, other, norm_first[None], one)
    early, late, others = first_down(at, hidden, width, two)

    fars = [other_core(x) for x in (early, late)]
    mids = [
        gates(core, own[c], other[c], term, far, norm_mix[None], others, chans)
        for c, term, far in zip(chunks, (early, late), fars)
    ]
    terms = [
        mix(
            act,
            sums,
            other_core(sums),
            ln_gain[None],
            ln_bias[None],
            spatial_weight,
            spatial_bias.T,
            others,
        )
        for _, act, sums in mids
    ]
    fars = [other_core(x) for x in terms]
    ends = [
        second_pass(core, middle, term, far, norm_second[None], first, others)
        for (middle, _, _), term, far in zip(mids, terms, fars)
    ]
    fars = [other_core(x[0]) for x in ends]
    result = None
    for c, far, (_, keep, base) in zip(chunks, fars, ends):
        result = finish(base, keep, far, count, c.start, result)
    return result


def solution(mesh):
    torus = Mesh(
        mesh.devices.reshape(mesh.shape["rep"], 2, 4, 4, mesh.shape["tp"]),
        ("rep", "fs_0", "fs_1", "fs_2", "tp"),
    )
    in_specs = (
        P(REP_FS, "tp"),
        P(),
        P(),
        P(),
        P(FS, "tp"),
        P(FS, "tp"),
        P("tp", FS),
        P("tp"),
        P("tp"),
        P(FS),
        P(FS, "tp"),
        P(FS, "tp"),
        P("tp"),
        P("tp"),
        P("tp"),
        P("tp"),
        P("tp", None, None),
        P("tp", None),
        P("tp", FS),
        P(FS),
    )
    out_specs = P(REP_FS, "tp")
    return jax.shard_map(layer, mesh=torus, in_specs=in_specs, out_specs=out_specs, check_vma=False)
```

```python
import functools

import jax
import jax.numpy as jnp
from jax import lax
from jax.experimental import pallas as pl
from jax.experimental.pallas import tpu as pltpu
from jax.sharding import Mesh
from jax.sharding import PartitionSpec as P


BW = 1024
SPAN = 128
FS = ("fs_0", "fs_1", "fs_2")
REP_FS = ("rep", "fs_0", "fs_1", "fs_2")
LANES = 128
WIDE = 512
HALF_ROWS = 32
FIRST = (4, 4, 4, 4, 3, 3)
OTHERS = (4, 4, 4, 3, 4, 4)
RINGS = (("fs_2", 1), ("fs_1", 1), ("z", 1), ("fs_2", 3), ("fs_1", 3), ("z", 3))
PLACES = (2, 8, 32, 6, 24, 33)
ROUNDS = (
    (0, 4, 5, 3, 2, 1),
    (0, 4, 3, 5, 1, 2),
    (1, 5, 4, 2, 3, 0),
    (1, 5, 2, 4, 0, 3),
    (2, 3, 1, 0, 5, 4),
    (2, 3, 0, 1, 4, 5),
)

EPS = 1e-06


def other_core(x):
    return lax.ppermute(x, "tp", [(0, 1), (1, 0)])


def normed_rows(values, gain):
    factor = lax.rsqrt(jnp.mean(values * values, axis=1, keepdims=True) + EPS)
    return (values * factor * gain).astype(jnp.bfloat16)


def dot(left, right):
    return jnp.dot(left, right, preferred_element_type=jnp.float32)


def dot_rows(left, rows):
    return lax.dot_general(
        left, rows, (((1,), (1,)), ((), ())), preferred_element_type=jnp.float32
    )


def gelu(a):
    return 0.5 * a * (1.0 + jnp.tanh(0.7978845608028654 * (a + 0.044715 * a * a * a)))


def spec(block, index):
    return pl.BlockSpec(block, index)


def whole(shape):
    return pl.BlockSpec(shape, lambda *_: (0,) * len(shape))


ANY = pl.BlockSpec(memory_space=pl.ANY)


def params(steps):
    return pltpu.CompilerParams(
        dimension_semantics=("arbitrary",) * steps, vmem_limit_bytes=60 * 1024 * 1024
    )


def cost(flops, moved, special):
    return pl.CostEstimate(flops=flops, bytes_accessed=moved, transcendentals=special)


def exchange(x, color, turn):
    name, flip = RINGS[ROUNDS[color][turn]]
    axis = ("rep", "fs_0") if name == "z" else name
    return lax.ppermute(x, axis, [(i, i ^ flip) for i in range(4)])


def place(color, slot):
    at = 0
    for turn in range(6):
        if slot >> turn & 1:
            at ^= PLACES[ROUNDS[color][turn]]
    return at


def starts(widths):
    ends = [0]
    for n in widths:
        ends.append(ends[-1] + n * LANES)
    return ends


PAIRS = [(p, t + k) for t in (0, 2, 4, 6) for p in (0, 1) for k in (0, 1)]
PAIRS += [(0, 8), (0, 9), (1, 8), (1, 9), (0, 10), (1, 10)]


def prepare_kernel(rep, *refs):
    inputs, colors, held, sems = refs[:12], refs[12:15], refs[15:27], refs[27]
    copies = [
        pltpu.make_async_copy(x, y, sems.at[k]) for k, (x, y) in enumerate(zip(inputs, held))
    ]
    for copy in copies:
        copy.start()
    for copy in copies:
        copy.wait()
    gate, up, down, u, v, out, gate_s, up_s, down_s, u_s, v_s, out_s = held
    rows = pl.ds(pl.multiple_of(rep[0] * HALF_ROWS, HALF_ROWS), HALF_ROWS)
    low = jnp.bfloat16

    def across(scale):
        return scale[...][None, :]

    def down_rows(scale):
        size = scale.shape[0]
        row = lax.broadcasted_iota(jnp.int32, (HALF_ROWS, size), 0) + rep[0] * HALF_ROWS
        column = lax.broadcasted_iota(jnp.int32, (HALF_ROWS, size), 1)
        return jnp.sum(jnp.where(row == column, across(scale), 0.0), axis=1, keepdims=True)

    pair = ((gate[rows, :] * across(gate_s)).astype(low), (up[rows, :] * across(up_s)).astype(low))
    firsts = [pair[p][:, t * LANES : (t + 1) * LANES] for p, t in PAIRS]
    rest = jnp.concatenate(
        [
            (out[rows, :] * down_rows(out_s)).astype(low),
            (u[rows, :] * across(u_s)).astype(low),
            (v[rows, :] * across(v_s)).astype(low),
            (down[rows, :] * down_rows(down_s)).astype(low),
        ],
        axis=1,
    )
    at, begin = 0, starts(OTHERS)
    mine = []
    for c in range(6):
        mine.append(firsts[at : at + FIRST[c]] + [rest[:, begin[c] : begin[c + 1]]])
        at += FIRST[c]
    for pair, ref in enumerate(colors):
        ref[...] = jnp.concatenate(mine[2 * pair] + mine[2 * pair + 1], axis=1)


WIDTHS = [(a + b) * LANES for a, b in zip(FIRST, OTHERS)]
VMEM = pl.BlockSpec(memory_space=pltpu.VMEM)
SMEM = pl.BlockSpec(memory_space=pltpu.SMEM)
HBM = pl.BlockSpec(memory_space=pltpu.HBM)


def prepare(rep, *arrays):
    pairs = [WIDTHS[k] + WIDTHS[k + 1] for k in (0, 2, 4)]
    return pl.pallas_call(
        prepare_kernel,
        out_shape=[jax.ShapeDtypeStruct((HALF_ROWS, n), jnp.bfloat16) for n in pairs],
        in_specs=[SMEM] + [HBM] * len(arrays),
        out_specs=[VMEM] * 3,
        scratch_shapes=[pltpu.VMEM(x.shape, x.dtype) for x in arrays]
        + [pltpu.SemaphoreType.DMA((len(arrays),))],
        compiler_params=pltpu.CompilerParams(vmem_limit_bytes=60 * 1024 * 1024),
        name="prepare",
    )(rep, *arrays)


def join_kernel(cuts, *refs):
    sources = (len(refs) - len(cuts)) // 2
    for joined, (source, begin, end) in zip(refs[2 * sources :], cuts):
        held, arrived = refs[source], refs[sources + source]
        rows = held.shape[0]
        joined[pl.ds(0, rows), :] = held[:, begin:end]
        joined[pl.ds(rows, rows), :] = arrived[:, begin:end]


def join(held, arrived, cuts=None):
    rows, low = held[0].shape[0], jnp.bfloat16
    if cuts is None:
        cuts = [(k, 0, x.shape[1]) for k, x in enumerate(held)]
    return pl.pallas_call(
        functools.partial(join_kernel, cuts),
        out_shape=[jax.ShapeDtypeStruct((2 * rows, b - a), low) for _, a, b in cuts],
        in_specs=[VMEM] * (2 * len(held)),
        out_specs=[VMEM] * len(cuts),
        compiler_params=pltpu.CompilerParams(vmem_limit_bytes=16 * 1024 * 1024),
        name="join",
    )(*held, *arrived)


def gather(pairs):
    ready = []
    for p, x in enumerate(pairs):
        (held,) = join([x], [exchange(x, 2 * p, 0)])
        edge = WIDTHS[2 * p]
        cuts = [(0, 0, edge), (0, edge, held.shape[1])]
        held = join([held], [exchange(held, 2 * p, 1)], cuts)
        for turn in (2, 3):
            held = join(held, [exchange(y, 2 * p + k, turn) for k, y in enumerate(held)])
        ready.append((held, [exchange(y, 2 * p + k, 4) for k, y in enumerate(held)]))
    groups = []
    for g in range(2):
        pieces = []
        for p, (held, arrived) in enumerate(ready):
            cuts = []
            for k, y in enumerate(held):
                edge = FIRST[2 * p + k] * LANES
                cuts.append((k, edge, y.shape[1]) if g else (k, 0, edge))
            halves = join(held, arrived, cuts)
            for k, y in enumerate(halves):
                pieces += [y, exchange(y, 2 * p + k, 5)]
        groups.append(pieces)
    return groups


def place_blocks(at, pieces, weight, sems, widths, colors, first=0):
    begin = starts(widths)
    for c in colors:
        columns = pl.ds(begin[c], widths[c] * LANES)
        for k in range(2):

            def copy_four(high, carry, c=c, k=k, columns=columns):
                moved = at ^ place(first + c, 32 * k)
                for bit in range(3):
                    moved = moved ^ ((high >> bit & 1) * place(first + c, 4 << bit))
                for low in range(4):
                    to = (moved ^ place(first + c, low)) * HALF_ROWS
                    origin = (high * 4 + low) * HALF_ROWS
                    pltpu.make_async_copy(
                        pieces[2 * c + k].at[
                            pl.ds(pl.multiple_of(origin, HALF_ROWS), HALF_ROWS), :
                        ],
                        weight.at[pl.ds(pl.multiple_of(to, HALF_ROWS), HALF_ROWS), columns],
                        sems.at[c],
                    ).start()
                return carry

            lax.fori_loop(0, 8, copy_four, 0)


def wait_color(weight, sems, widths, c):
    columns = pl.ds(starts(widths)[c], widths[c] * LANES)
    part = weight.at[:, columns]
    pltpu.make_async_copy(part, part, sems.at[c]).wait()


def silu_product(gate, up):
    return (gate / (1.0 + jnp.exp(-gate)) * up).astype(jnp.bfloat16)


def narrow_step(normed, weight):
    both = dot(normed, weight)
    tile = [both[:, k * LANES : (k + 1) * LANES] for k in range(6)]
    gate = jnp.concatenate([tile[0], tile[1], tile[4]], axis=1)
    up = jnp.concatenate([tile[2], tile[3], tile[5]], axis=1)
    return silu_product(gate, up)


def hidden_step(step, normed, weight, hidden):
    @pl.when((step >= 0) & (step < 4))
    def _():
        columns = pl.ds(pl.multiple_of(step * WIDE, WIDE), WIDE)
        both = dot(normed[...], weight[:, columns])
        to = pl.ds(pl.multiple_of(step * (WIDE // 2), WIDE // 2), WIDE // 2)
        hidden[:, to] = silu_product(both[:, : WIDE // 2], both[:, WIDE // 2 :])

    @pl.when(step == 4)
    def _():
        hidden[:, 2 * WIDE :] = narrow_step(normed[...], weight[:, 4 * WIDE :])


def first_kernel(core, at, own, other, gain, *rest):
    pieces, (hidden, kept, weight, normed, sems, out_sem) = rest[:12], rest[12:]
    step = pl.program_id(0)

    @pl.when(step == 0)
    def _():
        place_blocks(at[0], pieces, weight, sems, FIRST, range(6))
        left = jnp.where(core[0] == 0, own[...], other[...])
        right = jnp.where(core[0] == 0, other[...], own[...])
        values = jnp.concatenate([left, right], axis=1).astype(jnp.float32)
        normed[...] = normed_rows(values, gain[...])

    for c in range(6):

        @pl.when(step == min(c, 4))
        def _():
            wait_color(weight, sems, FIRST, c)

    hidden_step(step, normed, weight, hidden)

    @pl.when(step == 4)
    def _():
        copy = pltpu.make_async_copy(weight, kept, out_sem)
        copy.start()
        copy.wait()


def first_hidden(core, at, own, other, gain, pieces):
    count, half = own.shape
    width = 2 * half
    columns = sum(FIRST) * LANES
    units = columns // 2
    return pl.pallas_call(
        first_kernel,
        out_shape=[
            jax.ShapeDtypeStruct((count, units), jnp.bfloat16),
            jax.ShapeDtypeStruct((width, columns), jnp.bfloat16),
        ],
        grid_spec=pltpu.PrefetchScalarGridSpec(
            num_scalar_prefetch=2,
            grid=(5,),
            in_specs=[whole((count, half)), whole((count, half)), whole((1, width))] + [ANY] * 12,
            out_specs=[whole((count, units)), ANY],
            scratch_shapes=[
                pltpu.VMEM((width, columns), jnp.bfloat16),
                pltpu.VMEM((count, width), jnp.bfloat16),
                pltpu.SemaphoreType.DMA((6,)),
                pltpu.SemaphoreType.DMA,
            ],
        ),
        compiler_params=params(1),
        cost_estimate=cost(2 * count * width * columns, 4 * width * columns, count * units),
        name="first_hidden",
    )(core, at, own, other, gain, *pieces)


MIXER, DOWN = OTHERS[:3], OTHERS[3:]


def place_blocks_of(at, pieces, weight, sems, widths, first):
    place_blocks(at, pieces, weight, sems, widths, range(len(widths)), first)


def down_kernel(at, hidden, *rest):
    pieces, (term, kept, weight, sems, out_sem) = rest[:6], rest[6:]
    step = pl.program_id(0)
    copy = pltpu.make_async_copy(weight, kept, out_sem)

    @pl.when(step == 0)
    def _():
        place_blocks_of(at[0], pieces, weight, sems, DOWN, 3)
        for c in range(3):
            wait_color(weight, sems, DOWN, c)
        copy.start()

    rows = pl.ds(pl.multiple_of(step * WIDE, WIDE), WIDE)
    term[...] = dot_rows(hidden[...], weight[rows, :]).astype(jnp.bfloat16)

    @pl.when(step == pl.num_programs(0) - 1)
    def _():
        copy.wait()


def first_down(at, hidden, width, pieces):
    count, units = hidden.shape
    return pl.pallas_call(
        down_kernel,
        out_shape=[
            jax.ShapeDtypeStruct((count, width), jnp.bfloat16),
            jax.ShapeDtypeStruct((width, units), jnp.bfloat16),
        ],
        grid_spec=pltpu.PrefetchScalarGridSpec(
            num_scalar_prefetch=1,
            grid=(width // WIDE,),
            in_specs=[whole((count, units))] + [ANY] * 6,
            out_specs=[spec((count, WIDE), lambda j, a: (0, j)), ANY],
            scratch_shapes=[
                pltpu.VMEM((width, units), jnp.bfloat16),
                pltpu.SemaphoreType.DMA((3,)),
                pltpu.SemaphoreType.DMA,
            ],
        ),
        compiler_params=params(1),
        cost_estimate=cost(2 * count * width * units, 4 * width * units, 0),
        name="first_down",
    )(at, hidden, *pieces)


def assemble_kernel(at, *rest):
    pieces, (kept, weight, sems, out_sems) = rest[:6], rest[6:]
    place_blocks_of(at[0], pieces, weight, sems, MIXER, 0)
    begin = starts(MIXER)
    copies = []
    for c in range(3):
        wait_color(weight, sems, MIXER, c)
        columns = pl.ds(begin[c], MIXER[c] * LANES)
        copy = pltpu.make_async_copy(weight.at[:, columns], kept.at[:, columns], out_sems.at[c])
        copy.start()
        copies.append(copy)
    for copy in copies:
        copy.wait()


def assemble(at, width, pieces):
    shape = (width, sum(MIXER) * LANES)
    return pl.pallas_call(
        assemble_kernel,
        out_shape=jax.ShapeDtypeStruct(shape, jnp.bfloat16),
        grid_spec=pltpu.PrefetchScalarGridSpec(
            num_scalar_prefetch=1,
            grid=(1,),
            in_specs=[ANY] * 6,
            out_specs=ANY,
            scratch_shapes=[
                pltpu.VMEM(shape, jnp.bfloat16),
                pltpu.SemaphoreType.DMA((3,)),
                pltpu.SemaphoreType.DMA((3,)),
            ],
        ),
        compiler_params=params(1),
        cost_estimate=cost(5 * 10**9, 8 * shape[0] * shape[1], 0),
        name="assemble",
    )(at, *pieces)


def gates_kernel(blocks, core, own, other, term, far, gain, rows, middle, act, sums, normed):
    step = pl.program_id(0)

    @pl.when(step < blocks)
    def _():
        left = jnp.where(core[0] == 0, own[...], other[...])
        right = jnp.where(core[0] == 0, other[...], own[...])
        values = jnp.concatenate([left, right], axis=1).astype(jnp.float32)
        values = values + 0.5 * (term[...].astype(jnp.float32) + far[...].astype(jnp.float32))
        mid = values.astype(jnp.bfloat16)
        middle[...] = mid
        block = pl.ds(pl.multiple_of(step * SPAN, SPAN), SPAN)
        normed[block, :] = normed_rows(mid.astype(jnp.float32), gain[...])

    @pl.when(step >= blocks)
    def _():
        acted = gelu(dot(normed[...], rows[...]))
        act[0] = acted

        @pl.when(step == blocks)
        def _():
            lane = lax.broadcasted_iota(jnp.int32, sums.shape, 1)
            total = jnp.sum(acted, axis=1, keepdims=True)
            squares = jnp.sum(acted * acted, axis=1, keepdims=True)
            sums[...] = jnp.where(lane == 0, total, squares)


def gates(core, own, other, term, far, gain, weight, chans):
    count, half = own.shape
    width = 2 * half
    blocks = count // SPAN

    def block(columns):
        return spec((SPAN, columns), lambda i, c: (jnp.minimum(i, blocks - 1), 0))

    return pl.pallas_call(
        functools.partial(gates_kernel, blocks),
        out_shape=[
            jax.ShapeDtypeStruct((count, width), jnp.bfloat16),
            jax.ShapeDtypeStruct((2, count, chans), jnp.float32),
            jax.ShapeDtypeStruct((count, LANES), jnp.float32),
        ],
        grid_spec=pltpu.PrefetchScalarGridSpec(
            num_scalar_prefetch=1,
            grid=(blocks + 2,),
            in_specs=[
                block(half),
                block(half),
                block(width),
                block(width),
                whole((1, width)),
                spec((width, chans), lambda i, c: (0, 2 - jnp.maximum(i - blocks, 0))),
            ],
            out_specs=[
                block(width),
                spec((1, count, chans), lambda i, c: (jnp.maximum(i - blocks, 0), 0, 0)),
                whole((count, LANES)),
            ],
            scratch_shapes=[pltpu.VMEM((count, width), jnp.bfloat16)],
        ),
        compiler_params=params(1),
        cost_estimate=cost(4 * count * width * chans, 4 * width * chans, 2 * count * chans),
        name="gates",
    )(core, own, other, term, far, gain, weight)


def mix_kernel(act, sums, far, gain, bias, weight, shift, rows, term, mixed):
    groups = weight.shape[0]

    @pl.when(pl.program_id(0) == 0)
    def _():
        at = lax.broadcasted_iota(jnp.int32, (SPAN, SPAN), 0)
        source = lax.broadcasted_iota(jnp.int32, (SPAN, SPAN), 1)
        masked = [
            jnp.where(source <= at, weight[g], jnp.zeros_like(weight[g])) for g in range(groups)
        ]
        count, chans = mixed.shape
        wide = chans // groups
        column = [
            jnp.sum(jnp.where(source == at, shift[g : g + 1, :], 0.0), axis=1, keepdims=True)
            for g in range(groups)
        ]
        for n in range(count // SPAN):
            block = pl.ds(n * SPAN, SPAN)
            totals = (sums[block, :] + far[block, :]) / BW
            v_mean = totals[:, 0:1]
            v_var = totals[:, 1:2] - v_mean * v_mean
            v_normed = (act[0, block, :] - v_mean) * lax.rsqrt(v_var + EPS) * gain[...] + bias[...]
            v_normed = v_normed.astype(jnp.bfloat16)
            spatial = [
                dot(masked[g], v_normed[:, g * wide : (g + 1) * wide]) + column[g]
                for g in range(groups)
            ]
            product = act[1, block, :] * jnp.concatenate(spatial, axis=1)
            mixed[block, :] = product.astype(jnp.bfloat16)

    term[...] = dot_rows(mixed[...], rows[...]).astype(jnp.bfloat16)


def mix(act, sums, far, gain, bias, weight, shift, rows):
    _, count, chans = act.shape
    width = rows.shape[0]
    groups = weight.shape[0]
    return pl.pallas_call(
        mix_kernel,
        out_shape=jax.ShapeDtypeStruct((count, width), jnp.bfloat16),
        grid=(width // WIDE,),
        in_specs=[
            whole(act.shape),
            whole((count, LANES)),
            whole((count, LANES)),
            whole((1, chans)),
            whole((1, chans)),
            whole((groups, SPAN, SPAN)),
            whole((groups, SPAN)),
            spec((WIDE, chans), lambda j: (j, 0)),
        ],
        out_specs=spec((count, WIDE), lambda j: (0, j)),
        scratch_shapes=[pltpu.VMEM((count, chans), jnp.bfloat16)],
        compiler_params=params(1),
        cost_estimate=cost(2 * count * width * chans, 2 * width * chans, count),
        name="mix",
    )(act, sums, far, gain, bias, weight, shift, rows)


def second_kernel(
    blocks,
    core,
    middle,
    term,
    far,
    gain,
    first,
    others,
    send,
    keep,
    base,
    normed,
    hidden,
    wide,
    down,
    sems,
):
    step = pl.program_id(0)
    steps = 5
    outs = down.shape[0] // WIDE
    cuts = [pl.ds(k * WIDE, WIDE) for k in range(4)] + [pl.ds(4 * WIDE, 6 * LANES)]
    copies = [
        pltpu.make_async_copy(first.at[:, cut], wide.at[:, cut], sems.at[k])
        for k, cut in enumerate(cuts)
    ]
    copies.append(pltpu.make_async_copy(others, down, sems.at[steps]))

    for k, copy in enumerate(copies):

        @pl.when(step == k)
        def _():
            copy.start()

        @pl.when(step == blocks + k)
        def _():
            copy.wait()

    @pl.when(step < blocks)
    def _():
        values = middle[...].astype(jnp.float32) + (
            term[...].astype(jnp.float32) + far[...].astype(jnp.float32)
        )
        second = values.astype(jnp.bfloat16)
        half = second.shape[1] // 2
        base[...] = jnp.where(core[0] == 0, second[:, :half], second[:, half:])
        block = pl.ds(pl.multiple_of(step * SPAN, SPAN), SPAN)
        normed[block, :] = normed_rows(second.astype(jnp.float32), gain[...])

    hidden_step(step - blocks, normed, wide, hidden)

    @pl.when(step >= blocks + steps)
    def _():
        n = step - blocks - steps
        mine = jnp.where(n < outs // 2, 1 - core[0], core[0])
        row = mine * (outs // 2) + lax.rem(n, outs // 2)
        rows = pl.ds(pl.multiple_of(row * WIDE, WIDE), WIDE)
        part = dot_rows(hidden[...], down[rows, :]).astype(jnp.bfloat16)

        @pl.when(n < outs // 2)
        def _():
            send[...] = part

        @pl.when(n >= outs // 2)
        def _():
            keep[...] = part


def second_pass(core, middle, term, far, gain, first, others):
    count, width = middle.shape
    half = width // 2
    columns = first.shape[1]
    units = columns // 2
    outs = width // WIDE
    sent = outs // 2
    blocks = count // SPAN
    done = blocks + 5

    def block(size):
        return spec((SPAN, size), lambda j, c: (jnp.minimum(j, blocks - 1), 0))

    return pl.pallas_call(
        functools.partial(second_kernel, blocks),
        out_shape=[jax.ShapeDtypeStruct((count, half), jnp.bfloat16)] * 3,
        grid_spec=pltpu.PrefetchScalarGridSpec(
            num_scalar_prefetch=1,
            grid=(done + outs,),
            in_specs=[block(width)] * 3 + [whole((1, width)), ANY, ANY],
            out_specs=[
                spec((count, WIDE), lambda j, c: (0, jnp.clip(j - done, 0, sent - 1))),
                spec((count, WIDE), lambda j, c: (0, jnp.maximum(j - done - sent, 0))),
                block(half),
            ],
            scratch_shapes=[
                pltpu.VMEM((count, width), jnp.bfloat16),
                pltpu.VMEM((count, units), jnp.bfloat16),
                pltpu.VMEM((width, columns), jnp.bfloat16),
                pltpu.VMEM((width, units), jnp.bfloat16),
                pltpu.SemaphoreType.DMA((6,)),
            ],
        ),
        compiler_params=params(1),
        cost_estimate=cost(6 * count * width * units, 6 * width * units, count * units),
        name="second_pass",
    )(core, middle, term, far, gain, first, others)


def finish_kernel(base, keep, far, result):
    last = keep[...].astype(jnp.float32) + far[...].astype(jnp.float32)
    result[...] = (base[...].astype(jnp.float32) + 0.5 * last).astype(jnp.bfloat16)


def finish(base, keep, far):
    count, half = base.shape
    block = spec((SPAN, half), lambda i: (i, 0))
    return pl.pallas_call(
        finish_kernel,
        out_shape=jax.ShapeDtypeStruct((count, half), jnp.bfloat16),
        grid=(count // SPAN,),
        in_specs=[block] * 3,
        out_specs=block,
        compiler_params=params(1),
        cost_estimate=cost(4 * count * half, 8 * count * half, 0),
        name="finish",
    )(base, keep, far)


def layer(
    tokens,
    norm_first,
    norm_mix,
    norm_second,
    gate_weight,
    up_weight,
    down_weight,
    gate_scale,
    up_scale,
    down_scale,
    u_weight,
    v_weight,
    u_scale,
    v_scale,
    ln_gain,
    ln_bias,
    spatial_weight,
    spatial_bias,
    out_weight,
    out_scale,
):
    chans = u_weight.shape[1]
    width = 2 * tokens.shape[1]

    def number(x):
        return x.reshape(1).astype(jnp.int32)

    core = number(lax.axis_index("tp"))
    rep = lax.axis_index("rep")
    at = number(2 * lax.axis_index(FS) + rep)

    colors = prepare(
        number(rep),
        gate_weight,
        up_weight,
        down_weight.T,
        u_weight,
        v_weight,
        out_weight.T,
        gate_scale,
        up_scale,
        down_scale,
        u_scale,
        v_scale,
        out_scale,
    )
    one, two = gather(colors)

    own, other = tokens, other_core(tokens)
    hidden, first = first_hidden(core, at, own, other, norm_first[None], one)
    term, down = first_down(at, hidden, width, two[6:])
    far = other_core(term)
    mixer = assemble(at, width, two[:6])
    middle, act, sums = gates(core, own, other, term, far, norm_mix[None], mixer, chans)
    term = mix(
        act,
        sums,
        other_core(sums),
        ln_gain[None],
        ln_bias[None],
        spatial_weight,
        spatial_bias,
        mixer,
    )
    send, keep, base = second_pass(
        core, middle, term, other_core(term), norm_second[None], first, down
    )
    return finish(base, keep, other_core(send))


def solution(mesh):
    torus = Mesh(
        mesh.devices.reshape(mesh.shape["rep"], 2, 4, 4, mesh.shape["tp"]),
        ("rep", "fs_0", "fs_1", "fs_2", "tp"),
    )
    in_specs = (
        P(REP_FS, "tp"),
        P(),
        P(),
        P(),
        P(FS, "tp"),
        P(FS, "tp"),
        P("tp", FS),
        P("tp"),
        P("tp"),
        P(FS),
        P(FS, "tp"),
        P(FS, "tp"),
        P("tp"),
        P("tp"),
        P("tp"),
        P("tp"),
        P("tp", None, None),
        P("tp", None),
        P("tp", FS),
        P(FS),
    )
    out_specs = P(REP_FS, "tp")
    return jax.shard_map(layer, mesh=torus, in_specs=in_specs, out_specs=out_specs, check_vma=False)
```

```python
import functools

import jax
import jax.numpy as jnp
from jax import lax
from jax.experimental import pallas as pl
from jax.experimental.pallas import tpu as pltpu
from jax.sharding import Mesh
from jax.sharding import PartitionSpec as P


BW = 1024
SPAN = 128
FS = ("fs_0", "fs_1", "fs_2")
REP_FS = ("rep", "fs_0", "fs_1", "fs_2")
LANES = 128
WIDE = 512
HALF_ROWS = 32
FIRST = (4, 4, 4, 4, 3, 3)
OTHERS = (4, 4, 4, 3, 4, 4)
RINGS = (("fs_2", 1), ("fs_1", 1), ("z", 1), ("fs_2", 3), ("fs_1", 3), ("z", 3))
PLACES = (2, 8, 32, 6, 24, 33)
ROUNDS = (
    (0, 4, 5, 3, 2, 1),
    (0, 4, 3, 5, 1, 2),
    (1, 5, 4, 2, 3, 0),
    (1, 5, 2, 4, 0, 3),
    (2, 3, 1, 0, 5, 4),
    (2, 3, 0, 1, 4, 5),
)

EPS = 1e-06


def other_core(x):
    return lax.ppermute(x, "tp", [(0, 1), (1, 0)])


def normed_rows(values, gain):
    factor = lax.rsqrt(jnp.mean(values * values, axis=1, keepdims=True) + EPS)
    return (values * factor * gain).astype(jnp.bfloat16)


def dot(left, right):
    return jnp.dot(left, right, preferred_element_type=jnp.float32)


def dot_rows(left, rows):
    return lax.dot_general(
        left, rows, (((1,), (1,)), ((), ())), preferred_element_type=jnp.float32
    )


def gelu(a):
    return 0.5 * a * (1.0 + jnp.tanh(0.7978845608028654 * (a + 0.044715 * a * a * a)))


def spec(block, index):
    return pl.BlockSpec(block, index)


def whole(shape):
    return pl.BlockSpec(shape, lambda *_: (0,) * len(shape))


ANY = pl.BlockSpec(memory_space=pl.ANY)


def params(steps):
    return pltpu.CompilerParams(
        dimension_semantics=("arbitrary",) * steps, vmem_limit_bytes=60 * 1024 * 1024
    )


def cost(flops, moved, special):
    return pl.CostEstimate(flops=flops, bytes_accessed=moved, transcendentals=special)


def exchange(x, color, turn):
    name, flip = RINGS[ROUNDS[color][turn]]
    axis = ("rep", "fs_0") if name == "z" else name
    return lax.ppermute(x, axis, [(i, i ^ flip) for i in range(4)])


def place(color, slot):
    at = 0
    for turn in range(6):
        if slot >> turn & 1:
            at ^= PLACES[ROUNDS[color][turn]]
    return at


def starts(widths):
    ends = [0]
    for n in widths:
        ends.append(ends[-1] + n * LANES)
    return ends


PAIRS = [(p, t + k) for t in (0, 2, 4, 6) for p in (0, 1) for k in (0, 1)]
PAIRS += [(0, 8), (0, 9), (1, 8), (1, 9), (0, 10), (1, 10)]


def prepare_kernel(rep, *refs):
    inputs, colors, held, sems = refs[:12], refs[12:15], refs[15:27], refs[27]
    copies = [
        pltpu.make_async_copy(x, y, sems.at[k]) for k, (x, y) in enumerate(zip(inputs, held))
    ]
    for copy in copies:
        copy.start()
    for copy in copies:
        copy.wait()
    gate, up, down, u, v, out, gate_s, up_s, down_s, u_s, v_s, out_s = held
    rows = pl.ds(pl.multiple_of(rep[0] * HALF_ROWS, HALF_ROWS), HALF_ROWS)
    low = jnp.bfloat16

    def across(scale):
        return scale[...][None, :]

    def down_rows(scale):
        size = scale.shape[0]
        row = lax.broadcasted_iota(jnp.int32, (HALF_ROWS, size), 0) + rep[0] * HALF_ROWS
        column = lax.broadcasted_iota(jnp.int32, (HALF_ROWS, size), 1)
        return jnp.sum(jnp.where(row == column, across(scale), 0.0), axis=1, keepdims=True)

    pair = ((gate[rows, :] * across(gate_s)).astype(low), (up[rows, :] * across(up_s)).astype(low))
    firsts = [pair[p][:, t * LANES : (t + 1) * LANES] for p, t in PAIRS]
    rest = jnp.concatenate(
        [
            (out[rows, :] * down_rows(out_s)).astype(low),
            (u[rows, :] * across(u_s)).astype(low),
            (v[rows, :] * across(v_s)).astype(low),
            (down[rows, :] * down_rows(down_s)).astype(low),
        ],
        axis=1,
    )
    at, begin = 0, starts(OTHERS)
    mine = []
    for c in range(6):
        mine.append(firsts[at : at + FIRST[c]] + [rest[:, begin[c] : begin[c + 1]]])
        at += FIRST[c]
    for pair, ref in enumerate(colors):
        ref[...] = jnp.concatenate(mine[2 * pair] + mine[2 * pair + 1], axis=1)


WIDTHS = [(a + b) * LANES for a, b in zip(FIRST, OTHERS)]
VMEM = pl.BlockSpec(memory_space=pltpu.VMEM)
SMEM = pl.BlockSpec(memory_space=pltpu.SMEM)
HBM = pl.BlockSpec(memory_space=pltpu.HBM)


def prepare(rep, *arrays):
    pairs = [WIDTHS[k] + WIDTHS[k + 1] for k in (0, 2, 4)]
    return pl.pallas_call(
        prepare_kernel,
        out_shape=[jax.ShapeDtypeStruct((HALF_ROWS, n), jnp.bfloat16) for n in pairs],
        in_specs=[SMEM] + [HBM] * len(arrays),
        out_specs=[VMEM] * 3,
        scratch_shapes=[pltpu.VMEM(x.shape, x.dtype) for x in arrays]
        + [pltpu.SemaphoreType.DMA((len(arrays),))],
        compiler_params=pltpu.CompilerParams(vmem_limit_bytes=60 * 1024 * 1024),
        name="prepare",
    )(rep, *arrays)


def join_kernel(cuts, *refs):
    sources = (len(refs) - len(cuts)) // 2
    for joined, (source, begin, end) in zip(refs[2 * sources :], cuts):
        held, arrived = refs[source], refs[sources + source]
        rows = held.shape[0]
        joined[pl.ds(0, rows), :] = held[:, begin:end]
        joined[pl.ds(rows, rows), :] = arrived[:, begin:end]


def cut_kernel(*refs):
    for k in range(len(refs) // 2):
        refs[len(refs) // 2 + k][...] = refs[k][:, : refs[len(refs) // 2 + k].shape[1]]


def first_columns(arrays, widths):
    return pl.pallas_call(
        cut_kernel,
        out_shape=[
            jax.ShapeDtypeStruct((x.shape[0], n * LANES), x.dtype) for x, n in zip(arrays, widths)
        ],
        in_specs=[VMEM] * len(arrays),
        out_specs=[VMEM] * len(arrays),
        compiler_params=pltpu.CompilerParams(vmem_limit_bytes=16 * 1024 * 1024),
        name="first_columns",
    )(*arrays)


def join(held, arrived, cuts=None):
    rows, low = held[0].shape[0], jnp.bfloat16
    if cuts is None:
        cuts = [(k, 0, x.shape[1]) for k, x in enumerate(held)]
    return pl.pallas_call(
        functools.partial(join_kernel, cuts),
        out_shape=[jax.ShapeDtypeStruct((2 * rows, b - a), low) for _, a, b in cuts],
        in_specs=[VMEM] * (2 * len(held)),
        out_specs=[VMEM] * len(cuts),
        compiler_params=pltpu.CompilerParams(vmem_limit_bytes=16 * 1024 * 1024),
        name="join",
    )(*held, *arrived)


def gather(pairs):
    ready = []
    for p, x in enumerate(pairs):
        (held,) = join([x], [exchange(x, 2 * p, 0)])
        edge = WIDTHS[2 * p]
        cuts = [(0, 0, edge), (0, edge, held.shape[1])]
        held = join([held], [exchange(held, 2 * p, 1)], cuts)
        held = join(held, [exchange(y, 2 * p + k, 2) for k, y in enumerate(held)])
        arrived = [exchange(y, 2 * p + k, 3) for k, y in enumerate(held)]
        held = join(held, arrived)
        ready.append((held, [exchange(y, 2 * p + k, 4) for k, y in enumerate(held)]))
    one, two = [], []
    for p, (held, arrived) in enumerate(ready):
        kept = first_columns(held, FIRST[2 * p : 2 * p + 2])
        early = [exchange(x, 2 * p + k, 5) for k, x in enumerate(kept)]
        come = first_columns(arrived, FIRST[2 * p : 2 * p + 2])
        late = [exchange(x, 2 * p + k, 5) for k, x in enumerate(come)]
        for k in range(2):
            one += [kept[k], come[k], early[k], late[k]]
        cuts = [(k, FIRST[2 * p + k] * LANES, y.shape[1]) for k, y in enumerate(held)]
        halves = join(held, arrived, cuts)
        for k, y in enumerate(halves):
            two += [y, exchange(y, 2 * p + k, 5)]
    return one, two


def place_blocks(at, pieces, weight, sems, widths, colors, first=0):
    begin = starts(widths)
    parts = len(pieces) // len(widths)
    slots = 64 // parts
    for c in colors:
        columns = pl.ds(begin[c], widths[c] * LANES)
        for k in range(parts):

            def copy_four(high, carry, c=c, k=k, columns=columns):
                moved = at ^ place(first + c, slots * k)
                for bit in range(slots.bit_length() - 3):
                    moved = moved ^ ((high >> bit & 1) * place(first + c, 4 << bit))
                for low in range(4):
                    to = (moved ^ place(first + c, low)) * HALF_ROWS
                    origin = (high * 4 + low) * HALF_ROWS
                    pltpu.make_async_copy(
                        pieces[parts * c + k].at[
                            pl.ds(pl.multiple_of(origin, HALF_ROWS), HALF_ROWS), :
                        ],
                        weight.at[pl.ds(pl.multiple_of(to, HALF_ROWS), HALF_ROWS), columns],
                        sems.at[c],
                    ).start()
                return carry

            lax.fori_loop(0, slots // 4, copy_four, 0)


def wait_color(weight, sems, widths, c):
    columns = pl.ds(starts(widths)[c], widths[c] * LANES)
    part = weight.at[:, columns]
    pltpu.make_async_copy(part, part, sems.at[c]).wait()


def silu_product(gate, up):
    return (gate / (1.0 + jnp.exp(-gate)) * up).astype(jnp.bfloat16)


def narrow_step(normed, weight):
    both = dot(normed, weight)
    tile = [both[:, k * LANES : (k + 1) * LANES] for k in range(6)]
    gate = jnp.concatenate([tile[0], tile[1], tile[4]], axis=1)
    up = jnp.concatenate([tile[2], tile[3], tile[5]], axis=1)
    return silu_product(gate, up)


def hidden_step(step, normed, weight, hidden):
    @pl.when((step >= 0) & (step < 4))
    def _():
        columns = pl.ds(pl.multiple_of(step * WIDE, WIDE), WIDE)
        both = dot(normed[...], weight[:, columns])
        to = pl.ds(pl.multiple_of(step * (WIDE // 2), WIDE // 2), WIDE // 2)
        hidden[:, to] = silu_product(both[:, : WIDE // 2], both[:, WIDE // 2 :])

    @pl.when(step == 4)
    def _():
        hidden[:, 2 * WIDE :] = narrow_step(normed[...], weight[:, 4 * WIDE :])


def first_kernel(core, at, own, other, gain, *rest):
    pieces, (hidden, kept, weight, normed, sems, out_sem) = rest[:24], rest[24:]
    step = pl.program_id(0)

    @pl.when(step == 0)
    def _():
        place_blocks(at[0], pieces, weight, sems, FIRST, range(6))
        left = jnp.where(core[0] == 0, own[...], other[...])
        right = jnp.where(core[0] == 0, other[...], own[...])
        values = jnp.concatenate([left, right], axis=1).astype(jnp.float32)
        normed[...] = normed_rows(values, gain[...])

    for c in range(6):

        @pl.when(step == min(c, 4))
        def _():
            wait_color(weight, sems, FIRST, c)

    hidden_step(step, normed, weight, hidden)

    @pl.when(step == 4)
    def _():
        copy = pltpu.make_async_copy(weight, kept, out_sem)
        copy.start()
        copy.wait()


def first_hidden(core, at, own, other, gain, pieces):
    count, half = own.shape
    width = 2 * half
    columns = sum(FIRST) * LANES
    units = columns // 2
    return pl.pallas_call(
        first_kernel,
        out_shape=[
            jax.ShapeDtypeStruct((count, units), jnp.bfloat16),
            jax.ShapeDtypeStruct((width, columns), jnp.bfloat16),
        ],
        grid_spec=pltpu.PrefetchScalarGridSpec(
            num_scalar_prefetch=2,
            grid=(5,),
            in_specs=[whole((count, half)), whole((count, half)), whole((1, width))] + [ANY] * 24,
            out_specs=[whole((count, units)), ANY],
            scratch_shapes=[
                pltpu.VMEM((width, columns), jnp.bfloat16),
                pltpu.VMEM((count, width), jnp.bfloat16),
                pltpu.SemaphoreType.DMA((6,)),
                pltpu.SemaphoreType.DMA,
            ],
        ),
        compiler_params=params(1),
        cost_estimate=cost(2 * count * width * columns, 4 * width * columns, count * units),
        name="first_hidden",
    )(core, at, own, other, gain, *pieces)


MIXER, DOWN = OTHERS[:3], OTHERS[3:]


def place_blocks_of(at, pieces, weight, sems, widths, first):
    place_blocks(at, pieces, weight, sems, widths, range(len(widths)), first)


def down_kernel(at, hidden, *rest):
    pieces, (term, kept, weight, sems, out_sem) = rest[:6], rest[6:]
    step = pl.program_id(0)
    copy = pltpu.make_async_copy(weight, kept, out_sem)

    @pl.when(step == 0)
    def _():
        place_blocks_of(at[0], pieces, weight, sems, DOWN, 3)
        for c in range(3):
            wait_color(weight, sems, DOWN, c)
        copy.start()

    rows = pl.ds(pl.multiple_of(step * WIDE, WIDE), WIDE)
    term[...] = dot_rows(hidden[...], weight[rows, :]).astype(jnp.bfloat16)

    @pl.when(step == pl.num_programs(0) - 1)
    def _():
        copy.wait()


def first_down(at, hidden, width, pieces):
    count, units = hidden.shape
    return pl.pallas_call(
        down_kernel,
        out_shape=[
            jax.ShapeDtypeStruct((count, width), jnp.bfloat16),
            jax.ShapeDtypeStruct((width, units), jnp.bfloat16),
        ],
        grid_spec=pltpu.PrefetchScalarGridSpec(
            num_scalar_prefetch=1,
            grid=(width // WIDE,),
            in_specs=[whole((count, units))] + [ANY] * 6,
            out_specs=[spec((count, WIDE), lambda j, a: (0, j)), ANY],
            scratch_shapes=[
                pltpu.VMEM((width, units), jnp.bfloat16),
                pltpu.SemaphoreType.DMA((3,)),
                pltpu.SemaphoreType.DMA,
            ],
        ),
        compiler_params=params(1),
        cost_estimate=cost(2 * count * width * units, 4 * width * units, 0),
        name="first_down",
    )(at, hidden, *pieces)


def assemble_kernel(at, *rest):
    pieces, (kept, weight, sems, out_sems) = rest[:6], rest[6:]
    place_blocks_of(at[0], pieces, weight, sems, MIXER, 0)
    begin = starts(MIXER)
    copies = []
    for c in range(3):
        wait_color(weight, sems, MIXER, c)
        columns = pl.ds(begin[c], MIXER[c] * LANES)
        copy = pltpu.make_async_copy(weight.at[:, columns], kept.at[:, columns], out_sems.at[c])
        copy.start()
        copies.append(copy)
    for copy in copies:
        copy.wait()


def assemble(at, width, pieces):
    shape = (width, sum(MIXER) * LANES)
    return pl.pallas_call(
        assemble_kernel,
        out_shape=jax.ShapeDtypeStruct(shape, jnp.bfloat16),
        grid_spec=pltpu.PrefetchScalarGridSpec(
            num_scalar_prefetch=1,
            grid=(1,),
            in_specs=[ANY] * 6,
            out_specs=ANY,
            scratch_shapes=[
                pltpu.VMEM(shape, jnp.bfloat16),
                pltpu.SemaphoreType.DMA((3,)),
                pltpu.SemaphoreType.DMA((3,)),
            ],
        ),
        compiler_params=params(1),
        cost_estimate=cost(5 * 10**9, 8 * shape[0] * shape[1], 0),
        name="assemble",
    )(at, *pieces)


def gates_kernel(blocks, core, own, other, term, far, gain, rows, middle, act, sums, normed):
    step = pl.program_id(0)

    @pl.when(step < blocks)
    def _():
        left = jnp.where(core[0] == 0, own[...], other[...])
        right = jnp.where(core[0] == 0, other[...], own[...])
        values = jnp.concatenate([left, right], axis=1).astype(jnp.float32)
        values = values + 0.5 * (term[...].astype(jnp.float32) + far[...].astype(jnp.float32))
        mid = values.astype(jnp.bfloat16)
        middle[...] = mid
        block = pl.ds(pl.multiple_of(step * SPAN, SPAN), SPAN)
        normed[block, :] = normed_rows(mid.astype(jnp.float32), gain[...])

    @pl.when(step >= blocks)
    def _():
        acted = gelu(dot(normed[...], rows[...]))
        act[0] = acted

        @pl.when(step == blocks)
        def _():
            lane = lax.broadcasted_iota(jnp.int32, sums.shape, 1)
            total = jnp.sum(acted, axis=1, keepdims=True)
            squares = jnp.sum(acted * acted, axis=1, keepdims=True)
            sums[...] = jnp.where(lane == 0, total, squares)


def gates(core, own, other, term, far, gain, weight, chans):
    count, half = own.shape
    width = 2 * half
    blocks = count // SPAN

    def block(columns):
        return spec((SPAN, columns), lambda i, c: (jnp.minimum(i, blocks - 1), 0))

    return pl.pallas_call(
        functools.partial(gates_kernel, blocks),
        out_shape=[
            jax.ShapeDtypeStruct((count, width), jnp.bfloat16),
            jax.ShapeDtypeStruct((2, count, chans), jnp.float32),
            jax.ShapeDtypeStruct((count, LANES), jnp.float32),
        ],
        grid_spec=pltpu.PrefetchScalarGridSpec(
            num_scalar_prefetch=1,
            grid=(blocks + 2,),
            in_specs=[
                block(half),
                block(half),
                block(width),
                block(width),
                whole((1, width)),
                spec((width, chans), lambda i, c: (0, 2 - jnp.maximum(i - blocks, 0))),
            ],
            out_specs=[
                block(width),
                spec((1, count, chans), lambda i, c: (jnp.maximum(i - blocks, 0), 0, 0)),
                whole((count, LANES)),
            ],
            scratch_shapes=[pltpu.VMEM((count, width), jnp.bfloat16)],
        ),
        compiler_params=params(1),
        cost_estimate=cost(4 * count * width * chans, 4 * width * chans, 2 * count * chans),
        name="gates",
    )(core, own, other, term, far, gain, weight)


def mix_kernel(act, sums, far, gain, bias, weight, shift, rows, term, mixed):
    groups = weight.shape[0]

    @pl.when(pl.program_id(0) == 0)
    def _():
        at = lax.broadcasted_iota(jnp.int32, (SPAN, SPAN), 0)
        source = lax.broadcasted_iota(jnp.int32, (SPAN, SPAN), 1)
        masked = [
            jnp.where(source <= at, weight[g], jnp.zeros_like(weight[g])) for g in range(groups)
        ]
        count, chans = mixed.shape
        wide = chans // groups
        column = [
            jnp.sum(jnp.where(source == at, shift[g : g + 1, :], 0.0), axis=1, keepdims=True)
            for g in range(groups)
        ]
        for n in range(count // SPAN):
            block = pl.ds(n * SPAN, SPAN)
            totals = (sums[block, :] + far[block, :]) / BW
            v_mean = totals[:, 0:1]
            v_var = totals[:, 1:2] - v_mean * v_mean
            v_normed = (act[0, block, :] - v_mean) * lax.rsqrt(v_var + EPS) * gain[...] + bias[...]
            v_normed = v_normed.astype(jnp.bfloat16)
            spatial = [
                dot(masked[g], v_normed[:, g * wide : (g + 1) * wide]) + column[g]
                for g in range(groups)
            ]
            product = act[1, block, :] * jnp.concatenate(spatial, axis=1)
            mixed[block, :] = product.astype(jnp.bfloat16)

    term[...] = dot_rows(mixed[...], rows[...]).astype(jnp.bfloat16)


def mix(act, sums, far, gain, bias, weight, shift, rows):
    _, count, chans = act.shape
    width = rows.shape[0]
    groups = weight.shape[0]
    return pl.pallas_call(
        mix_kernel,
        out_shape=jax.ShapeDtypeStruct((count, width), jnp.bfloat16),
        grid=(width // WIDE,),
        in_specs=[
            whole(act.shape),
            whole((count, LANES)),
            whole((count, LANES)),
            whole((1, chans)),
            whole((1, chans)),
            whole((groups, SPAN, SPAN)),
            whole((groups, SPAN)),
            spec((WIDE, chans), lambda j: (j, 0)),
        ],
        out_specs=spec((count, WIDE), lambda j: (0, j)),
        scratch_shapes=[pltpu.VMEM((count, chans), jnp.bfloat16)],
        compiler_params=params(1),
        cost_estimate=cost(2 * count * width * chans, 2 * width * chans, count),
        name="mix",
    )(act, sums, far, gain, bias, weight, shift, rows)


def second_kernel(
    core, middle, term, far, gain, first, others, send, keep, base, normed, hidden, wide, down, sems
):
    step = pl.program_id(0)
    steps = 5
    outs = down.shape[0] // WIDE
    cuts = [pl.ds(k * WIDE, WIDE) for k in range(4)] + [pl.ds(4 * WIDE, 6 * LANES)]
    copies = [
        pltpu.make_async_copy(first.at[:, cut], wide.at[:, cut], sems.at[k])
        for k, cut in enumerate(cuts)
    ]
    copies.append(pltpu.make_async_copy(others, down, sems.at[steps]))

    @pl.when(step == 0)
    def _():
        for copy in copies:
            copy.start()
        values = middle[...].astype(jnp.float32) + (
            term[...].astype(jnp.float32) + far[...].astype(jnp.float32)
        )
        second = values.astype(jnp.bfloat16)
        half = second.shape[1] // 2
        base[...] = jnp.where(core[0] == 0, second[:, :half], second[:, half:])
        normed[...] = normed_rows(second.astype(jnp.float32), gain[...])

    for k, copy in enumerate(copies):

        @pl.when(step == k)
        def _():
            copy.wait()

    hidden_step(step, normed, wide, hidden)

    @pl.when(step >= steps)
    def _():
        n = step - steps
        mine = jnp.where(n < outs // 2, 1 - core[0], core[0])
        row = mine * (outs // 2) + lax.rem(n, outs // 2)
        rows = pl.ds(pl.multiple_of(row * WIDE, WIDE), WIDE)
        part = dot_rows(hidden[...], down[rows, :]).astype(jnp.bfloat16)

        @pl.when(n < outs // 2)
        def _():
            send[...] = part

        @pl.when(n >= outs // 2)
        def _():
            keep[...] = part


def second_pass(core, middle, term, far, gain, first, others):
    count, width = middle.shape
    half = width // 2
    columns = first.shape[1]
    units = columns // 2
    outs = width // WIDE
    sent = outs // 2
    return pl.pallas_call(
        second_kernel,
        out_shape=[jax.ShapeDtypeStruct((count, half), jnp.bfloat16)] * 3,
        grid_spec=pltpu.PrefetchScalarGridSpec(
            num_scalar_prefetch=1,
            grid=(5 + outs,),
            in_specs=[
                whole((count, width)),
                whole((count, width)),
                whole((count, width)),
                whole((1, width)),
                ANY,
                ANY,
            ],
            out_specs=[
                spec((count, WIDE), lambda j, c: (0, jnp.clip(j - 5, 0, sent - 1))),
                spec((count, WIDE), lambda j, c: (0, jnp.maximum(j - 5 - sent, 0))),
                whole((count, half)),
            ],
            scratch_shapes=[
                pltpu.VMEM((count, width), jnp.bfloat16),
                pltpu.VMEM((count, units), jnp.bfloat16),
                pltpu.VMEM((width, columns), jnp.bfloat16),
                pltpu.VMEM((width, units), jnp.bfloat16),
                pltpu.SemaphoreType.DMA((6,)),
            ],
        ),
        compiler_params=params(1),
        cost_estimate=cost(6 * count * width * units, 6 * width * units, count * units),
        name="second_pass",
    )(core, middle, term, far, gain, first, others)


def layer(
    tokens,
    norm_first,
    norm_mix,
    norm_second,
    gate_weight,
    up_weight,
    down_weight,
    gate_scale,
    up_scale,
    down_scale,
    u_weight,
    v_weight,
    u_scale,
    v_scale,
    ln_gain,
    ln_bias,
    spatial_weight,
    spatial_bias,
    out_weight,
    out_scale,
):
    chans = u_weight.shape[1]
    width = 2 * tokens.shape[1]

    def number(x):
        return x.reshape(1).astype(jnp.int32)

    core = number(lax.axis_index("tp"))
    rep = lax.axis_index("rep")
    at = number(2 * lax.axis_index(FS) + rep)

    colors = prepare(
        number(rep),
        gate_weight,
        up_weight,
        down_weight.T,
        u_weight,
        v_weight,
        out_weight.T,
        gate_scale,
        up_scale,
        down_scale,
        u_scale,
        v_scale,
        out_scale,
    )
    one, two = gather(colors)

    own, other = tokens, other_core(tokens)
    hidden, first = first_hidden(core, at, own, other, norm_first[None], one)
    term, down = first_down(at, hidden, width, two[6:])
    far = other_core(term)
    mixer = assemble(at, width, two[:6])
    middle, act, sums = gates(core, own, other, term, far, norm_mix[None], mixer, chans)
    term = mix(
        act,
        sums,
        other_core(sums),
        ln_gain[None],
        ln_bias[None],
        spatial_weight,
        spatial_bias,
        mixer,
    )
    send, keep, base = second_pass(
        core, middle, term, other_core(term), norm_second[None], first, down
    )
    last = keep.astype(jnp.float32) + other_core(send).astype(jnp.float32)
    return (base.astype(jnp.float32) + 0.5 * last).astype(jnp.bfloat16)


def solution(mesh):
    torus = Mesh(
        mesh.devices.reshape(mesh.shape["rep"], 2, 4, 4, mesh.shape["tp"]),
        ("rep", "fs_0", "fs_1", "fs_2", "tp"),
    )
    in_specs = (
        P(REP_FS, "tp"),
        P(),
        P(),
        P(),
        P(FS, "tp"),
        P(FS, "tp"),
        P("tp", FS),
        P("tp"),
        P("tp"),
        P(FS),
        P(FS, "tp"),
        P(FS, "tp"),
        P("tp"),
        P("tp"),
        P("tp"),
        P("tp"),
        P("tp", None, None),
        P("tp", None),
        P("tp", FS),
        P(FS),
    )
    out_specs = P(REP_FS, "tp")
    return jax.shard_map(layer, mesh=torus, in_specs=in_specs, out_specs=out_specs, check_vma=False)
```

```python
import functools

import jax
import jax.numpy as jnp
from jax import lax
from jax.experimental import pallas as pl
from jax.experimental.pallas import tpu as pltpu
from jax.sharding import Mesh
from jax.sharding import PartitionSpec as P


BW = 1024
SPAN = 128
FS = ("fs_0", "fs_1", "fs_2")
REP_FS = ("rep", "fs_0", "fs_1", "fs_2")
LANES = 128
WIDE = 512
HALF_ROWS = 32
FIRST = (4, 4, 4, 4, 3, 3)
OTHERS = (4, 4, 4, 3, 4, 4)
RINGS = (("fs_2", 1), ("fs_1", 1), ("z", 1), ("fs_2", 3), ("fs_1", 3), ("z", 3))
PLACES = (2, 8, 32, 6, 24, 33)
ROUNDS = (
    (0, 4, 5, 3, 2, 1),
    (0, 4, 3, 5, 1, 2),
    (1, 5, 4, 2, 3, 0),
    (1, 5, 2, 4, 0, 3),
    (2, 3, 1, 0, 5, 4),
    (2, 3, 0, 1, 4, 5),
)

EPS = 1e-06


def other_core(x):
    return lax.ppermute(x, "tp", [(0, 1), (1, 0)])


def normed_rows(values, gain):
    factor = lax.rsqrt(jnp.mean(values * values, axis=1, keepdims=True) + EPS)
    return (values * factor * gain).astype(jnp.bfloat16)


def dot(left, right):
    return jnp.dot(left, right, preferred_element_type=jnp.float32)


def dot_rows(left, rows):
    return lax.dot_general(
        left, rows, (((1,), (1,)), ((), ())), preferred_element_type=jnp.float32
    )


def gelu(a):
    return 0.5 * a * (1.0 + jnp.tanh(0.7978845608028654 * (a + 0.044715 * a * a * a)))


def spec(block, index):
    return pl.BlockSpec(block, index)


def whole(shape):
    return pl.BlockSpec(shape, lambda *_: (0,) * len(shape))


ANY = pl.BlockSpec(memory_space=pl.ANY)


def params(steps, mib=60):
    return pltpu.CompilerParams(
        dimension_semantics=("arbitrary",) * steps, vmem_limit_bytes=mib * 1024 * 1024
    )


def cost(flops, moved, special):
    return pl.CostEstimate(flops=flops, bytes_accessed=moved, transcendentals=special)


def exchange(x, color, turn):
    name, flip = RINGS[ROUNDS[color][turn]]
    axis = ("rep", "fs_0") if name == "z" else name
    return lax.ppermute(x, axis, [(i, i ^ flip) for i in range(4)])


def place(color, slot):
    at = 0
    for turn in range(6):
        if slot >> turn & 1:
            at ^= PLACES[ROUNDS[color][turn]]
    return at


def starts(widths):
    ends = [0]
    for n in widths:
        ends.append(ends[-1] + n * LANES)
    return ends


PAIRS = [(p, t + k) for t in (0, 2, 4, 6) for p in (0, 1) for k in (0, 1)]
PAIRS += [(0, 8), (0, 9), (1, 8), (1, 9), (0, 10), (1, 10)]


def prepare_kernel(rep, *refs):
    inputs, colors, held, sems = refs[:12], refs[12:15], refs[15:27], refs[27]
    copies = [
        pltpu.make_async_copy(x, y, sems.at[k]) for k, (x, y) in enumerate(zip(inputs, held))
    ]
    for copy in copies:
        copy.start()
    for copy in copies:
        copy.wait()
    gate, up, down, u, v, out, gate_s, up_s, down_s, u_s, v_s, out_s = held
    rows = pl.ds(pl.multiple_of(rep[0] * HALF_ROWS, HALF_ROWS), HALF_ROWS)
    low = jnp.bfloat16

    def across(scale):
        return scale[...][None, :]

    def down_rows(scale):
        size = scale.shape[0]
        row = lax.broadcasted_iota(jnp.int32, (HALF_ROWS, size), 0) + rep[0] * HALF_ROWS
        column = lax.broadcasted_iota(jnp.int32, (HALF_ROWS, size), 1)
        return jnp.sum(jnp.where(row == column, across(scale), 0.0), axis=1, keepdims=True)

    pair = ((gate[rows, :] * across(gate_s)).astype(low), (up[rows, :] * across(up_s)).astype(low))
    firsts = [pair[p][:, t * LANES : (t + 1) * LANES] for p, t in PAIRS]
    rest = jnp.concatenate(
        [
            (out[rows, :] * down_rows(out_s)).astype(low),
            (u[rows, :] * across(u_s)).astype(low),
            (v[rows, :] * across(v_s)).astype(low),
            (down[rows, :] * down_rows(down_s)).astype(low),
        ],
        axis=1,
    )
    at, begin = 0, starts(OTHERS)
    mine = []
    for c in range(6):
        mine.append(firsts[at : at + FIRST[c]] + [rest[:, begin[c] : begin[c + 1]]])
        at += FIRST[c]
    for pair, ref in enumerate(colors):
        ref[...] = jnp.concatenate(mine[2 * pair] + mine[2 * pair + 1], axis=1)


WIDTHS = [(a + b) * LANES for a, b in zip(FIRST, OTHERS)]
VMEM = pl.BlockSpec(memory_space=pltpu.VMEM)
SMEM = pl.BlockSpec(memory_space=pltpu.SMEM)
HBM = pl.BlockSpec(memory_space=pltpu.HBM)


def prepare(rep, *arrays):
    pairs = [WIDTHS[k] + WIDTHS[k + 1] for k in (0, 2, 4)]
    return pl.pallas_call(
        prepare_kernel,
        out_shape=[jax.ShapeDtypeStruct((HALF_ROWS, n), jnp.bfloat16) for n in pairs],
        in_specs=[SMEM] + [HBM] * len(arrays),
        out_specs=[VMEM] * 3,
        scratch_shapes=[pltpu.VMEM(x.shape, x.dtype) for x in arrays]
        + [pltpu.SemaphoreType.DMA((len(arrays),))],
        compiler_params=pltpu.CompilerParams(vmem_limit_bytes=60 * 1024 * 1024),
        name="prepare",
    )(rep, *arrays)


def join_kernel(cuts, *refs):
    sources = (len(refs) - len(cuts)) // 2
    for joined, (source, begin, end) in zip(refs[2 * sources :], cuts):
        held, arrived = refs[source], refs[sources + source]
        rows = held.shape[0]
        joined[pl.ds(0, rows), :] = held[:, begin:end]
        joined[pl.ds(rows, rows), :] = arrived[:, begin:end]


def cut_kernel(*refs):
    for k in range(len(refs) // 2):
        refs[len(refs) // 2 + k][...] = refs[k][:, : refs[len(refs) // 2 + k].shape[1]]


def first_columns(arrays, widths):
    return pl.pallas_call(
        cut_kernel,
        out_shape=[
            jax.ShapeDtypeStruct((x.shape[0], n * LANES), x.dtype) for x, n in zip(arrays, widths)
        ],
        in_specs=[VMEM] * len(arrays),
        out_specs=[VMEM] * len(arrays),
        compiler_params=pltpu.CompilerParams(vmem_limit_bytes=16 * 1024 * 1024),
        name="first_columns",
    )(*arrays)


def join(held, arrived, cuts=None):
    rows, low = held[0].shape[0], jnp.bfloat16
    if cuts is None:
        cuts = [(k, 0, x.shape[1]) for k, x in enumerate(held)]
    return pl.pallas_call(
        functools.partial(join_kernel, cuts),
        out_shape=[jax.ShapeDtypeStruct((2 * rows, b - a), low) for _, a, b in cuts],
        in_specs=[VMEM] * (2 * len(held)),
        out_specs=[VMEM] * len(cuts),
        compiler_params=pltpu.CompilerParams(vmem_limit_bytes=16 * 1024 * 1024),
        name="join",
    )(*held, *arrived)


def gather(pairs):
    ready = []
    for p, x in enumerate(pairs):
        (held,) = join([x], [exchange(x, 2 * p, 0)])
        edge = WIDTHS[2 * p]
        cuts = [(0, 0, edge), (0, edge, held.shape[1])]
        held = join([held], [exchange(held, 2 * p, 1)], cuts)
        held = join(held, [exchange(y, 2 * p + k, 2) for k, y in enumerate(held)])
        arrived = [exchange(y, 2 * p + k, 3) for k, y in enumerate(held)]
        held = join(held, arrived)
        ready.append((held, [exchange(y, 2 * p + k, 4) for k, y in enumerate(held)]))
    one, two = [], []
    for p, (held, arrived) in enumerate(ready):
        kept = first_columns(held, FIRST[2 * p : 2 * p + 2])
        early = [exchange(x, 2 * p + k, 5) for k, x in enumerate(kept)]
        come = first_columns(arrived, FIRST[2 * p : 2 * p + 2])
        late = [exchange(x, 2 * p + k, 5) for k, x in enumerate(come)]
        for k in range(2):
            one += [kept[k], come[k], early[k], late[k]]
        cuts = [(k, FIRST[2 * p + k] * LANES, y.shape[1]) for k, y in enumerate(held)]
        halves = join(held, arrived, cuts)
        for k, y in enumerate(halves):
            two += [y, exchange(y, 2 * p + k, 5)]
    return one, two


def place_blocks(at, pieces, weight, sems, widths, colors, first=0):
    begin = starts(widths)
    parts = len(pieces) // len(widths)
    slots = 64 // parts
    for c in colors:
        columns = pl.ds(begin[c], widths[c] * LANES)
        for k in range(parts):

            def copy_four(high, carry, c=c, k=k, columns=columns):
                moved = at ^ place(first + c, slots * k)
                for bit in range(slots.bit_length() - 3):
                    moved = moved ^ ((high >> bit & 1) * place(first + c, 4 << bit))
                for low in range(4):
                    to = (moved ^ place(first + c, low)) * HALF_ROWS
                    origin = (high * 4 + low) * HALF_ROWS
                    pltpu.make_async_copy(
                        pieces[parts * c + k].at[
                            pl.ds(pl.multiple_of(origin, HALF_ROWS), HALF_ROWS), :
                        ],
                        weight.at[pl.ds(pl.multiple_of(to, HALF_ROWS), HALF_ROWS), columns],
                        sems.at[c],
                    ).start()
                return carry

            lax.fori_loop(0, slots // 4, copy_four, 0)


def wait_color(weight, sems, widths, c):
    columns = pl.ds(starts(widths)[c], widths[c] * LANES)
    part = weight.at[:, columns]
    pltpu.make_async_copy(part, part, sems.at[c]).wait()


def silu_product(gate, up):
    return (gate / (1.0 + jnp.exp(-gate)) * up).astype(jnp.bfloat16)


def narrow_step(normed, weight):
    both = dot(normed, weight)
    tile = [both[:, k * LANES : (k + 1) * LANES] for k in range(6)]
    gate = jnp.concatenate([tile[0], tile[1], tile[4]], axis=1)
    up = jnp.concatenate([tile[2], tile[3], tile[5]], axis=1)
    return silu_product(gate, up)


def hidden_step(step, normed, weight, hidden):
    @pl.when((step >= 0) & (step < 4))
    def _():
        columns = pl.ds(pl.multiple_of(step * WIDE, WIDE), WIDE)
        both = dot(normed[...], weight[:, columns])
        to = pl.ds(pl.multiple_of(step * (WIDE // 2), WIDE // 2), WIDE // 2)
        hidden[:, to] = silu_product(both[:, : WIDE // 2], both[:, WIDE // 2 :])

    @pl.when(step == 4)
    def _():
        hidden[:, 2 * WIDE :] = narrow_step(normed[...], weight[:, 4 * WIDE :])


def norm_kernel(core, own, other, gain, normed):
    left = jnp.where(core[0] == 0, own[...], other[...])
    right = jnp.where(core[0] == 0, other[...], own[...])
    values = jnp.concatenate([left, right], axis=1).astype(jnp.float32)
    normed[...] = normed_rows(values, gain[...])


def first_norm(core, own, other, gain):
    count, half = own.shape
    block = spec((SPAN, half), lambda i, c: (i, 0))
    return pl.pallas_call(
        norm_kernel,
        out_shape=jax.ShapeDtypeStruct((count, 2 * half), jnp.bfloat16),
        grid_spec=pltpu.PrefetchScalarGridSpec(
            num_scalar_prefetch=1,
            grid=(count // SPAN,),
            in_specs=[block, block, whole((1, 2 * half))],
            out_specs=spec((SPAN, 2 * half), lambda i, c: (i, 0)),
        ),
        compiler_params=params(1),
        cost_estimate=cost(5 * 10**9, 8 * count * half, count),
        name="first_norm",
    )(core, own, other, gain)


def first_kernel(at, normed, *rest):
    pieces, (hidden, kept, weight, sems, out_sems) = rest[:24], rest[24:]
    step = pl.program_id(0)
    begin = starts(FIRST)
    copies = []
    for c in range(6):
        columns = pl.ds(begin[c], FIRST[c] * LANES)
        copies.append(
            pltpu.make_async_copy(weight.at[:, columns], kept.at[:, columns], out_sems.at[c])
        )

    for k, colors in enumerate(((0, 1, 2), (3,), (4,), (5,))):

        @pl.when(step == k)
        def _():
            place_blocks(at[0], pieces, weight, sems, FIRST, colors)

    for c in range(6):

        @pl.when(step == min(c, 4))
        def _():
            wait_color(weight, sems, FIRST, c)
            copies[c].start()

    hidden_step(step, normed, weight, hidden)

    @pl.when(step == 4)
    def _():
        for copy in copies:
            copy.wait()


def first_hidden(at, normed, pieces):
    count, width = normed.shape
    columns = sum(FIRST) * LANES
    units = columns // 2
    return pl.pallas_call(
        first_kernel,
        out_shape=[
            jax.ShapeDtypeStruct((count, units), jnp.bfloat16),
            jax.ShapeDtypeStruct((width, columns), jnp.bfloat16),
        ],
        grid_spec=pltpu.PrefetchScalarGridSpec(
            num_scalar_prefetch=1,
            grid=(5,),
            in_specs=[whole((count, width))] + [ANY] * 24,
            out_specs=[whole((count, units)), ANY],
            scratch_shapes=[
                pltpu.VMEM((width, columns), jnp.bfloat16),
                pltpu.SemaphoreType.DMA((6,)),
                pltpu.SemaphoreType.DMA((6,)),
            ],
        ),
        compiler_params=params(1),
        cost_estimate=cost(2 * count * width * columns, 4 * width * columns, count * units),
        name="first_hidden",
    )(at, normed, *pieces)


MIXER, DOWN = OTHERS[:3], OTHERS[3:]


def place_blocks_of(at, pieces, weight, sems, widths, first):
    place_blocks(at, pieces, weight, sems, widths, range(len(widths)), first)


def down_kernel(at, hidden, *rest):
    pieces, (term, kept, weight, sems, out_sem) = rest[:6], rest[6:]
    step = pl.program_id(0)
    copy = pltpu.make_async_copy(weight, kept, out_sem)

    @pl.when(step == 0)
    def _():
        place_blocks_of(at[0], pieces, weight, sems, DOWN, 3)
        for c in range(3):
            wait_color(weight, sems, DOWN, c)
        copy.start()

    rows = pl.ds(pl.multiple_of(step * WIDE, WIDE), WIDE)
    term[...] = dot_rows(hidden[...], weight[rows, :]).astype(jnp.bfloat16)

    @pl.when(step == pl.num_programs(0) - 1)
    def _():
        copy.wait()


def first_down(at, hidden, width, pieces):
    count, units = hidden.shape
    return pl.pallas_call(
        down_kernel,
        out_shape=[
            jax.ShapeDtypeStruct((count, width), jnp.bfloat16),
            jax.ShapeDtypeStruct((width, units), jnp.bfloat16),
        ],
        grid_spec=pltpu.PrefetchScalarGridSpec(
            num_scalar_prefetch=1,
            grid=(width // WIDE,),
            in_specs=[whole((count, units))] + [ANY] * 6,
            out_specs=[spec((count, WIDE), lambda j, a: (0, j)), ANY],
            scratch_shapes=[
                pltpu.VMEM((width, units), jnp.bfloat16),
                pltpu.SemaphoreType.DMA((3,)),
                pltpu.SemaphoreType.DMA,
            ],
        ),
        compiler_params=params(1),
        cost_estimate=cost(2 * count * width * units, 4 * width * units, 0),
        name="first_down",
    )(at, hidden, *pieces)


def assemble_kernel(at, *rest):
    pieces, (kept, weight, sems, out_sems) = rest[:6], rest[6:]
    place_blocks_of(at[0], pieces, weight, sems, MIXER, 0)
    begin = starts(MIXER)
    copies = []
    for c in range(3):
        wait_color(weight, sems, MIXER, c)
        columns = pl.ds(begin[c], MIXER[c] * LANES)
        copy = pltpu.make_async_copy(weight.at[:, columns], kept.at[:, columns], out_sems.at[c])
        copy.start()
        copies.append(copy)
    for copy in copies:
        copy.wait()


def assemble(at, width, pieces):
    shape = (width, sum(MIXER) * LANES)
    return pl.pallas_call(
        assemble_kernel,
        out_shape=jax.ShapeDtypeStruct(shape, jnp.bfloat16),
        grid_spec=pltpu.PrefetchScalarGridSpec(
            num_scalar_prefetch=1,
            grid=(1,),
            in_specs=[ANY] * 6,
            out_specs=ANY,
            scratch_shapes=[
                pltpu.VMEM(shape, jnp.bfloat16),
                pltpu.SemaphoreType.DMA((3,)),
                pltpu.SemaphoreType.DMA((3,)),
            ],
        ),
        compiler_params=params(1),
        cost_estimate=cost(5 * 10**9, 8 * shape[0] * shape[1], 0),
        name="assemble",
    )(at, *pieces)


def gates_kernel(
    blocks, core, own, other, term, far, gain, u_rows, v_rows, middle, act, sums, normed
):
    step = pl.program_id(0)

    @pl.when(step < blocks)
    def _():
        left = jnp.where(core[0] == 0, own[...], other[...])
        right = jnp.where(core[0] == 0, other[...], own[...])
        values = jnp.concatenate([left, right], axis=1).astype(jnp.float32)
        values = values + 0.5 * (term[...].astype(jnp.float32) + far[...].astype(jnp.float32))
        mid = values.astype(jnp.bfloat16)
        middle[...] = mid
        block = pl.ds(pl.multiple_of(step * SPAN, SPAN), SPAN)
        normed[block, :] = normed_rows(mid.astype(jnp.float32), gain[...])

    @pl.when(step == blocks)
    def _():
        v_pre = dot(normed[...], v_rows[...])
        u_pre = dot(normed[...], u_rows[...])
        v_act = gelu(v_pre)
        act[0] = v_act
        lane = lax.broadcasted_iota(jnp.int32, sums.shape, 1)
        total = jnp.sum(v_act, axis=1, keepdims=True)
        squares = jnp.sum(v_act * v_act, axis=1, keepdims=True)
        sums[...] = jnp.where(lane == 0, total, squares)
        act[1] = gelu(u_pre)


def gates(core, own, other, term, far, gain, weight, chans):
    count, half = own.shape
    width = 2 * half
    blocks = count // SPAN

    def block(columns):
        return spec((SPAN, columns), lambda i, c: (jnp.minimum(i, blocks - 1), 0))

    return pl.pallas_call(
        functools.partial(gates_kernel, blocks),
        out_shape=[
            jax.ShapeDtypeStruct((count, width), jnp.bfloat16),
            jax.ShapeDtypeStruct((2, count, chans), jnp.float32),
            jax.ShapeDtypeStruct((count, LANES), jnp.float32),
        ],
        grid_spec=pltpu.PrefetchScalarGridSpec(
            num_scalar_prefetch=1,
            grid=(blocks + 1,),
            in_specs=[
                block(half),
                block(half),
                block(width),
                block(width),
                whole((1, width)),
                spec((width, chans), lambda i, c: (0, 1)),
                spec((width, chans), lambda i, c: (0, 2)),
            ],
            out_specs=[block(width), whole((2, count, chans)), whole((count, LANES))],
            scratch_shapes=[pltpu.VMEM((count, width), jnp.bfloat16)],
        ),
        compiler_params=params(1),
        cost_estimate=cost(4 * count * width * chans, 4 * width * chans, 2 * count * chans),
        name="gates",
    )(core, own, other, term, far, gain, weight, weight)


def mix_kernel(act, sums, far, gain, bias, weight, shift, rows, term, mixed):
    groups = weight.shape[0]

    @pl.when(pl.program_id(0) == 0)
    def _():
        at = lax.broadcasted_iota(jnp.int32, (SPAN, SPAN), 0)
        source = lax.broadcasted_iota(jnp.int32, (SPAN, SPAN), 1)
        masked = [
            jnp.where(source <= at, weight[g], jnp.zeros_like(weight[g])) for g in range(groups)
        ]
        count, chans = mixed.shape
        wide = chans // groups
        column = [
            jnp.sum(jnp.where(source == at, shift[g : g + 1, :], 0.0), axis=1, keepdims=True)
            for g in range(groups)
        ]
        for n in range(count // SPAN):
            block = pl.ds(n * SPAN, SPAN)
            totals = (sums[block, :] + far[block, :]) / BW
            v_mean = totals[:, 0:1]
            v_var = totals[:, 1:2] - v_mean * v_mean
            v_normed = (act[0, block, :] - v_mean) * lax.rsqrt(v_var + EPS) * gain[...] + bias[...]
            v_normed = v_normed.astype(jnp.bfloat16)
            spatial = [
                dot(masked[g], v_normed[:, g * wide : (g + 1) * wide]) + column[g]
                for g in range(groups)
            ]
            product = act[1, block, :] * jnp.concatenate(spatial, axis=1)
            mixed[block, :] = product.astype(jnp.bfloat16)

    term[...] = dot_rows(mixed[...], rows[...]).astype(jnp.bfloat16)


def mix(act, sums, far, gain, bias, weight, shift, rows):
    _, count, chans = act.shape
    width = rows.shape[0]
    groups = weight.shape[0]
    return pl.pallas_call(
        mix_kernel,
        out_shape=jax.ShapeDtypeStruct((count, width), jnp.bfloat16),
        grid=(width // WIDE,),
        in_specs=[
            whole(act.shape),
            whole((count, LANES)),
            whole((count, LANES)),
            whole((1, chans)),
            whole((1, chans)),
            whole((groups, SPAN, SPAN)),
            whole((groups, SPAN)),
            spec((WIDE, chans), lambda j: (j, 0)),
        ],
        out_specs=spec((count, WIDE), lambda j: (0, j)),
        scratch_shapes=[pltpu.VMEM((count, chans), jnp.bfloat16)],
        compiler_params=params(1),
        cost_estimate=cost(2 * count * width * chans, 2 * width * chans, count),
        name="mix",
    )(act, sums, far, gain, bias, weight, shift, rows)


def second_kernel(
    core, middle, term, far, gain, first, others, send, keep, base, normed, hidden, wide, down, sems
):
    step = pl.program_id(0)
    steps = 5
    outs = down.shape[0] // WIDE
    cuts = [pl.ds(k * WIDE, WIDE) for k in range(4)] + [pl.ds(4 * WIDE, 6 * LANES)]
    copies = [
        pltpu.make_async_copy(first.at[:, cut], wide.at[:, cut], sems.at[k])
        for k, cut in enumerate(cuts)
    ]
    copies.append(pltpu.make_async_copy(others, down, sems.at[steps]))

    @pl.when(step == 0)
    def _():
        for copy in copies:
            copy.start()
        values = middle[...].astype(jnp.float32) + (
            term[...].astype(jnp.float32) + far[...].astype(jnp.float32)
        )
        second = values.astype(jnp.bfloat16)
        half = second.shape[1] // 2
        base[...] = jnp.where(core[0] == 0, second[:, :half], second[:, half:])
        normed[...] = normed_rows(second.astype(jnp.float32), gain[...])

    for k, copy in enumerate(copies):

        @pl.when(step == k)
        def _():
            copy.wait()

    hidden_step(step, normed, wide, hidden)

    @pl.when(step >= steps)
    def _():
        n = step - steps
        mine = jnp.where(n < outs // 2, 1 - core[0], core[0])
        row = mine * (outs // 2) + lax.rem(n, outs // 2)
        rows = pl.ds(pl.multiple_of(row * WIDE, WIDE), WIDE)
        part = dot_rows(hidden[...], down[rows, :]).astype(jnp.bfloat16)

        @pl.when(n < outs // 2)
        def _():
            send[...] = part

        @pl.when(n >= outs // 2)
        def _():
            keep[...] = part


def second_pass(core, middle, term, far, gain, first, others):
    count, width = middle.shape
    half = width // 2
    columns = first.shape[1]
    units = columns // 2
    outs = width // WIDE
    sent = outs // 2
    return pl.pallas_call(
        second_kernel,
        out_shape=[jax.ShapeDtypeStruct((count, half), jnp.bfloat16)] * 3,
        grid_spec=pltpu.PrefetchScalarGridSpec(
            num_scalar_prefetch=1,
            grid=(5 + outs,),
            in_specs=[
                whole((count, width)),
                whole((count, width)),
                whole((count, width)),
                whole((1, width)),
                ANY,
                ANY,
            ],
            out_specs=[
                spec((count, WIDE), lambda j, c: (0, jnp.clip(j - 5, 0, sent - 1))),
                spec((count, WIDE), lambda j, c: (0, jnp.maximum(j - 5 - sent, 0))),
                whole((count, half)),
            ],
            scratch_shapes=[
                pltpu.VMEM((count, width), jnp.bfloat16),
                pltpu.VMEM((count, units), jnp.bfloat16),
                pltpu.VMEM((width, columns), jnp.bfloat16),
                pltpu.VMEM((width, units), jnp.bfloat16),
                pltpu.SemaphoreType.DMA((6,)),
            ],
        ),
        compiler_params=params(1),
        cost_estimate=cost(6 * count * width * units, 6 * width * units, count * units),
        name="second_pass",
    )(core, middle, term, far, gain, first, others)


def layer(
    tokens,
    norm_first,
    norm_mix,
    norm_second,
    gate_weight,
    up_weight,
    down_weight,
    gate_scale,
    up_scale,
    down_scale,
    u_weight,
    v_weight,
    u_scale,
    v_scale,
    ln_gain,
    ln_bias,
    spatial_weight,
    spatial_bias,
    out_weight,
    out_scale,
):
    chans = u_weight.shape[1]
    width = 2 * tokens.shape[1]

    def number(x):
        return x.reshape(1).astype(jnp.int32)

    core = number(lax.axis_index("tp"))
    rep = lax.axis_index("rep")
    at = number(2 * lax.axis_index(FS) + rep)

    colors = prepare(
        number(rep),
        gate_weight,
        up_weight,
        down_weight.T,
        u_weight,
        v_weight,
        out_weight.T,
        gate_scale,
        up_scale,
        down_scale,
        u_scale,
        v_scale,
        out_scale,
    )
    one, two = gather(colors)

    own, other = tokens, other_core(tokens)
    normed = first_norm(core, own, other, norm_first[None])
    hidden, first = first_hidden(at, normed, one)
    term, down = first_down(at, hidden, width, two[6:])
    far = other_core(term)
    mixer = assemble(at, width, two[:6])
    middle, act, sums = gates(core, own, other, term, far, norm_mix[None], mixer, chans)
    term = mix(
        act,
        sums,
        other_core(sums),
        ln_gain[None],
        ln_bias[None],
        spatial_weight,
        spatial_bias,
        mixer,
    )
    send, keep, base = second_pass(
        core, middle, term, other_core(term), norm_second[None], first, down
    )
    last = keep.astype(jnp.float32) + other_core(send).astype(jnp.float32)
    return (base.astype(jnp.float32) + 0.5 * last).astype(jnp.bfloat16)


def solution(mesh):
    torus = Mesh(
        mesh.devices.reshape(mesh.shape["rep"], 2, 4, 4, mesh.shape["tp"]),
        ("rep", "fs_0", "fs_1", "fs_2", "tp"),
    )
    in_specs = (
        P(REP_FS, "tp"),
        P(),
        P(),
        P(),
        P(FS, "tp"),
        P(FS, "tp"),
        P("tp", FS),
        P("tp"),
        P("tp"),
        P(FS),
        P(FS, "tp"),
        P(FS, "tp"),
        P("tp"),
        P("tp"),
        P("tp"),
        P("tp"),
        P("tp", None, None),
        P("tp", None),
        P("tp", FS),
        P(FS),
    )
    out_specs = P(REP_FS, "tp")
    return jax.shard_map(layer, mesh=torus, in_specs=in_specs, out_specs=out_specs, check_vma=False)
```

```python
import functools

import jax
import jax.numpy as jnp
from jax import lax
from jax.experimental import pallas as pl
from jax.experimental.pallas import tpu as pltpu
from jax.sharding import Mesh
from jax.sharding import PartitionSpec as P


BW = 1024
SPAN = 128
FS = ("fs_0", "fs_1", "fs_2")
REP_FS = ("rep", "fs_0", "fs_1", "fs_2")
LANES = 128
WIDE = 512
HALF_ROWS = 32
FIRST = (4, 4, 4, 4, 3, 3)
OTHERS = (4, 4, 4, 3, 4, 4)
RINGS = (("fs_2", 1), ("fs_1", 1), ("z", 1), ("fs_2", 3), ("fs_1", 3), ("z", 3))
PLACES = (2, 8, 32, 6, 24, 33)
ROUNDS = (
    (0, 4, 5, 3, 2, 1),
    (0, 4, 3, 5, 1, 2),
    (1, 5, 4, 2, 3, 0),
    (1, 5, 2, 4, 0, 3),
    (2, 3, 1, 0, 5, 4),
    (2, 3, 0, 1, 4, 5),
)

EPS = 1e-06


def other_core(x):
    return lax.ppermute(x, "tp", [(0, 1), (1, 0)])


def normed_rows(values, gain):
    factor = lax.rsqrt(jnp.mean(values * values, axis=1, keepdims=True) + EPS)
    return (values * factor * gain).astype(jnp.bfloat16)


def dot(left, right):
    return jnp.dot(left, right, preferred_element_type=jnp.float32)


def dot_rows(left, rows):
    return lax.dot_general(
        left, rows, (((1,), (1,)), ((), ())), preferred_element_type=jnp.float32
    )


def gelu(a):
    return 0.5 * a * (1.0 + jnp.tanh(0.7978845608028654 * (a + 0.044715 * a * a * a)))


def spec(block, index):
    return pl.BlockSpec(block, index)


def whole(shape):
    return pl.BlockSpec(shape, lambda *_: (0,) * len(shape))


ANY = pl.BlockSpec(memory_space=pl.ANY)


def params(steps):
    return pltpu.CompilerParams(
        dimension_semantics=("arbitrary",) * steps, vmem_limit_bytes=60 * 1024 * 1024
    )


def cost(flops, moved, special):
    return pl.CostEstimate(flops=flops, bytes_accessed=moved, transcendentals=special)


def exchange(x, color, turn):
    name, flip = RINGS[ROUNDS[color][turn]]
    axis = ("rep", "fs_0") if name == "z" else name
    return lax.ppermute(x, axis, [(i, i ^ flip) for i in range(4)])


def place(color, slot):
    at = 0
    for turn in range(6):
        if slot >> turn & 1:
            at ^= PLACES[ROUNDS[color][turn]]
    return at


def starts(widths):
    ends = [0]
    for n in widths:
        ends.append(ends[-1] + n * LANES)
    return ends


PAIRS = [(p, t + k) for t in (0, 2, 4, 6) for p in (0, 1) for k in (0, 1)]
PAIRS += [(0, 8), (0, 9), (1, 8), (1, 9), (0, 10), (1, 10)]


def prepare_kernel(rep, *refs):
    inputs, colors, held, sems = refs[:12], refs[12:15], refs[15:27], refs[27]
    copies = [
        pltpu.make_async_copy(x, y, sems.at[k]) for k, (x, y) in enumerate(zip(inputs, held))
    ]
    for copy in copies:
        copy.start()
    for copy in copies:
        copy.wait()
    gate, up, down, u, v, out, gate_s, up_s, down_s, u_s, v_s, out_s = held
    rows = pl.ds(pl.multiple_of(rep[0] * HALF_ROWS, HALF_ROWS), HALF_ROWS)
    low = jnp.bfloat16

    def across(scale):
        return scale[...][None, :]

    def down_rows(scale):
        size = scale.shape[0]
        row = lax.broadcasted_iota(jnp.int32, (HALF_ROWS, size), 0) + rep[0] * HALF_ROWS
        column = lax.broadcasted_iota(jnp.int32, (HALF_ROWS, size), 1)
        return jnp.sum(jnp.where(row == column, across(scale), 0.0), axis=1, keepdims=True)

    pair = ((gate[rows, :] * across(gate_s)).astype(low), (up[rows, :] * across(up_s)).astype(low))
    firsts = [pair[p][:, t * LANES : (t + 1) * LANES] for p, t in PAIRS]
    rest = jnp.concatenate(
        [
            (out[rows, :] * down_rows(out_s)).astype(low),
            (u[rows, :] * across(u_s)).astype(low),
            (v[rows, :] * across(v_s)).astype(low),
            (down[rows, :] * down_rows(down_s)).astype(low),
        ],
        axis=1,
    )
    at, begin = 0, starts(OTHERS)
    mine = []
    for c in range(6):
        mine.append(firsts[at : at + FIRST[c]] + [rest[:, begin[c] : begin[c + 1]]])
        at += FIRST[c]
    for pair, ref in enumerate(colors):
        ref[...] = jnp.concatenate(mine[2 * pair] + mine[2 * pair + 1], axis=1)


WIDTHS = [(a + b) * LANES for a, b in zip(FIRST, OTHERS)]
VMEM = pl.BlockSpec(memory_space=pltpu.VMEM)
SMEM = pl.BlockSpec(memory_space=pltpu.SMEM)
HBM = pl.BlockSpec(memory_space=pltpu.HBM)


def prepare(rep, *arrays):
    pairs = [WIDTHS[k] + WIDTHS[k + 1] for k in (0, 2, 4)]
    return pl.pallas_call(
        prepare_kernel,
        out_shape=[jax.ShapeDtypeStruct((HALF_ROWS, n), jnp.bfloat16) for n in pairs],
        in_specs=[SMEM] + [HBM] * len(arrays),
        out_specs=[VMEM] * 3,
        scratch_shapes=[pltpu.VMEM(x.shape, x.dtype) for x in arrays]
        + [pltpu.SemaphoreType.DMA((len(arrays),))],
        compiler_params=pltpu.CompilerParams(vmem_limit_bytes=60 * 1024 * 1024),
        name="prepare",
    )(rep, *arrays)


def join_kernel(cuts, *refs):
    sources = (len(refs) - len(cuts)) // 2
    for joined, (source, begin, end) in zip(refs[2 * sources :], cuts):
        held, arrived = refs[source], refs[sources + source]
        rows = held.shape[0]
        joined[pl.ds(0, rows), :] = held[:, begin:end]
        joined[pl.ds(rows, rows), :] = arrived[:, begin:end]


def cut_kernel(*refs):
    for k in range(len(refs) // 2):
        refs[len(refs) // 2 + k][...] = refs[k][:, : refs[len(refs) // 2 + k].shape[1]]


def first_columns(arrays, widths):
    return pl.pallas_call(
        cut_kernel,
        out_shape=[
            jax.ShapeDtypeStruct((x.shape[0], n * LANES), x.dtype) for x, n in zip(arrays, widths)
        ],
        in_specs=[VMEM] * len(arrays),
        out_specs=[VMEM] * len(arrays),
        compiler_params=pltpu.CompilerParams(vmem_limit_bytes=16 * 1024 * 1024),
        name="first_columns",
    )(*arrays)


def join(held, arrived, cuts=None):
    rows, low = held[0].shape[0], jnp.bfloat16
    if cuts is None:
        cuts = [(k, 0, x.shape[1]) for k, x in enumerate(held)]
    return pl.pallas_call(
        functools.partial(join_kernel, cuts),
        out_shape=[jax.ShapeDtypeStruct((2 * rows, b - a), low) for _, a, b in cuts],
        in_specs=[VMEM] * (2 * len(held)),
        out_specs=[VMEM] * len(cuts),
        compiler_params=pltpu.CompilerParams(vmem_limit_bytes=16 * 1024 * 1024),
        name="join",
    )(*held, *arrived)


def gather(pairs):
    ready = []
    for p, x in enumerate(pairs):
        (held,) = join([x], [exchange(x, 2 * p, 0)])
        edge = WIDTHS[2 * p]
        cuts = [(0, 0, edge), (0, edge, held.shape[1])]
        held = join([held], [exchange(held, 2 * p, 1)], cuts)
        held = join(held, [exchange(y, 2 * p + k, 2) for k, y in enumerate(held)])
        arrived = [exchange(y, 2 * p + k, 3) for k, y in enumerate(held)]
        held = join(held, arrived)
        ready.append((held, [exchange(y, 2 * p + k, 4) for k, y in enumerate(held)]))
    one, two = [], []
    for p, (held, arrived) in enumerate(ready):
        kept = first_columns(held, FIRST[2 * p : 2 * p + 2])
        early = [exchange(x, 2 * p + k, 5) for k, x in enumerate(kept)]
        come = first_columns(arrived, FIRST[2 * p : 2 * p + 2])
        late = [exchange(x, 2 * p + k, 5) for k, x in enumerate(come)]
        for k in range(2):
            one += [kept[k], come[k], early[k], late[k]]
        cuts = [(k, FIRST[2 * p + k] * LANES, y.shape[1]) for k, y in enumerate(held)]
        halves = join(held, arrived, cuts)
        for k, y in enumerate(halves):
            two += [y, exchange(y, 2 * p + k, 5)]
    return one, two


def place_blocks(at, pieces, weight, sems, widths, colors, first=0):
    begin = starts(widths)
    parts = len(pieces) // len(widths)
    slots = 64 // parts
    for c in colors:
        columns = pl.ds(begin[c], widths[c] * LANES)
        for k in range(parts):

            def copy_four(high, carry, c=c, k=k, columns=columns):
                moved = at ^ place(first + c, slots * k)
                for bit in range(slots.bit_length() - 3):
                    moved = moved ^ ((high >> bit & 1) * place(first + c, 4 << bit))
                for low in range(4):
                    to = (moved ^ place(first + c, low)) * HALF_ROWS
                    origin = (high * 4 + low) * HALF_ROWS
                    pltpu.make_async_copy(
                        pieces[parts * c + k].at[
                            pl.ds(pl.multiple_of(origin, HALF_ROWS), HALF_ROWS), :
                        ],
                        weight.at[pl.ds(pl.multiple_of(to, HALF_ROWS), HALF_ROWS), columns],
                        sems.at[c],
                    ).start()
                return carry

            lax.fori_loop(0, slots // 4, copy_four, 0)


def wait_color(weight, sems, widths, c):
    columns = pl.ds(starts(widths)[c], widths[c] * LANES)
    part = weight.at[:, columns]
    pltpu.make_async_copy(part, part, sems.at[c]).wait()


def silu_product(gate, up):
    return (gate / (1.0 + jnp.exp(-gate)) * up).astype(jnp.bfloat16)


def narrow_step(normed, weight):
    both = dot(normed, weight)
    tile = [both[:, k * LANES : (k + 1) * LANES] for k in range(6)]
    gate = jnp.concatenate([tile[0], tile[1], tile[4]], axis=1)
    up = jnp.concatenate([tile[2], tile[3], tile[5]], axis=1)
    return silu_product(gate, up)


def hidden_step(step, normed, weight, hidden):
    @pl.when((step >= 0) & (step < 4))
    def _():
        columns = pl.ds(pl.multiple_of(step * WIDE, WIDE), WIDE)
        both = dot(normed[...], weight[:, columns])
        to = pl.ds(pl.multiple_of(step * (WIDE // 2), WIDE // 2), WIDE // 2)
        hidden[:, to] = silu_product(both[:, : WIDE // 2], both[:, WIDE // 2 :])

    @pl.when(step == 4)
    def _():
        hidden[:, 2 * WIDE :] = narrow_step(normed[...], weight[:, 4 * WIDE :])


def first_kernel(core, at, own, other, gain, *rest):
    pieces, (hidden, kept, weight, normed, sems, out_sems) = rest[:24], rest[24:]
    step = pl.program_id(0)
    begin = starts(FIRST)
    copies = []
    for c in range(6):
        columns = pl.ds(begin[c], FIRST[c] * LANES)
        copies.append(
            pltpu.make_async_copy(weight.at[:, columns], kept.at[:, columns], out_sems.at[c])
        )

    for k, colors in enumerate(((0, 1, 2), (3,), (4,), (5,))):

        @pl.when(step == k)
        def _():
            place_blocks(at[0], pieces, weight, sems, FIRST, colors)

    @pl.when(step == 0)
    def _():
        left = jnp.where(core[0] == 0, own[...], other[...])
        right = jnp.where(core[0] == 0, other[...], own[...])
        values = jnp.concatenate([left, right], axis=1).astype(jnp.float32)
        normed[...] = normed_rows(values, gain[...])

    for c in range(6):

        @pl.when(step == min(c, 4))
        def _():
            wait_color(weight, sems, FIRST, c)
            copies[c].start()

    hidden_step(step, normed, weight, hidden)

    @pl.when(step == 4)
    def _():
        for copy in copies:
            copy.wait()


def first_hidden(core, at, own, other, gain, pieces):
    count, half = own.shape
    width = 2 * half
    columns = sum(FIRST) * LANES
    units = columns // 2
    return pl.pallas_call(
        first_kernel,
        out_shape=[
            jax.ShapeDtypeStruct((count, units), jnp.bfloat16),
            jax.ShapeDtypeStruct((width, columns), jnp.bfloat16),
        ],
        grid_spec=pltpu.PrefetchScalarGridSpec(
            num_scalar_prefetch=2,
            grid=(5,),
            in_specs=[whole((count, half)), whole((count, half)), whole((1, width))] + [ANY] * 24,
            out_specs=[whole((count, units)), ANY],
            scratch_shapes=[
                pltpu.VMEM((width, columns), jnp.bfloat16),
                pltpu.VMEM((count, width), jnp.bfloat16),
                pltpu.SemaphoreType.DMA((6,)),
                pltpu.SemaphoreType.DMA((6,)),
            ],
        ),
        compiler_params=params(1),
        cost_estimate=cost(2 * count * width * columns, 4 * width * columns, count * units),
        name="first_hidden",
    )(core, at, own, other, gain, *pieces)


MIXER, DOWN = OTHERS[:3], OTHERS[3:]


def place_blocks_of(at, pieces, weight, sems, widths, first):
    place_blocks(at, pieces, weight, sems, widths, range(len(widths)), first)


def down_kernel(at, hidden, *rest):
    pieces, (term, kept, weight, sems, out_sem) = rest[:6], rest[6:]
    step = pl.program_id(0)
    copy = pltpu.make_async_copy(weight, kept, out_sem)

    @pl.when(step == 0)
    def _():
        place_blocks_of(at[0], pieces, weight, sems, DOWN, 3)
        for c in range(3):
            wait_color(weight, sems, DOWN, c)
        copy.start()

    rows = pl.ds(pl.multiple_of(step * WIDE, WIDE), WIDE)
    term[...] = dot_rows(hidden[...], weight[rows, :]).astype(jnp.bfloat16)

    @pl.when(step == pl.num_programs(0) - 1)
    def _():
        copy.wait()


def first_down(at, hidden, width, pieces):
    count, units = hidden.shape
    return pl.pallas_call(
        down_kernel,
        out_shape=[
            jax.ShapeDtypeStruct((count, width), jnp.bfloat16),
            jax.ShapeDtypeStruct((width, units), jnp.bfloat16),
        ],
        grid_spec=pltpu.PrefetchScalarGridSpec(
            num_scalar_prefetch=1,
            grid=(width // WIDE,),
            in_specs=[whole((count, units))] + [ANY] * 6,
            out_specs=[spec((count, WIDE), lambda j, a: (0, j)), ANY],
            scratch_shapes=[
                pltpu.VMEM((width, units), jnp.bfloat16),
                pltpu.SemaphoreType.DMA((3,)),
                pltpu.SemaphoreType.DMA,
            ],
        ),
        compiler_params=params(1),
        cost_estimate=cost(2 * count * width * units, 4 * width * units, 0),
        name="first_down",
    )(at, hidden, *pieces)


def assemble_kernel(at, *rest):
    pieces, (kept, weight, sems, out_sems) = rest[:6], rest[6:]
    place_blocks_of(at[0], pieces, weight, sems, MIXER, 0)
    begin = starts(MIXER)
    copies = []
    for c in range(3):
        wait_color(weight, sems, MIXER, c)
        columns = pl.ds(begin[c], MIXER[c] * LANES)
        copy = pltpu.make_async_copy(weight.at[:, columns], kept.at[:, columns], out_sems.at[c])
        copy.start()
        copies.append(copy)
    for copy in copies:
        copy.wait()


def assemble(at, width, pieces):
    shape = (width, sum(MIXER) * LANES)
    return pl.pallas_call(
        assemble_kernel,
        out_shape=jax.ShapeDtypeStruct(shape, jnp.bfloat16),
        grid_spec=pltpu.PrefetchScalarGridSpec(
            num_scalar_prefetch=1,
            grid=(1,),
            in_specs=[ANY] * 6,
            out_specs=ANY,
            scratch_shapes=[
                pltpu.VMEM(shape, jnp.bfloat16),
                pltpu.SemaphoreType.DMA((3,)),
                pltpu.SemaphoreType.DMA((3,)),
            ],
        ),
        compiler_params=params(1),
        cost_estimate=cost(5 * 10**9, 8 * shape[0] * shape[1], 0),
        name="assemble",
    )(at, *pieces)


def gates_kernel(core, own, other, term, far, gain, rows, middle, act, sums, normed):
    @pl.when(pl.program_id(0) == 0)
    def _():
        left = jnp.where(core[0] == 0, own[...], other[...])
        right = jnp.where(core[0] == 0, other[...], own[...])
        values = jnp.concatenate([left, right], axis=1).astype(jnp.float32)
        values = values + 0.5 * (term[...].astype(jnp.float32) + far[...].astype(jnp.float32))
        mid = values.astype(jnp.bfloat16)
        middle[...] = mid
        normed[...] = normed_rows(mid.astype(jnp.float32), gain[...])

    acted = gelu(dot(normed[...], rows[...]))
    act[0] = acted

    @pl.when(pl.program_id(0) == 0)
    def _():
        lane = lax.broadcasted_iota(jnp.int32, sums.shape, 1)
        total = jnp.sum(acted, axis=1, keepdims=True)
        squares = jnp.sum(acted * acted, axis=1, keepdims=True)
        sums[...] = jnp.where(lane == 0, total, squares)


def gates(core, own, other, term, far, gain, weight, chans):
    count, half = own.shape
    width = 2 * half
    return pl.pallas_call(
        gates_kernel,
        out_shape=[
            jax.ShapeDtypeStruct((count, width), jnp.bfloat16),
            jax.ShapeDtypeStruct((2, count, chans), jnp.float32),
            jax.ShapeDtypeStruct((count, LANES), jnp.float32),
        ],
        grid_spec=pltpu.PrefetchScalarGridSpec(
            num_scalar_prefetch=1,
            grid=(2,),
            in_specs=[
                whole((count, half)),
                whole((count, half)),
                whole((count, width)),
                whole((count, width)),
                whole((1, width)),
                spec((width, chans), lambda i, c: (0, 2 - i)),
            ],
            out_specs=[
                whole((count, width)),
                spec((1, count, chans), lambda i, c: (i, 0, 0)),
                whole((count, LANES)),
            ],
            scratch_shapes=[pltpu.VMEM((count, width), jnp.bfloat16)],
        ),
        compiler_params=params(1),
        cost_estimate=cost(4 * count * width * chans, 4 * width * chans, 2 * count * chans),
        name="gates",
    )(core, own, other, term, far, gain, weight)


def mix_kernel(act, sums, far, gain, bias, weight, shift, rows, term, mixed):
    groups = weight.shape[0]

    @pl.when(pl.program_id(0) == 0)
    def _():
        at = lax.broadcasted_iota(jnp.int32, (SPAN, SPAN), 0)
        source = lax.broadcasted_iota(jnp.int32, (SPAN, SPAN), 1)
        masked = [
            jnp.where(source <= at, weight[g], jnp.zeros_like(weight[g])) for g in range(groups)
        ]
        count, chans = mixed.shape
        wide = chans // groups
        column = [
            jnp.sum(jnp.where(source == at, shift[g : g + 1, :], 0.0), axis=1, keepdims=True)
            for g in range(groups)
        ]
        for n in range(count // SPAN):
            block = pl.ds(n * SPAN, SPAN)
            totals = (sums[block, :] + far[block, :]) / BW
            v_mean = totals[:, 0:1]
            v_var = totals[:, 1:2] - v_mean * v_mean
            v_normed = (act[0, block, :] - v_mean) * lax.rsqrt(v_var + EPS) * gain[...] + bias[...]
            v_normed = v_normed.astype(jnp.bfloat16)
            spatial = [
                dot(masked[g], v_normed[:, g * wide : (g + 1) * wide]) + column[g]
                for g in range(groups)
            ]
            product = act[1, block, :] * jnp.concatenate(spatial, axis=1)
            mixed[block, :] = product.astype(jnp.bfloat16)

    term[...] = dot_rows(mixed[...], rows[...]).astype(jnp.bfloat16)


def mix(act, sums, far, gain, bias, weight, shift, rows):
    _, count, chans = act.shape
    width = rows.shape[0]
    groups = weight.shape[0]
    return pl.pallas_call(
        mix_kernel,
        out_shape=jax.ShapeDtypeStruct((count, width), jnp.bfloat16),
        grid=(width // WIDE,),
        in_specs=[
            whole(act.shape),
            whole((count, LANES)),
            whole((count, LANES)),
            whole((1, chans)),
            whole((1, chans)),
            whole((groups, SPAN, SPAN)),
            whole((groups, SPAN)),
            spec((WIDE, chans), lambda j: (j, 0)),
        ],
        out_specs=spec((count, WIDE), lambda j: (0, j)),
        scratch_shapes=[pltpu.VMEM((count, chans), jnp.bfloat16)],
        compiler_params=params(1),
        cost_estimate=cost(2 * count * width * chans, 2 * width * chans, count),
        name="mix",
    )(act, sums, far, gain, bias, weight, shift, rows)


def second_kernel(
    core, middle, term, far, gain, first, others, send, keep, base, normed, hidden, wide, down, sems
):
    step = pl.program_id(0)
    steps = 5
    outs = down.shape[0] // WIDE
    cuts = [pl.ds(k * WIDE, WIDE) for k in range(4)] + [pl.ds(4 * WIDE, 6 * LANES)]
    copies = [
        pltpu.make_async_copy(first.at[:, cut], wide.at[:, cut], sems.at[k])
        for k, cut in enumerate(cuts)
    ]
    copies.append(pltpu.make_async_copy(others, down, sems.at[steps]))

    @pl.when(step == 0)
    def _():
        for copy in copies:
            copy.start()
        values = middle[...].astype(jnp.float32) + (
            term[...].astype(jnp.float32) + far[...].astype(jnp.float32)
        )
        second = values.astype(jnp.bfloat16)
        half = second.shape[1] // 2
        base[...] = jnp.where(core[0] == 0, second[:, :half], second[:, half:])
        normed[...] = normed_rows(second.astype(jnp.float32), gain[...])

    for k, copy in enumerate(copies):

        @pl.when(step == k)
        def _():
            copy.wait()

    hidden_step(step, normed, wide, hidden)

    @pl.when(step >= steps)
    def _():
        n = step - steps
        mine = jnp.where(n < outs // 2, 1 - core[0], core[0])
        row = mine * (outs // 2) + lax.rem(n, outs // 2)
        rows = pl.ds(pl.multiple_of(row * WIDE, WIDE), WIDE)
        part = dot_rows(hidden[...], down[rows, :]).astype(jnp.bfloat16)

        @pl.when(n < outs // 2)
        def _():
            send[...] = part

        @pl.when(n >= outs // 2)
        def _():
            keep[...] = part


def second_pass(core, middle, term, far, gain, first, others):
    count, width = middle.shape
    half = width // 2
    columns = first.shape[1]
    units = columns // 2
    outs = width // WIDE
    sent = outs // 2
    return pl.pallas_call(
        second_kernel,
        out_shape=[jax.ShapeDtypeStruct((count, half), jnp.bfloat16)] * 3,
        grid_spec=pltpu.PrefetchScalarGridSpec(
            num_scalar_prefetch=1,
            grid=(5 + outs,),
            in_specs=[
                whole((count, width)),
                whole((count, width)),
                whole((count, width)),
                whole((1, width)),
                ANY,
                ANY,
            ],
            out_specs=[
                spec((count, WIDE), lambda j, c: (0, jnp.clip(j - 5, 0, sent - 1))),
                spec((count, WIDE), lambda j, c: (0, jnp.maximum(j - 5 - sent, 0))),
                whole((count, half)),
            ],
            scratch_shapes=[
                pltpu.VMEM((count, width), jnp.bfloat16),
                pltpu.VMEM((count, units), jnp.bfloat16),
                pltpu.VMEM((width, columns), jnp.bfloat16),
                pltpu.VMEM((width, units), jnp.bfloat16),
                pltpu.SemaphoreType.DMA((6,)),
            ],
        ),
        compiler_params=params(1),
        cost_estimate=cost(6 * count * width * units, 6 * width * units, count * units),
        name="second_pass",
    )(core, middle, term, far, gain, first, others)


def layer(
    tokens,
    norm_first,
    norm_mix,
    norm_second,
    gate_weight,
    up_weight,
    down_weight,
    gate_scale,
    up_scale,
    down_scale,
    u_weight,
    v_weight,
    u_scale,
    v_scale,
    ln_gain,
    ln_bias,
    spatial_weight,
    spatial_bias,
    out_weight,
    out_scale,
):
    chans = u_weight.shape[1]
    width = 2 * tokens.shape[1]

    def number(x):
        return x.reshape(1).astype(jnp.int32)

    core = number(lax.axis_index("tp"))
    rep = lax.axis_index("rep")
    at = number(2 * lax.axis_index(FS) + rep)

    colors = prepare(
        number(rep),
        gate_weight,
        up_weight,
        down_weight.T,
        u_weight,
        v_weight,
        out_weight.T,
        gate_scale,
        up_scale,
        down_scale,
        u_scale,
        v_scale,
        out_scale,
    )
    one, two = gather(colors)

    own, other = tokens, other_core(tokens)
    hidden, first = first_hidden(core, at, own, other, norm_first[None], one)
    term, down = first_down(at, hidden, width, two[6:])
    far = other_core(term)
    mixer = assemble(at, width, two[:6])
    middle, act, sums = gates(core, own, other, term, far, norm_mix[None], mixer, chans)
    term = mix(
        act,
        sums,
        other_core(sums),
        ln_gain[None],
        ln_bias[None],
        spatial_weight,
        spatial_bias,
        mixer,
    )
    send, keep, base = second_pass(
        core, middle, term, other_core(term), norm_second[None], first, down
    )
    last = keep.astype(jnp.float32) + other_core(send).astype(jnp.float32)
    return (base.astype(jnp.float32) + 0.5 * last).astype(jnp.bfloat16)


def solution(mesh):
    torus = Mesh(
        mesh.devices.reshape(mesh.shape["rep"], 2, 4, 4, mesh.shape["tp"]),
        ("rep", "fs_0", "fs_1", "fs_2", "tp"),
    )
    in_specs = (
        P(REP_FS, "tp"),
        P(),
        P(),
        P(),
        P(FS, "tp"),
        P(FS, "tp"),
        P("tp", FS),
        P("tp"),
        P("tp"),
        P(FS),
        P(FS, "tp"),
        P(FS, "tp"),
        P("tp"),
        P("tp"),
        P("tp"),
        P("tp"),
        P("tp", None, None),
        P("tp", None),
        P("tp", FS),
        P(FS),
    )
    out_specs = P(REP_FS, "tp")
    return jax.shard_map(layer, mesh=torus, in_specs=in_specs, out_specs=out_specs, check_vma=False)
```

```python
import functools

import jax
import jax.numpy as jnp
from jax import lax
from jax.experimental import pallas as pl
from jax.experimental.pallas import tpu as pltpu
from jax.sharding import Mesh
from jax.sharding import PartitionSpec as P


BW = 1024
SPAN = 128
FS = ("fs_0", "fs_1", "fs_2")
REP_FS = ("rep", "fs_0", "fs_1", "fs_2")
LANES = 128
WIDE = 512
HALF_ROWS = 32
FIRST = (4, 4, 4, 4, 3, 3)
OTHERS = (4, 4, 4, 3, 4, 4)
RINGS = (("fs_2", 1), ("fs_1", 1), ("z", 1), ("fs_2", 3), ("fs_1", 3), ("z", 3))
PLACES = (2, 8, 32, 6, 24, 33)
ROUNDS = (
    (0, 4, 5, 3, 2, 1),
    (0, 4, 3, 5, 1, 2),
    (1, 5, 4, 2, 3, 0),
    (1, 5, 2, 4, 0, 3),
    (2, 3, 1, 0, 5, 4),
    (2, 3, 0, 1, 4, 5),
)

EPS = 1e-06


def other_core(x):
    return lax.ppermute(x, "tp", [(0, 1), (1, 0)])


def normed_rows(values, gain):
    factor = lax.rsqrt(jnp.mean(values * values, axis=1, keepdims=True) + EPS)
    return (values * factor * gain).astype(jnp.bfloat16)


def dot(left, right):
    return jnp.dot(left, right, preferred_element_type=jnp.float32)


def dot_rows(left, rows):
    return lax.dot_general(
        left, rows, (((1,), (1,)), ((), ())), preferred_element_type=jnp.float32
    )


def gelu(a):
    return 0.5 * a * (1.0 + jnp.tanh(0.7978845608028654 * (a + 0.044715 * a * a * a)))


def spec(block, index):
    return pl.BlockSpec(block, index)


def whole(shape):
    return pl.BlockSpec(shape, lambda *_: (0,) * len(shape))


ANY = pl.BlockSpec(memory_space=pl.ANY)


def params(steps):
    return pltpu.CompilerParams(
        dimension_semantics=("arbitrary",) * steps, vmem_limit_bytes=60 * 1024 * 1024
    )


def cost(flops, moved, special):
    return pl.CostEstimate(flops=flops, bytes_accessed=moved, transcendentals=special)


def exchange(x, color, turn):
    name, flip = RINGS[ROUNDS[color][turn]]
    axis = ("rep", "fs_0") if name == "z" else name
    return lax.ppermute(x, axis, [(i, i ^ flip) for i in range(4)])


def place(color, slot):
    at = 0
    for turn in range(6):
        if slot >> turn & 1:
            at ^= PLACES[ROUNDS[color][turn]]
    return at


def starts(widths):
    ends = [0]
    for n in widths:
        ends.append(ends[-1] + n * LANES)
    return ends


PAIRS = [(p, t + k) for t in (0, 2, 4, 6) for p in (0, 1) for k in (0, 1)]
PAIRS += [(0, 8), (0, 9), (1, 8), (1, 9), (0, 10), (1, 10)]


def prepare_kernel(rep, *refs):
    inputs, colors, held, sems = refs[:12], refs[12:15], refs[15:27], refs[27]
    copies = [
        pltpu.make_async_copy(x, y, sems.at[k]) for k, (x, y) in enumerate(zip(inputs, held))
    ]
    for copy in copies:
        copy.start()
    for copy in copies:
        copy.wait()
    gate, up, down, u, v, out, gate_s, up_s, down_s, u_s, v_s, out_s = held
    rows = pl.ds(pl.multiple_of(rep[0] * HALF_ROWS, HALF_ROWS), HALF_ROWS)
    low = jnp.bfloat16

    def across(scale):
        return scale[...][None, :]

    def down_rows(scale):
        size = scale.shape[0]
        row = lax.broadcasted_iota(jnp.int32, (HALF_ROWS, size), 0) + rep[0] * HALF_ROWS
        column = lax.broadcasted_iota(jnp.int32, (HALF_ROWS, size), 1)
        return jnp.sum(jnp.where(row == column, across(scale), 0.0), axis=1, keepdims=True)

    pair = ((gate[rows, :] * across(gate_s)).astype(low), (up[rows, :] * across(up_s)).astype(low))
    firsts = [pair[p][:, t * LANES : (t + 1) * LANES] for p, t in PAIRS]
    rest = jnp.concatenate(
        [
            (out[rows, :] * down_rows(out_s)).astype(low),
            (u[rows, :] * across(u_s)).astype(low),
            (v[rows, :] * across(v_s)).astype(low),
            (down[rows, :] * down_rows(down_s)).astype(low),
        ],
        axis=1,
    )
    at, begin = 0, starts(OTHERS)
    mine = []
    for c in range(6):
        mine.append(firsts[at : at + FIRST[c]] + [rest[:, begin[c] : begin[c + 1]]])
        at += FIRST[c]
    for pair, ref in enumerate(colors):
        ref[...] = jnp.concatenate(mine[2 * pair] + mine[2 * pair + 1], axis=1)


WIDTHS = [(a + b) * LANES for a, b in zip(FIRST, OTHERS)]
VMEM = pl.BlockSpec(memory_space=pltpu.VMEM)
SMEM = pl.BlockSpec(memory_space=pltpu.SMEM)
HBM = pl.BlockSpec(memory_space=pltpu.HBM)


def prepare(rep, *arrays):
    pairs = [WIDTHS[k] + WIDTHS[k + 1] for k in (0, 2, 4)]
    return pl.pallas_call(
        prepare_kernel,
        out_shape=[jax.ShapeDtypeStruct((HALF_ROWS, n), jnp.bfloat16) for n in pairs],
        in_specs=[SMEM] + [HBM] * len(arrays),
        out_specs=[VMEM] * 3,
        scratch_shapes=[pltpu.VMEM(x.shape, x.dtype) for x in arrays]
        + [pltpu.SemaphoreType.DMA((len(arrays),))],
        compiler_params=pltpu.CompilerParams(vmem_limit_bytes=60 * 1024 * 1024),
        name="prepare",
    )(rep, *arrays)


def join_kernel(cuts, *refs):
    sources = (len(refs) - len(cuts)) // 2
    for joined, (source, begin, end) in zip(refs[2 * sources :], cuts):
        held, arrived = refs[source], refs[sources + source]
        rows = held.shape[0]
        joined[pl.ds(0, rows), :] = held[:, begin:end]
        joined[pl.ds(rows, rows), :] = arrived[:, begin:end]


def cut_kernel(*refs):
    for k in range(len(refs) // 2):
        refs[len(refs) // 2 + k][...] = refs[k][:, : refs[len(refs) // 2 + k].shape[1]]


def first_columns(arrays, widths):
    return pl.pallas_call(
        cut_kernel,
        out_shape=[
            jax.ShapeDtypeStruct((x.shape[0], n * LANES), x.dtype) for x, n in zip(arrays, widths)
        ],
        in_specs=[VMEM] * len(arrays),
        out_specs=[VMEM] * len(arrays),
        compiler_params=pltpu.CompilerParams(vmem_limit_bytes=16 * 1024 * 1024),
        name="first_columns",
    )(*arrays)


def join(held, arrived, cuts=None):
    rows, low = held[0].shape[0], jnp.bfloat16
    if cuts is None:
        cuts = [(k, 0, x.shape[1]) for k, x in enumerate(held)]
    return pl.pallas_call(
        functools.partial(join_kernel, cuts),
        out_shape=[jax.ShapeDtypeStruct((2 * rows, b - a), low) for _, a, b in cuts],
        in_specs=[VMEM] * (2 * len(held)),
        out_specs=[VMEM] * len(cuts),
        compiler_params=pltpu.CompilerParams(vmem_limit_bytes=16 * 1024 * 1024),
        name="join",
    )(*held, *arrived)


def gather(pairs):
    ready = []
    for p, x in enumerate(pairs):
        (held,) = join([x], [exchange(x, 2 * p, 0)])
        edge = WIDTHS[2 * p]
        cuts = [(0, 0, edge), (0, edge, held.shape[1])]
        held = join([held], [exchange(held, 2 * p, 1)], cuts)
        held = join(held, [exchange(y, 2 * p + k, 2) for k, y in enumerate(held)])
        arrived = [exchange(y, 2 * p + k, 3) for k, y in enumerate(held)]
        held = join(held, arrived)
        ready.append((held, [exchange(y, 2 * p + k, 4) for k, y in enumerate(held)]))
    one, two = [], []
    for p, (held, arrived) in enumerate(ready):
        kept = first_columns(held, FIRST[2 * p : 2 * p + 2])
        early = [exchange(x, 2 * p + k, 5) for k, x in enumerate(kept)]
        come = first_columns(arrived, FIRST[2 * p : 2 * p + 2])
        late = [exchange(x, 2 * p + k, 5) for k, x in enumerate(come)]
        for k in range(2):
            one += [kept[k], come[k], early[k], late[k]]
        cuts = [(k, FIRST[2 * p + k] * LANES, y.shape[1]) for k, y in enumerate(held)]
        halves = join(held, arrived, cuts)
        for k, y in enumerate(halves):
            two += [y, exchange(y, 2 * p + k, 5)]
    return one, two


def place_blocks(at, pieces, weight, sems, widths, colors, first=0):
    begin = starts(widths)
    parts = len(pieces) // len(widths)
    slots = 64 // parts
    for c in colors:
        columns = pl.ds(begin[c], widths[c] * LANES)
        for k in range(parts):

            def copy_four(high, carry, c=c, k=k, columns=columns):
                moved = at ^ place(first + c, slots * k)
                for bit in range(slots.bit_length() - 3):
                    moved = moved ^ ((high >> bit & 1) * place(first + c, 4 << bit))
                for low in range(4):
                    to = (moved ^ place(first + c, low)) * HALF_ROWS
                    origin = (high * 4 + low) * HALF_ROWS
                    pltpu.make_async_copy(
                        pieces[parts * c + k].at[
                            pl.ds(pl.multiple_of(origin, HALF_ROWS), HALF_ROWS), :
                        ],
                        weight.at[pl.ds(pl.multiple_of(to, HALF_ROWS), HALF_ROWS), columns],
                        sems.at[c],
                    ).start()
                return carry

            lax.fori_loop(0, slots // 4, copy_four, 0)


def wait_color(weight, sems, widths, c):
    columns = pl.ds(starts(widths)[c], widths[c] * LANES)
    part = weight.at[:, columns]
    pltpu.make_async_copy(part, part, sems.at[c]).wait()


def silu_product(gate, up):
    return (gate / (1.0 + jnp.exp(-gate)) * up).astype(jnp.bfloat16)


def narrow_step(normed, weight):
    both = dot(normed, weight)
    tile = [both[:, k * LANES : (k + 1) * LANES] for k in range(6)]
    gate = jnp.concatenate([tile[0], tile[1], tile[4]], axis=1)
    up = jnp.concatenate([tile[2], tile[3], tile[5]], axis=1)
    return silu_product(gate, up)


def hidden_step(step, normed, weight, hidden):
    @pl.when((step >= 0) & (step < 4))
    def _():
        columns = pl.ds(pl.multiple_of(step * WIDE, WIDE), WIDE)
        both = dot(normed[...], weight[:, columns])
        to = pl.ds(pl.multiple_of(step * (WIDE // 2), WIDE // 2), WIDE // 2)
        hidden[:, to] = silu_product(both[:, : WIDE // 2], both[:, WIDE // 2 :])

    @pl.when(step == 4)
    def _():
        hidden[:, 2 * WIDE :] = narrow_step(normed[...], weight[:, 4 * WIDE :])


def first_kernel(core, at, own, other, gain, *rest):
    pieces, (hidden, kept, weight, normed, sems, out_sems) = rest[:24], rest[24:]
    step = pl.program_id(0)
    begin = starts(FIRST)
    copies = []
    for c in range(6):
        columns = pl.ds(begin[c], FIRST[c] * LANES)
        copies.append(
            pltpu.make_async_copy(weight.at[:, columns], kept.at[:, columns], out_sems.at[c])
        )

    for k, colors in enumerate(((0, 1, 2), (3,), (4,), (5,))):

        @pl.when(step == k)
        def _():
            place_blocks(at[0], pieces, weight, sems, FIRST, colors)

    @pl.when(step == 0)
    def _():
        left = jnp.where(core[0] == 0, own[...], other[...])
        right = jnp.where(core[0] == 0, other[...], own[...])
        values = jnp.concatenate([left, right], axis=1).astype(jnp.float32)
        normed[...] = normed_rows(values, gain[...])

    for c in range(6):

        @pl.when(step == min(c, 4))
        def _():
            wait_color(weight, sems, FIRST, c)
            copies[c].start()

    hidden_step(step, normed, weight, hidden)

    @pl.when(step == 4)
    def _():
        for copy in copies:
            copy.wait()


def first_hidden(core, at, own, other, gain, pieces):
    count, half = own.shape
    width = 2 * half
    columns = sum(FIRST) * LANES
    units = columns // 2
    return pl.pallas_call(
        first_kernel,
        out_shape=[
            jax.ShapeDtypeStruct((count, units), jnp.bfloat16),
            jax.ShapeDtypeStruct((width, columns), jnp.bfloat16),
        ],
        grid_spec=pltpu.PrefetchScalarGridSpec(
            num_scalar_prefetch=2,
            grid=(5,),
            in_specs=[whole((count, half)), whole((count, half)), whole((1, width))] + [ANY] * 24,
            out_specs=[whole((count, units)), ANY],
            scratch_shapes=[
                pltpu.VMEM((width, columns), jnp.bfloat16),
                pltpu.VMEM((count, width), jnp.bfloat16),
                pltpu.SemaphoreType.DMA((6,)),
                pltpu.SemaphoreType.DMA((6,)),
            ],
        ),
        compiler_params=params(1),
        cost_estimate=cost(2 * count * width * columns, 4 * width * columns, count * units),
        name="first_hidden",
    )(core, at, own, other, gain, *pieces)


MIXER, DOWN = OTHERS[:3], OTHERS[3:]


def place_blocks_of(at, pieces, weight, sems, widths, first):
    place_blocks(at, pieces, weight, sems, widths, range(len(widths)), first)


QUARTER = WIDE // HALF_ROWS


def down_kernel(at, hidden, *rest):
    pieces, (term, kept, weight, sems, out_sems) = rest[:6], rest[6:]
    step = pl.program_id(0)
    begin = starts(DOWN)

    @pl.when(step == 0)
    def _():
        for quarter in range(4):
            for c in range(3):
                columns = pl.ds(begin[c], DOWN[c] * LANES)
                for slot in range(64):
                    moved = place(3 + c, slot)
                    if moved // QUARTER != quarter:
                        continue
                    to = pl.multiple_of((at[0] ^ moved) * HALF_ROWS, HALF_ROWS)
                    pltpu.make_async_copy(
                        pieces[2 * c + slot // 32].at[
                            pl.ds(slot % 32 * HALF_ROWS, HALF_ROWS), :
                        ],
                        weight.at[pl.ds(to, HALF_ROWS), columns],
                        sems.at[quarter],
                    ).start()

    def rows_of(quarter):
        block = ((at[0] // QUARTER) ^ quarter) * WIDE
        return pl.ds(pl.multiple_of(block, WIDE), WIDE)

    copies = []
    for quarter in range(4):
        part = weight.at[rows_of(quarter), :]
        copy = pltpu.make_async_copy(part, kept.at[rows_of(quarter), :], out_sems.at[quarter])
        copies.append(copy)

        @pl.when(step == quarter)
        def _():
            pltpu.make_async_copy(part, part, sems.at[quarter]).wait()
            copy.start()

    part = weight[rows_of(step), :]
    term[...] = dot_rows(hidden[...], part).astype(jnp.bfloat16)

    @pl.when(step == 3)
    def _():
        for copy in copies:
            copy.wait()


def first_down(at, hidden, width, pieces):
    count, units = hidden.shape
    return pl.pallas_call(
        down_kernel,
        out_shape=[
            jax.ShapeDtypeStruct((count, width), jnp.bfloat16),
            jax.ShapeDtypeStruct((width, units), jnp.bfloat16),
        ],
        grid_spec=pltpu.PrefetchScalarGridSpec(
            num_scalar_prefetch=1,
            grid=(width // WIDE,),
            in_specs=[whole((count, units))] + [ANY] * 6,
            out_specs=[spec((count, WIDE), lambda j, a: (0, (a[0] // QUARTER) ^ j)), ANY],
            scratch_shapes=[
                pltpu.VMEM((width, units), jnp.bfloat16),
                pltpu.SemaphoreType.DMA((4,)),
                pltpu.SemaphoreType.DMA((4,)),
            ],
        ),
        compiler_params=params(1),
        cost_estimate=cost(2 * count * width * units, 4 * width * units, 0),
        name="first_down",
    )(at, hidden, *pieces)


def assemble_kernel(at, *rest):
    pieces, (kept, weight, sems, out_sems) = rest[:6], rest[6:]
    place_blocks_of(at[0], pieces, weight, sems, MIXER, 0)
    begin = starts(MIXER)
    copies = []
    for c in range(3):
        wait_color(weight, sems, MIXER, c)
        columns = pl.ds(begin[c], MIXER[c] * LANES)
        copy = pltpu.make_async_copy(weight.at[:, columns], kept.at[:, columns], out_sems.at[c])
        copy.start()
        copies.append(copy)
    for copy in copies:
        copy.wait()


def assemble(at, width, pieces):
    shape = (width, sum(MIXER) * LANES)
    return pl.pallas_call(
        assemble_kernel,
        out_shape=jax.ShapeDtypeStruct(shape, jnp.bfloat16),
        grid_spec=pltpu.PrefetchScalarGridSpec(
            num_scalar_prefetch=1,
            grid=(1,),
            in_specs=[ANY] * 6,
            out_specs=ANY,
            scratch_shapes=[
                pltpu.VMEM(shape, jnp.bfloat16),
                pltpu.SemaphoreType.DMA((3,)),
                pltpu.SemaphoreType.DMA((3,)),
            ],
        ),
        compiler_params=params(1),
        cost_estimate=cost(5 * 10**9, 8 * shape[0] * shape[1], 0),
        name="assemble",
    )(at, *pieces)


def gates_kernel(core, own, other, term, far, gain, rows, middle, act, sums, normed):
    @pl.when(pl.program_id(0) == 0)
    def _():
        left = jnp.where(core[0] == 0, own[...], other[...])
        right = jnp.where(core[0] == 0, other[...], own[...])
        values = jnp.concatenate([left, right], axis=1).astype(jnp.float32)
        values = values + 0.5 * (term[...].astype(jnp.float32) + far[...].astype(jnp.float32))
        mid = values.astype(jnp.bfloat16)
        middle[...] = mid
        normed[...] = normed_rows(mid.astype(jnp.float32), gain[...])

    acted = gelu(dot(normed[...], rows[...]))
    act[0] = acted

    @pl.when(pl.program_id(0) == 0)
    def _():
        lane = lax.broadcasted_iota(jnp.int32, sums.shape, 1)
        total = jnp.sum(acted, axis=1, keepdims=True)
        squares = jnp.sum(acted * acted, axis=1, keepdims=True)
        sums[...] = jnp.where(lane == 0, total, squares)


def gates(core, own, other, term, far, gain, weight, chans):
    count, half = own.shape
    width = 2 * half
    return pl.pallas_call(
        gates_kernel,
        out_shape=[
            jax.ShapeDtypeStruct((count, width), jnp.bfloat16),
            jax.ShapeDtypeStruct((2, count, chans), jnp.float32),
            jax.ShapeDtypeStruct((count, LANES), jnp.float32),
        ],
        grid_spec=pltpu.PrefetchScalarGridSpec(
            num_scalar_prefetch=1,
            grid=(2,),
            in_specs=[
                whole((count, half)),
                whole((count, half)),
                whole((count, width)),
                whole((count, width)),
                whole((1, width)),
                spec((width, chans), lambda i, c: (0, 2 - i)),
            ],
            out_specs=[
                whole((count, width)),
                spec((1, count, chans), lambda i, c: (i, 0, 0)),
                whole((count, LANES)),
            ],
            scratch_shapes=[pltpu.VMEM((count, width), jnp.bfloat16)],
        ),
        compiler_params=params(1),
        cost_estimate=cost(4 * count * width * chans, 4 * width * chans, 2 * count * chans),
        name="gates",
    )(core, own, other, term, far, gain, weight)


def mix_kernel(act, sums, far, gain, bias, weight, shift, rows, term, mixed):
    groups = weight.shape[0]

    @pl.when(pl.program_id(0) == 0)
    def _():
        at = lax.broadcasted_iota(jnp.int32, (SPAN, SPAN), 0)
        source = lax.broadcasted_iota(jnp.int32, (SPAN, SPAN), 1)
        masked = [
            jnp.where(source <= at, weight[g], jnp.zeros_like(weight[g])) for g in range(groups)
        ]
        count, chans = mixed.shape
        wide = chans // groups
        column = [
            jnp.sum(jnp.where(source == at, shift[g : g + 1, :], 0.0), axis=1, keepdims=True)
            for g in range(groups)
        ]
        for n in range(count // SPAN):
            block = pl.ds(n * SPAN, SPAN)
            totals = (sums[block, :] + far[block, :]) / BW
            v_mean = totals[:, 0:1]
            v_var = totals[:, 1:2] - v_mean * v_mean
            v_normed = (act[0, block, :] - v_mean) * lax.rsqrt(v_var + EPS) * gain[...] + bias[...]
            v_normed = v_normed.astype(jnp.bfloat16)
            spatial = [
                dot(masked[g], v_normed[:, g * wide : (g + 1) * wide]) + column[g]
                for g in range(groups)
            ]
            product = act[1, block, :] * jnp.concatenate(spatial, axis=1)
            mixed[block, :] = product.astype(jnp.bfloat16)

    term[...] = dot_rows(mixed[...], rows[...]).astype(jnp.bfloat16)


def mix(act, sums, far, gain, bias, weight, shift, rows):
    _, count, chans = act.shape
    width = rows.shape[0]
    groups = weight.shape[0]
    return pl.pallas_call(
        mix_kernel,
        out_shape=jax.ShapeDtypeStruct((count, width), jnp.bfloat16),
        grid=(width // WIDE,),
        in_specs=[
            whole(act.shape),
            whole((count, LANES)),
            whole((count, LANES)),
            whole((1, chans)),
            whole((1, chans)),
            whole((groups, SPAN, SPAN)),
            whole((groups, SPAN)),
            spec((WIDE, chans), lambda j: (j, 0)),
        ],
        out_specs=spec((count, WIDE), lambda j: (0, j)),
        scratch_shapes=[pltpu.VMEM((count, chans), jnp.bfloat16)],
        compiler_params=params(1),
        cost_estimate=cost(2 * count * width * chans, 2 * width * chans, count),
        name="mix",
    )(act, sums, far, gain, bias, weight, shift, rows)


def second_kernel(
    core, middle, term, far, gain, first, others, send, keep, base, normed, hidden, wide, down, sems
):
    step = pl.program_id(0)
    steps = 5
    outs = down.shape[0] // WIDE
    cuts = [pl.ds(k * WIDE, WIDE) for k in range(4)] + [pl.ds(4 * WIDE, 6 * LANES)]
    copies = [
        pltpu.make_async_copy(first.at[:, cut], wide.at[:, cut], sems.at[k])
        for k, cut in enumerate(cuts)
    ]
    copies.append(pltpu.make_async_copy(others, down, sems.at[steps]))

    @pl.when(step == 0)
    def _():
        for copy in copies:
            copy.start()
        values = middle[...].astype(jnp.float32) + (
            term[...].astype(jnp.float32) + far[...].astype(jnp.float32)
        )
        second = values.astype(jnp.bfloat16)
        half = second.shape[1] // 2
        base[...] = jnp.where(core[0] == 0, second[:, :half], second[:, half:])
        normed[...] = normed_rows(second.astype(jnp.float32), gain[...])

    for k, copy in enumerate(copies):

        @pl.when(step == k)
        def _():
            copy.wait()

    hidden_step(step, normed, wide, hidden)

    @pl.when(step >= steps)
    def _():
        n = step - steps
        mine = jnp.where(n < outs // 2, 1 - core[0], core[0])
        row = mine * (outs // 2) + lax.rem(n, outs // 2)
        rows = pl.ds(pl.multiple_of(row * WIDE, WIDE), WIDE)
        part = dot_rows(hidden[...], down[rows, :]).astype(jnp.bfloat16)

        @pl.when(n < outs // 2)
        def _():
            send[...] = part

        @pl.when(n >= outs // 2)
        def _():
            keep[...] = part


def second_pass(core, middle, term, far, gain, first, others):
    count, width = middle.shape
    half = width // 2
    columns = first.shape[1]
    units = columns // 2
    outs = width // WIDE
    sent = outs // 2
    return pl.pallas_call(
        second_kernel,
        out_shape=[jax.ShapeDtypeStruct((count, half), jnp.bfloat16)] * 3,
        grid_spec=pltpu.PrefetchScalarGridSpec(
            num_scalar_prefetch=1,
            grid=(5 + outs,),
            in_specs=[
                whole((count, width)),
                whole((count, width)),
                whole((count, width)),
                whole((1, width)),
                ANY,
                ANY,
            ],
            out_specs=[
                spec((count, WIDE), lambda j, c: (0, jnp.clip(j - 5, 0, sent - 1))),
                spec((count, WIDE), lambda j, c: (0, jnp.maximum(j - 5 - sent, 0))),
                whole((count, half)),
            ],
            scratch_shapes=[
                pltpu.VMEM((count, width), jnp.bfloat16),
                pltpu.VMEM((count, units), jnp.bfloat16),
                pltpu.VMEM((width, columns), jnp.bfloat16),
                pltpu.VMEM((width, units), jnp.bfloat16),
                pltpu.SemaphoreType.DMA((6,)),
            ],
        ),
        compiler_params=params(1),
        cost_estimate=cost(6 * count * width * units, 6 * width * units, count * units),
        name="second_pass",
    )(core, middle, term, far, gain, first, others)


def layer(
    tokens,
    norm_first,
    norm_mix,
    norm_second,
    gate_weight,
    up_weight,
    down_weight,
    gate_scale,
    up_scale,
    down_scale,
    u_weight,
    v_weight,
    u_scale,
    v_scale,
    ln_gain,
    ln_bias,
    spatial_weight,
    spatial_bias,
    out_weight,
    out_scale,
):
    chans = u_weight.shape[1]
    width = 2 * tokens.shape[1]

    def number(x):
        return x.reshape(1).astype(jnp.int32)

    core = number(lax.axis_index("tp"))
    rep = lax.axis_index("rep")
    at = number(2 * lax.axis_index(FS) + rep)

    colors = prepare(
        number(rep),
        gate_weight,
        up_weight,
        down_weight.T,
        u_weight,
        v_weight,
        out_weight.T,
        gate_scale,
        up_scale,
        down_scale,
        u_scale,
        v_scale,
        out_scale,
    )
    one, two = gather(colors)

    own, other = tokens, other_core(tokens)
    hidden, first = first_hidden(core, at, own, other, norm_first[None], one)
    term, down = first_down(at, hidden, width, two[6:])
    far = other_core(term)
    mixer = assemble(at, width, two[:6])
    middle, act, sums = gates(core, own, other, term, far, norm_mix[None], mixer, chans)
    term = mix(
        act,
        sums,
        other_core(sums),
        ln_gain[None],
        ln_bias[None],
        spatial_weight,
        spatial_bias,
        mixer,
    )
    send, keep, base = second_pass(
        core, middle, term, other_core(term), norm_second[None], first, down
    )
    last = keep.astype(jnp.float32) + other_core(send).astype(jnp.float32)
    return (base.astype(jnp.float32) + 0.5 * last).astype(jnp.bfloat16)


def solution(mesh):
    torus = Mesh(
        mesh.devices.reshape(mesh.shape["rep"], 2, 4, 4, mesh.shape["tp"]),
        ("rep", "fs_0", "fs_1", "fs_2", "tp"),
    )
    in_specs = (
        P(REP_FS, "tp"),
        P(),
        P(),
        P(),
        P(FS, "tp"),
        P(FS, "tp"),
        P("tp", FS),
        P("tp"),
        P("tp"),
        P(FS),
        P(FS, "tp"),
        P(FS, "tp"),
        P("tp"),
        P("tp"),
        P("tp"),
        P("tp"),
        P("tp", None, None),
        P("tp", None),
        P("tp", FS),
        P(FS),
    )
    out_specs = P(REP_FS, "tp")
    return jax.shard_map(layer, mesh=torus, in_specs=in_specs, out_specs=out_specs, check_vma=False)
```

```python
import functools

import jax
import jax.numpy as jnp
from jax import lax
from jax.experimental import pallas as pl
from jax.experimental.pallas import tpu as pltpu
from jax.sharding import Mesh
from jax.sharding import PartitionSpec as P


BW = 1024
SPAN = 128
FS = ("fs_0", "fs_1", "fs_2")
REP_FS = ("rep", "fs_0", "fs_1", "fs_2")
LANES = 128
WIDE = 512
HALF_ROWS = 32
FIRST = (4, 4, 4, 4, 3, 3)
OTHERS = (4, 4, 4, 3, 4, 4)
RINGS = (("fs_2", 1), ("fs_1", 1), ("z", 1), ("fs_2", 3), ("fs_1", 3), ("z", 3))
PLACES = (2, 8, 32, 6, 24, 33)
ROUNDS = (
    (0, 4, 5, 3, 2, 1),
    (0, 4, 3, 5, 1, 2),
    (1, 5, 4, 2, 3, 0),
    (1, 5, 2, 4, 0, 3),
    (2, 3, 1, 0, 5, 4),
    (2, 3, 0, 1, 4, 5),
)

EPS = 1e-06


def other_core(x):
    return lax.ppermute(x, "tp", [(0, 1), (1, 0)])


def normed_rows(values, gain):
    factor = lax.rsqrt(jnp.mean(values * values, axis=1, keepdims=True) + EPS)
    return (values * factor * gain).astype(jnp.bfloat16)


def dot(left, right):
    return jnp.dot(left, right, preferred_element_type=jnp.float32)


def dot_rows(left, rows):
    return lax.dot_general(
        left, rows, (((1,), (1,)), ((), ())), preferred_element_type=jnp.float32
    )


def gelu(a):
    return 0.5 * a * (1.0 + jnp.tanh(0.7978845608028654 * (a + 0.044715 * a * a * a)))


def spec(block, index):
    return pl.BlockSpec(block, index)


def whole(shape):
    return pl.BlockSpec(shape, lambda *_: (0,) * len(shape))


ANY = pl.BlockSpec(memory_space=pl.ANY)


def params(steps):
    return pltpu.CompilerParams(
        dimension_semantics=("arbitrary",) * steps, vmem_limit_bytes=60 * 1024 * 1024
    )


def cost(flops, moved, special):
    return pl.CostEstimate(flops=flops, bytes_accessed=moved, transcendentals=special)


def exchange(x, color, turn):
    name, flip = RINGS[ROUNDS[color][turn]]
    axis = ("rep", "fs_0") if name == "z" else name
    return lax.ppermute(x, axis, [(i, i ^ flip) for i in range(4)])


def place(color, slot):
    at = 0
    for turn in range(6):
        if slot >> turn & 1:
            at ^= PLACES[ROUNDS[color][turn]]
    return at


def starts(widths):
    ends = [0]
    for n in widths:
        ends.append(ends[-1] + n * LANES)
    return ends


PAIRS = [(p, t + k) for t in (0, 2, 4, 6) for p in (0, 1) for k in (0, 1)]
PAIRS += [(0, 8), (0, 9), (1, 8), (1, 9), (0, 10), (1, 10)]


def prepare_kernel(rep, *refs):
    inputs, colors, held, sems = refs[:12], refs[12:15], refs[15:27], refs[27]
    copies = [
        pltpu.make_async_copy(x, y, sems.at[k]) for k, (x, y) in enumerate(zip(inputs, held))
    ]
    for copy in copies:
        copy.start()
    for copy in copies:
        copy.wait()
    gate, up, down, u, v, out, gate_s, up_s, down_s, u_s, v_s, out_s = held
    rows = pl.ds(pl.multiple_of(rep[0] * HALF_ROWS, HALF_ROWS), HALF_ROWS)
    low = jnp.bfloat16

    def across(scale):
        return scale[...][None, :]

    def down_rows(scale):
        size = scale.shape[0]
        row = lax.broadcasted_iota(jnp.int32, (HALF_ROWS, size), 0) + rep[0] * HALF_ROWS
        column = lax.broadcasted_iota(jnp.int32, (HALF_ROWS, size), 1)
        return jnp.sum(jnp.where(row == column, across(scale), 0.0), axis=1, keepdims=True)

    pair = ((gate[rows, :] * across(gate_s)).astype(low), (up[rows, :] * across(up_s)).astype(low))
    firsts = [pair[p][:, t * LANES : (t + 1) * LANES] for p, t in PAIRS]
    rest = jnp.concatenate(
        [
            (out[rows, :] * down_rows(out_s)).astype(low),
            (u[rows, :] * across(u_s)).astype(low),
            (v[rows, :] * across(v_s)).astype(low),
            (down[rows, :] * down_rows(down_s)).astype(low),
        ],
        axis=1,
    )
    at, begin = 0, starts(OTHERS)
    mine = []
    for c in range(6):
        mine.append(firsts[at : at + FIRST[c]] + [rest[:, begin[c] : begin[c + 1]]])
        at += FIRST[c]
    for pair, ref in enumerate(colors):
        ref[...] = jnp.concatenate(mine[2 * pair] + mine[2 * pair + 1], axis=1)


WIDTHS = [(a + b) * LANES for a, b in zip(FIRST, OTHERS)]
VMEM = pl.BlockSpec(memory_space=pltpu.VMEM)
SMEM = pl.BlockSpec(memory_space=pltpu.SMEM)
HBM = pl.BlockSpec(memory_space=pltpu.HBM)


def prepare(rep, *arrays):
    pairs = [WIDTHS[k] + WIDTHS[k + 1] for k in (0, 2, 4)]
    return pl.pallas_call(
        prepare_kernel,
        out_shape=[jax.ShapeDtypeStruct((HALF_ROWS, n), jnp.bfloat16) for n in pairs],
        in_specs=[SMEM] + [HBM] * len(arrays),
        out_specs=[VMEM] * 3,
        scratch_shapes=[pltpu.VMEM(x.shape, x.dtype) for x in arrays]
        + [pltpu.SemaphoreType.DMA((len(arrays),))],
        compiler_params=pltpu.CompilerParams(vmem_limit_bytes=60 * 1024 * 1024),
        name="prepare",
    )(rep, *arrays)


def join_kernel(cuts, *refs):
    sources = (len(refs) - len(cuts)) // 2
    for joined, (source, begin, end) in zip(refs[2 * sources :], cuts):
        held, arrived = refs[source], refs[sources + source]
        rows = held.shape[0]
        joined[pl.ds(0, rows), :] = held[:, begin:end]
        joined[pl.ds(rows, rows), :] = arrived[:, begin:end]


def cut_kernel(*refs):
    for k in range(len(refs) // 2):
        refs[len(refs) // 2 + k][...] = refs[k][:, : refs[len(refs) // 2 + k].shape[1]]


def first_columns(arrays, widths):
    return pl.pallas_call(
        cut_kernel,
        out_shape=[
            jax.ShapeDtypeStruct((x.shape[0], n * LANES), x.dtype) for x, n in zip(arrays, widths)
        ],
        in_specs=[VMEM] * len(arrays),
        out_specs=[VMEM] * len(arrays),
        compiler_params=pltpu.CompilerParams(vmem_limit_bytes=16 * 1024 * 1024),
        name="first_columns",
    )(*arrays)


def join(held, arrived, cuts=None):
    rows, low = held[0].shape[0], jnp.bfloat16
    if cuts is None:
        cuts = [(k, 0, x.shape[1]) for k, x in enumerate(held)]
    return pl.pallas_call(
        functools.partial(join_kernel, cuts),
        out_shape=[jax.ShapeDtypeStruct((2 * rows, b - a), low) for _, a, b in cuts],
        in_specs=[VMEM] * (2 * len(held)),
        out_specs=[VMEM] * len(cuts),
        compiler_params=pltpu.CompilerParams(vmem_limit_bytes=16 * 1024 * 1024),
        name="join",
    )(*held, *arrived)


def gather(pairs):
    ready = []
    for p, x in enumerate(pairs):
        (held,) = join([x], [exchange(x, 2 * p, 0)])
        edge = WIDTHS[2 * p]
        cuts = [(0, 0, edge), (0, edge, held.shape[1])]
        held = join([held], [exchange(held, 2 * p, 1)], cuts)
        held = join(held, [exchange(y, 2 * p + k, 2) for k, y in enumerate(held)])
        arrived = [exchange(y, 2 * p + k, 3) for k, y in enumerate(held)]
        held = join(held, arrived)
        ready.append((held, [exchange(y, 2 * p + k, 4) for k, y in enumerate(held)]))
    one, two = [], []
    for p, (held, arrived) in enumerate(ready):
        kept = first_columns(held, FIRST[2 * p : 2 * p + 2])
        early = [exchange(x, 2 * p + k, 5) for k, x in enumerate(kept)]
        come = first_columns(arrived, FIRST[2 * p : 2 * p + 2])
        late = [exchange(x, 2 * p + k, 5) for k, x in enumerate(come)]
        for k in range(2):
            one += [kept[k], come[k], early[k], late[k]]
        cuts = [(k, FIRST[2 * p + k] * LANES, y.shape[1]) for k, y in enumerate(held)]
        halves = join(held, arrived, cuts)
        for k, y in enumerate(halves):
            two += [y, exchange(y, 2 * p + k, 5)]
    return one, two


def place_blocks(at, pieces, weight, sems, widths, colors, first=0):
    begin = starts(widths)
    parts = len(pieces) // len(widths)
    slots = 64 // parts
    for c in colors:
        columns = pl.ds(begin[c], widths[c] * LANES)
        for k in range(parts):

            def copy_four(high, carry, c=c, k=k, columns=columns):
                moved = at ^ place(first + c, slots * k)
                for bit in range(slots.bit_length() - 3):
                    moved = moved ^ ((high >> bit & 1) * place(first + c, 4 << bit))
                for low in range(4):
                    to = (moved ^ place(first + c, low)) * HALF_ROWS
                    origin = (high * 4 + low) * HALF_ROWS
                    pltpu.make_async_copy(
                        pieces[parts * c + k].at[
                            pl.ds(pl.multiple_of(origin, HALF_ROWS), HALF_ROWS), :
                        ],
                        weight.at[pl.ds(pl.multiple_of(to, HALF_ROWS), HALF_ROWS), columns],
                        sems.at[c],
                    ).start()
                return carry

            lax.fori_loop(0, slots // 4, copy_four, 0)


def wait_color(weight, sems, widths, c):
    columns = pl.ds(starts(widths)[c], widths[c] * LANES)
    part = weight.at[:, columns]
    pltpu.make_async_copy(part, part, sems.at[c]).wait()


def silu_product(gate, up):
    return (gate / (1.0 + jnp.exp(-gate)) * up).astype(jnp.bfloat16)


def narrow_step(normed, weight):
    both = dot(normed, weight)
    tile = [both[:, k * LANES : (k + 1) * LANES] for k in range(6)]
    gate = jnp.concatenate([tile[0], tile[1], tile[4]], axis=1)
    up = jnp.concatenate([tile[2], tile[3], tile[5]], axis=1)
    return silu_product(gate, up)


def hidden_step(step, normed, weight, hidden):
    @pl.when((step >= 0) & (step < 4))
    def _():
        columns = pl.ds(pl.multiple_of(step * WIDE, WIDE), WIDE)
        both = dot(normed[...], weight[:, columns])
        to = pl.ds(pl.multiple_of(step * (WIDE // 2), WIDE // 2), WIDE // 2)
        hidden[:, to] = silu_product(both[:, : WIDE // 2], both[:, WIDE // 2 :])

    @pl.when(step == 4)
    def _():
        hidden[:, 2 * WIDE :] = narrow_step(normed[...], weight[:, 4 * WIDE :])


def first_kernel(core, at, own, other, gain, *rest):
    pieces, (hidden, kept, weight, normed, sems, out_sems) = rest[:24], rest[24:]
    step = pl.program_id(0)
    begin = starts(FIRST)
    copies = []
    for c in range(6):
        columns = pl.ds(begin[c], FIRST[c] * LANES)
        copies.append(
            pltpu.make_async_copy(weight.at[:, columns], kept.at[:, columns], out_sems.at[c])
        )

    for k, colors in enumerate(((0, 1, 2), (3,), (4,), (5,))):

        @pl.when(step == k)
        def _():
            place_blocks(at[0], pieces, weight, sems, FIRST, colors)

    @pl.when(step == 0)
    def _():
        left = jnp.where(core[0] == 0, own[...], other[...])
        right = jnp.where(core[0] == 0, other[...], own[...])
        values = jnp.concatenate([left, right], axis=1).astype(jnp.float32)
        normed[...] = normed_rows(values, gain[...])

    for c in range(6):

        @pl.when(step == min(c, 4))
        def _():
            wait_color(weight, sems, FIRST, c)
            copies[c].start()

    hidden_step(step, normed, weight, hidden)

    @pl.when(step == 4)
    def _():
        for copy in copies:
            copy.wait()


def first_hidden(core, at, own, other, gain, pieces):
    count, half = own.shape
    width = 2 * half
    columns = sum(FIRST) * LANES
    units = columns // 2
    return pl.pallas_call(
        first_kernel,
        out_shape=[
            jax.ShapeDtypeStruct((count, units), jnp.bfloat16),
            jax.ShapeDtypeStruct((width, columns), jnp.bfloat16),
        ],
        grid_spec=pltpu.PrefetchScalarGridSpec(
            num_scalar_prefetch=2,
            grid=(5,),
            in_specs=[whole((count, half)), whole((count, half)), whole((1, width))] + [ANY] * 24,
            out_specs=[whole((count, units)), ANY],
            scratch_shapes=[
                pltpu.VMEM((width, columns), jnp.bfloat16),
                pltpu.VMEM((count, width), jnp.bfloat16),
                pltpu.SemaphoreType.DMA((6,)),
                pltpu.SemaphoreType.DMA((6,)),
            ],
        ),
        compiler_params=params(1),
        cost_estimate=cost(2 * count * width * columns, 4 * width * columns, count * units),
        name="first_hidden",
    )(core, at, own, other, gain, *pieces)


MIXER, DOWN = OTHERS[:3], OTHERS[3:]


def place_blocks_of(at, pieces, weight, sems, widths, first):
    place_blocks(at, pieces, weight, sems, widths, range(len(widths)), first)


QUARTER = WIDE // HALF_ROWS


def down_kernel(at, hidden, *rest):
    pieces, (term, kept, weight, sems, out_sems) = rest[:6], rest[6:]
    step = pl.program_id(0)
    begin = starts(DOWN)

    @pl.when(step == 0)
    def _():
        for quarter in range(4):
            for c in range(3):
                columns = pl.ds(begin[c], DOWN[c] * LANES)
                for slot in range(64):
                    moved = place(3 + c, slot)
                    if moved // QUARTER != quarter:
                        continue
                    to = pl.multiple_of((at[0] ^ moved) * HALF_ROWS, HALF_ROWS)
                    pltpu.make_async_copy(
                        pieces[2 * c + slot // 32].at[
                            pl.ds(slot % 32 * HALF_ROWS, HALF_ROWS), :
                        ],
                        weight.at[pl.ds(to, HALF_ROWS), columns],
                        sems.at[quarter],
                    ).start()

    def rows_of(quarter):
        block = ((at[0] // QUARTER) ^ quarter) * WIDE
        return pl.ds(pl.multiple_of(block, WIDE), WIDE)

    copies = []
    for quarter in range(4):
        part = weight.at[rows_of(quarter), :]
        copy = pltpu.make_async_copy(part, kept.at[rows_of(quarter), :], out_sems.at[quarter])
        copies.append(copy)

        @pl.when(step == quarter)
        def _():
            pltpu.make_async_copy(part, part, sems.at[quarter]).wait()
            copy.start()

    part = weight[rows_of(step), :]
    term[...] = dot_rows(hidden[...], part).astype(jnp.bfloat16)

    @pl.when(step == 3)
    def _():
        for copy in copies:
            copy.wait()


def first_down(at, hidden, width, pieces):
    count, units = hidden.shape
    return pl.pallas_call(
        down_kernel,
        out_shape=[
            jax.ShapeDtypeStruct((count, width), jnp.bfloat16),
            jax.ShapeDtypeStruct((width, units), jnp.bfloat16),
        ],
        grid_spec=pltpu.PrefetchScalarGridSpec(
            num_scalar_prefetch=1,
            grid=(width // WIDE,),
            in_specs=[whole((count, units))] + [ANY] * 6,
            out_specs=[spec((count, WIDE), lambda j, a: (0, (a[0] // QUARTER) ^ j)), ANY],
            scratch_shapes=[
                pltpu.VMEM((width, units), jnp.bfloat16),
                pltpu.SemaphoreType.DMA((4,)),
                pltpu.SemaphoreType.DMA((4,)),
            ],
        ),
        compiler_params=params(1),
        cost_estimate=cost(2 * count * width * units, 4 * width * units, 0),
        name="first_down",
    )(at, hidden, *pieces)


def assemble_kernel(at, *rest):
    pieces, (kept, weight, sems, out_sems) = rest[:6], rest[6:]
    place_blocks_of(at[0], pieces, weight, sems, MIXER, 0)
    begin = starts(MIXER)
    copies = []
    for c in range(3):
        wait_color(weight, sems, MIXER, c)
        columns = pl.ds(begin[c], MIXER[c] * LANES)
        copy = pltpu.make_async_copy(weight.at[:, columns], kept.at[:, columns], out_sems.at[c])
        copy.start()
        copies.append(copy)
    for copy in copies:
        copy.wait()


def assemble(at, width, pieces):
    shape = (width, sum(MIXER) * LANES)
    return pl.pallas_call(
        assemble_kernel,
        out_shape=jax.ShapeDtypeStruct(shape, jnp.bfloat16),
        grid_spec=pltpu.PrefetchScalarGridSpec(
            num_scalar_prefetch=1,
            grid=(1,),
            in_specs=[ANY] * 6,
            out_specs=ANY,
            scratch_shapes=[
                pltpu.VMEM(shape, jnp.bfloat16),
                pltpu.SemaphoreType.DMA((3,)),
                pltpu.SemaphoreType.DMA((3,)),
            ],
        ),
        compiler_params=params(1),
        cost_estimate=cost(5 * 10**9, 8 * shape[0] * shape[1], 0),
        name="assemble",
    )(at, *pieces)


def gates_kernel(core, own, other, term, far, gain, rows, middle, act, sums, normed):
    @pl.when(pl.program_id(0) == 0)
    def _():
        left = jnp.where(core[0] == 0, own[...], other[...])
        right = jnp.where(core[0] == 0, other[...], own[...])
        values = jnp.concatenate([left, right], axis=1).astype(jnp.float32)
        values = values + 0.5 * (term[...].astype(jnp.float32) + far[...].astype(jnp.float32))
        mid = values.astype(jnp.bfloat16)
        middle[...] = mid
        normed[...] = normed_rows(mid.astype(jnp.float32), gain[...])

    acted = gelu(dot(normed[...], rows[...]))
    act[0] = acted

    @pl.when(pl.program_id(0) == 0)
    def _():
        lane = lax.broadcasted_iota(jnp.int32, sums.shape, 1)
        total = jnp.sum(acted, axis=1, keepdims=True)
        squares = jnp.sum(acted * acted, axis=1, keepdims=True)
        sums[...] = jnp.where(lane == 0, total, squares)


def gates(core, own, other, term, far, gain, weight, chans):
    count, half = own.shape
    width = 2 * half
    return pl.pallas_call(
        gates_kernel,
        out_shape=[
            jax.ShapeDtypeStruct((count, width), jnp.bfloat16),
            jax.ShapeDtypeStruct((2, count, chans), jnp.float32),
            jax.ShapeDtypeStruct((count, LANES), jnp.float32),
        ],
        grid_spec=pltpu.PrefetchScalarGridSpec(
            num_scalar_prefetch=1,
            grid=(2,),
            in_specs=[
                whole((count, half)),
                whole((count, half)),
                whole((count, width)),
                whole((count, width)),
                whole((1, width)),
                spec((width, chans), lambda i, c: (0, 2 - i)),
            ],
            out_specs=[
                whole((count, width)),
                spec((1, count, chans), lambda i, c: (i, 0, 0)),
                whole((count, LANES)),
            ],
            scratch_shapes=[pltpu.VMEM((count, width), jnp.bfloat16)],
        ),
        compiler_params=params(1),
        cost_estimate=cost(4 * count * width * chans, 4 * width * chans, 2 * count * chans),
        name="gates",
    )(core, own, other, term, far, gain, weight)


def mix_kernel(act, sums, far, gain, bias, weight, shift, rows, term, mixed):
    groups = weight.shape[0]

    @pl.when(pl.program_id(0) == 0)
    def _():
        at = lax.broadcasted_iota(jnp.int32, (SPAN, SPAN), 0)
        source = lax.broadcasted_iota(jnp.int32, (SPAN, SPAN), 1)
        masked = [
            jnp.where(source <= at, weight[g], jnp.zeros_like(weight[g])) for g in range(groups)
        ]
        count, chans = mixed.shape
        wide = chans // groups
        column = [
            jnp.sum(jnp.where(source == at, shift[g : g + 1, :], 0.0), axis=1, keepdims=True)
            for g in range(groups)
        ]
        for n in range(count // SPAN):
            block = pl.ds(n * SPAN, SPAN)
            totals = (sums[block, :] + far[block, :]) / BW
            v_mean = totals[:, 0:1]
            v_var = totals[:, 1:2] - v_mean * v_mean
            v_normed = (act[0, block, :] - v_mean) * lax.rsqrt(v_var + EPS) * gain[...] + bias[...]
            v_normed = v_normed.astype(jnp.bfloat16)
            spatial = [
                dot(masked[g], v_normed[:, g * wide : (g + 1) * wide]) + column[g]
                for g in range(groups)
            ]
            product = act[1, block, :] * jnp.concatenate(spatial, axis=1)
            mixed[block, :] = product.astype(jnp.bfloat16)

    term[...] = dot_rows(mixed[...], rows[...]).astype(jnp.bfloat16)


def mix(act, sums, far, gain, bias, weight, shift, rows):
    _, count, chans = act.shape
    width = rows.shape[0]
    groups = weight.shape[0]
    return pl.pallas_call(
        mix_kernel,
        out_shape=jax.ShapeDtypeStruct((count, width), jnp.bfloat16),
        grid=(width // WIDE,),
        in_specs=[
            whole(act.shape),
            whole((count, LANES)),
            whole((count, LANES)),
            whole((1, chans)),
            whole((1, chans)),
            whole((groups, SPAN, SPAN)),
            whole((groups, SPAN)),
            spec((WIDE, chans), lambda j: (j, 0)),
        ],
        out_specs=spec((count, WIDE), lambda j: (0, j)),
        scratch_shapes=[pltpu.VMEM((count, chans), jnp.bfloat16)],
        compiler_params=params(1),
        cost_estimate=cost(2 * count * width * chans, 2 * width * chans, count),
        name="mix",
    )(act, sums, far, gain, bias, weight, shift, rows)


def second_kernel(
    core, middle, term, far, gain, first, others, send, keep, base, normed, hidden, wide, down, sems
):
    step = pl.program_id(0)
    steps = 5
    outs = down.shape[0] // WIDE
    cuts = [pl.ds(k * WIDE, WIDE) for k in range(4)] + [pl.ds(4 * WIDE, 6 * LANES)]
    copies = [
        pltpu.make_async_copy(first.at[:, cut], wide.at[:, cut], sems.at[k])
        for k, cut in enumerate(cuts)
    ]
    copies.append(pltpu.make_async_copy(others, down, sems.at[steps]))

    @pl.when(step == 0)
    def _():
        for copy in copies:
            copy.start()
        values = middle[...].astype(jnp.float32) + (
            term[...].astype(jnp.float32) + far[...].astype(jnp.float32)
        )
        second = values.astype(jnp.bfloat16)
        half = second.shape[1] // 2
        base[...] = jnp.where(core[0] == 0, second[:, :half], second[:, half:])
        normed[...] = normed_rows(second.astype(jnp.float32), gain[...])

    for k, copy in enumerate(copies):

        @pl.when(step == k)
        def _():
            copy.wait()

    hidden_step(step, normed, wide, hidden)

    @pl.when(step >= steps)
    def _():
        n = step - steps
        mine = jnp.where(n < outs // 2, 1 - core[0], core[0])
        row = mine * (outs // 2) + lax.rem(n, outs // 2)
        rows = pl.ds(pl.multiple_of(row * WIDE, WIDE), WIDE)
        part = dot_rows(hidden[...], down[rows, :]).astype(jnp.bfloat16)

        @pl.when(n < outs // 2)
        def _():
            send[...] = part

        @pl.when(n >= outs // 2)
        def _():
            columns = pl.ds(pl.multiple_of((n - outs // 2) * WIDE, WIDE), WIDE)
            keep[...] = base[:, columns].astype(jnp.float32) + 0.5 * part.astype(jnp.float32)


def second_pass(core, middle, term, far, gain, first, others):
    count, width = middle.shape
    half = width // 2
    columns = first.shape[1]
    units = columns // 2
    outs = width // WIDE
    sent = outs // 2
    return pl.pallas_call(
        second_kernel,
        out_shape=[jax.ShapeDtypeStruct((count, half), x) for x in (jnp.bfloat16, jnp.float32)],
        grid_spec=pltpu.PrefetchScalarGridSpec(
            num_scalar_prefetch=1,
            grid=(5 + outs,),
            in_specs=[
                whole((count, width)),
                whole((count, width)),
                whole((count, width)),
                whole((1, width)),
                ANY,
                ANY,
            ],
            out_specs=[
                spec((count, WIDE), lambda j, c: (0, jnp.clip(j - 5, 0, sent - 1))),
                spec((count, WIDE), lambda j, c: (0, jnp.maximum(j - 5 - sent, 0))),
            ],
            scratch_shapes=[
                pltpu.VMEM((count, half), jnp.bfloat16),
                pltpu.VMEM((count, width), jnp.bfloat16),
                pltpu.VMEM((count, units), jnp.bfloat16),
                pltpu.VMEM((width, columns), jnp.bfloat16),
                pltpu.VMEM((width, units), jnp.bfloat16),
                pltpu.SemaphoreType.DMA((6,)),
            ],
        ),
        compiler_params=params(1),
        cost_estimate=cost(6 * count * width * units, 6 * width * units, count * units),
        name="second_pass",
    )(core, middle, term, far, gain, first, others)


def layer(
    tokens,
    norm_first,
    norm_mix,
    norm_second,
    gate_weight,
    up_weight,
    down_weight,
    gate_scale,
    up_scale,
    down_scale,
    u_weight,
    v_weight,
    u_scale,
    v_scale,
    ln_gain,
    ln_bias,
    spatial_weight,
    spatial_bias,
    out_weight,
    out_scale,
):
    chans = u_weight.shape[1]
    width = 2 * tokens.shape[1]

    def number(x):
        return x.reshape(1).astype(jnp.int32)

    core = number(lax.axis_index("tp"))
    rep = lax.axis_index("rep")
    at = number(2 * lax.axis_index(FS) + rep)

    colors = prepare(
        number(rep),
        gate_weight,
        up_weight,
        down_weight.T,
        u_weight,
        v_weight,
        out_weight.T,
        gate_scale,
        up_scale,
        down_scale,
        u_scale,
        v_scale,
        out_scale,
    )
    one, two = gather(colors)

    own, other = tokens, other_core(tokens)
    hidden, first = first_hidden(core, at, own, other, norm_first[None], one)
    term, down = first_down(at, hidden, width, two[6:])
    far = other_core(term)
    mixer = assemble(at, width, two[:6])
    middle, act, sums = gates(core, own, other, term, far, norm_mix[None], mixer, chans)
    term = mix(
        act,
        sums,
        other_core(sums),
        ln_gain[None],
        ln_bias[None],
        spatial_weight,
        spatial_bias,
        mixer,
    )
    send, keep = second_pass(
        core, middle, term, other_core(term), norm_second[None], first, down
    )
    return (keep + 0.5 * other_core(send).astype(jnp.float32)).astype(jnp.bfloat16)


def solution(mesh):
    torus = Mesh(
        mesh.devices.reshape(mesh.shape["rep"], 2, 4, 4, mesh.shape["tp"]),
        ("rep", "fs_0", "fs_1", "fs_2", "tp"),
    )
    in_specs = (
        P(REP_FS, "tp"),
        P(),
        P(),
        P(),
        P(FS, "tp"),
        P(FS, "tp"),
        P("tp", FS),
        P("tp"),
        P("tp"),
        P(FS),
        P(FS, "tp"),
        P(FS, "tp"),
        P("tp"),
        P("tp"),
        P("tp"),
        P("tp"),
        P("tp", None, None),
        P("tp", None),
        P("tp", FS),
        P(FS),
    )
    out_specs = P(REP_FS, "tp")
    return jax.shard_map(layer, mesh=torus, in_specs=in_specs, out_specs=out_specs, check_vma=False)
```
